128 devices in a mesh: sp: 32 (over z, y, core), tp: 4 (over x).
Axes of the slice: x: 4, y: 4, z: 4, core: 2. Of those that a mesh axis runs over, the one named last changes fastest.
Arguments:
- tokens: bfloat16 [12288, 4096], P(('sp', 'tp')), may hold values from -6 to 6
- norm_gain: float32 [4096], replicated, may hold values from 0.1 to 1.9
- w_query: bfloat16 [4096, 2048], P('sp', 'tp'), may hold values from -0.09375 to 0.09375
- w_key: bfloat16 [4096, 512], P('sp', 'tp'), may hold values from -1.5 to 1.5
- w_value: bfloat16 [4096, 512], P('sp', 'tp'), may hold values from -0.09375 to 0.09375
- w_mem_query: bfloat16 [4096, 1024], P('sp', 'tp'), may hold values from -0.09375 to 0.09375
- w_mem_key: bfloat16 [4096, 1024], P('sp', 'tp'), may hold values from -0.09375 to 0.09375
- w_mem_value: bfloat16 [4096, 1024], P('sp', 'tp'), may hold values from -0.09375 to 0.09375
- w_mem_gate: bfloat16 [4096, 1024], P('sp', 'tp'), may hold values from -0.09375 to 0.09375
- w_gates: bfloat16 [4096, 2, 16], replicated, may hold values from -0.09375 to 0.09375
- sinks: float32 [32], P('tp'), may hold values from 2 to 6
- forget_bias: float32 [16], P('tp'), may hold values from 3 to 13
- forget_shift: float32 [12288, 16], P('sp', 'tp'), may hold values from -1 to 0
- w_out: bfloat16 [3072, 4096], P('sp', 'tp'), may hold values from -0.21650635 to 0.21650635
Outputs:
- mixed: bfloat16 [12288, 4096], P('sp', 'tp')
- log_total: float32 [12288, 32], P('sp', 'tp')
The draws below stay inside these ranges and needn't reach their ends.
All inputs are finite; a program needn't handle non-finite values.
Results may differ from the reference program's by a relative error of at most 0.018.
Values may be sent and summed in bfloat16 or wider, within the bound.
A program may use at most 128 MiB of HBM per device.

```python
import math
import jax
import jax.numpy as jnp
from jax import lax

D = 4096
QH = 32
KVH = 8
CELL_SUBSPACES = 16
HD = 64
WINDOW = 128
BLK = 128
TOK_DEV = 384
ITEM_COUNT = 12288
MIX = 3072


def query_base(key):
    normal_noise = jax.random.normal(jax.random.fold_in(key, 101), (D, QH * HD), jnp.float32)
    return jnp.clip(normal_noise, -6.0, 6.0) * D ** (-0.5)


def draw_w_query(key, part):
    return query_base(key).astype(jnp.bfloat16)


def draw_w_key(key, part):
    normal_noise = jax.random.normal(jax.random.fold_in(key, 102), (D, KVH * HD), jnp.float32)
    own_columns = jnp.clip(normal_noise, -6.0, 6.0) * D ** (-0.5)
    return own_columns.astype(jnp.bfloat16)


def draw_forget_bias(key, part):
    ordering = jax.random.permutation(jax.random.fold_in(key, 201), CELL_SUBSPACES)
    slow_heads = ordering < CELL_SUBSPACES // 2
    jitter = jax.random.uniform(jax.random.fold_in(key, 202), (CELL_SUBSPACES,), jnp.float32, -0.3, 0.3)
    fast_values = jax.random.uniform(jax.random.fold_in(key, 203), (CELL_SUBSPACES,), jnp.float32, 3.4, 4.6)
    slow_values = math.log(4.0 * ITEM_COUNT) + jitter
    return jnp.where(slow_heads, slow_values, fast_values).astype(jnp.float32)


def draw_forget_shift(key, part):
    device_count = ITEM_COUNT // TOK_DEV
    spread = jax.random.uniform(jax.random.fold_in(key, 301), (device_count,), jnp.float32, math.log(0.35), math.log(2.8))
    rates = jnp.exp(spread) * (-0.3 / ITEM_COUNT)
    per_element = jnp.repeat(rates, TOK_DEV, total_repeat_length=ITEM_COUNT)
    place_indices = jax.random.randint(jax.random.fold_in(key, 302), (3, CELL_SUBSPACES), 0, ITEM_COUNT)
    stack_tiers = jax.random.uniform(jax.random.fold_in(key, 303), (3, CELL_SUBSPACES), jnp.float32, 0.22, 0.69)
    element_tally = jnp.arange(ITEM_COUNT)[:, None]
    spurt_bundles = jnp.zeros((ITEM_COUNT, CELL_SUBSPACES), jnp.float32)
    for spurt_tally in range(3):
        spurt_bundles = spurt_bundles + jnp.where(element_tally == place_indices[spurt_tally][None, :], stack_tiers[spurt_tally][None, :], 0.0)
    return (per_element[:, None] - spurt_bundles).astype(jnp.float32)


def draw_w_out(key, part):
    normal_noise = jax.random.normal(jax.random.fold_in(key, 401), (MIX, D), jnp.float32)
    row_scale = jnp.where(jnp.arange(MIX) < QH * HD, 2.0, 1.0)
    return (jnp.clip(normal_noise, -6.0, 6.0) * MIX ** (-0.5) * row_scale[:, None]).astype(jnp.bfloat16)


def block_scale(stream_key, extent, pieces, smallest, high):
    gain = 1.0
    for dim, shards_of in pieces:
        draws = jax.random.uniform(jax.random.fold_in(jax.random.fold_in(stream_key, 6), dim), (shards_of,), jnp.float32, smallest / len(pieces), high / len(pieces))
        gain = gain * jnp.repeat(jnp.exp(draws), extent[dim] // shards_of).reshape((-1,) + (1,) * (len(extent) - 1 - dim))
    return gain


def noise(key, shape, scale, reach, cuts=(), held_as=jnp.bfloat16):
    values = scale * jax.random.normal(key, shape, jnp.float32)
    if cuts:
        values = values * block_scale(key, shape, cuts, -0.22, 0.18)
    return jnp.clip(values, -reach, reach).astype(held_as)


def setup_inputs(seed: int = 0) -> dict:
    key_list = jax.random.split(jax.random.key(seed), 15)
    return {
        "tokens": noise(key_list[0], (ITEM_COUNT, D), 1.0, 6.0, ((0, 128),)),
        "norm_gain": jnp.clip(1.0 + 0.18 * jax.random.normal(key_list[1], (D,), jnp.float32), 0.1, 1.9),
        "w_query": draw_w_query(jax.random.fold_in(key_list[14], 71), 0),
        "w_key": draw_w_key(jax.random.fold_in(key_list[14], 71), 0),
        "w_value": noise(key_list[4], (D, KVH * HD), D ** -0.5, 0.09375, ((0, 32), (1, 4))),
        "w_mem_query": noise(key_list[5], (D, CELL_SUBSPACES * HD), D ** -0.5, 0.09375, ((0, 32), (1, 4))),
        "w_mem_key": noise(key_list[6], (D, CELL_SUBSPACES * HD), D ** -0.5, 0.09375, ((0, 32), (1, 4))),
        "w_mem_value": noise(key_list[7], (D, CELL_SUBSPACES * HD), D ** -0.5, 0.09375, ((0, 32), (1, 4))),
        "w_mem_gate": noise(key_list[8], (D, CELL_SUBSPACES * HD), D ** -0.5, 0.09375, ((0, 32), (1, 4))),
        "w_gates": noise(key_list[9], (D, 2, CELL_SUBSPACES), D ** -0.5, 0.09375),
        "sinks": jnp.clip(2.0 + 4.0 * jax.random.uniform(key_list[10], (QH,), jnp.float32) ** block_scale(key_list[10], (QH,), ((0, 4),), -0.2, 0.2), 2.0, 6.0),
        "forget_bias": draw_forget_bias(jax.random.fold_in(key_list[14], 71), 0),
        "forget_shift": draw_forget_shift(jax.random.fold_in(key_list[14], 71), 0),
        "w_out": draw_w_out(jax.random.fold_in(key_list[14], 71), 0),
    }


EPSILON = 1e-06
MASKED = -1e+30
exact_precision = lax.Precision.HIGHEST

def normalize(tokens, norm_gain):
    values = tokens.astype(jnp.float32)
    rescale = lax.rsqrt(lax.optimization_barrier(jnp.mean(values * values, axis=-1, keepdims=True)) + EPSILON)
    return (values * rescale * norm_gain).astype(jnp.bfloat16)

def advance(carried, key_block, value_block, in_block, cumulative):
    memory_state, normalizer, stabilizer = carried
    block_total = cumulative[:, -1]
    decays = block_total[:, None] - cumulative + in_block
    new_stabilizer = jnp.maximum(block_total + stabilizer, lax.optimization_barrier(jnp.max(decays, axis=-1)))
    weights = jnp.exp(decays - new_stabilizer[:, None])
    rescale = jnp.exp(block_total + stabilizer - new_stabilizer)
    new_state = rescale[:, None, None] * memory_state + jnp.einsum('hsv,hsk->hvk', value_block * weights[:, :, None], key_block, precision=exact_precision)
    new_normalizer = rescale[:, None] * normalizer + jnp.einsum('hs,hsk->hk', weights, key_block, precision=exact_precision)
    return (new_state, new_normalizer, new_stabilizer)

def block_step(carried, block_data):
    memory_state, normalizer, stabilizer = carried
    query_block, key_block, value_block, in_block, forget_block = block_data
    length = in_block.shape[-1]
    cumulative = jnp.cumsum(forget_block, axis=-1)
    causal = lax.broadcasted_iota(jnp.int32, (length, length), 0) >= lax.broadcasted_iota(jnp.int32, (length, length), 1)
    log_weight = jnp.where(causal[None], cumulative[:, :, None] - cumulative[:, None, :] + in_block[:, None, :], MASKED)
    row_level = jnp.maximum(cumulative + stabilizer[:, None], lax.optimization_barrier(jnp.max(log_weight, axis=-1)))
    carried_part = jnp.exp(cumulative + stabilizer[:, None] - row_level)
    affinity = jnp.einsum('htd,hsd->hts', query_block, key_block, precision=exact_precision) * jnp.exp(log_weight - row_level[:, :, None])
    numerator = carried_part[:, :, None] * jnp.einsum('hvk,htk->htv', memory_state, query_block, precision=exact_precision) + jnp.einsum('hts,hsv->htv', affinity, value_block, precision=exact_precision)
    denominator = carried_part * jnp.einsum('hk,htk->ht', normalizer, query_block, precision=exact_precision) + lax.optimization_barrier(jnp.sum(affinity, axis=-1))
    recall = numerator / jnp.maximum(jnp.abs(denominator), jnp.exp(-row_level))[:, :, None]
    return (advance(carried, key_block, value_block, in_block, cumulative), recall)

def reference(tokens, norm_gain, w_query, w_key, w_value, w_mem_query, w_mem_key, w_mem_value, w_mem_gate, w_gates, sinks, forget_bias, forget_shift, w_out):
    normed = normalize(tokens, norm_gain)

    def project(weight):
        return jnp.dot(normed, weight, preferred_element_type=jnp.float32).astype(jnp.bfloat16)
    query = project(w_query)
    key_rows = project(w_key)
    value_rows = project(w_value)
    mem_query = project(w_mem_query)
    mem_key = project(w_mem_key)
    mem_value = project(w_mem_value)
    mem_gate = project(w_mem_gate)
    gate_pre = jnp.dot(normed, w_gates.reshape(D, 2 * CELL_SUBSPACES), preferred_element_type=jnp.float32).reshape(ITEM_COUNT, 2, CELL_SUBSPACES)
    group_size = QH // KVH
    block_count = ITEM_COUNT // WINDOW
    q_blocks = query.reshape(block_count, WINDOW, KVH, group_size, HD)
    zero_rim = jnp.zeros((WINDOW, KVH * HD), jnp.bfloat16)
    padded_keys = jnp.concatenate([zero_rim, key_rows], axis=0).reshape(block_count + 1, WINDOW, KVH, HD)
    padded_values = jnp.concatenate([zero_rim, value_rows], axis=0).reshape(block_count + 1, WINDOW, KVH, HD)
    key_window = jnp.concatenate([padded_keys[:-1], padded_keys[1:]], axis=1)
    value_window = jnp.concatenate([padded_values[:-1], padded_values[1:]], axis=1)
    query_index = lax.broadcasted_iota(jnp.int32, (WINDOW, 2 * WINDOW), 0)
    key_index = lax.broadcasted_iota(jnp.int32, (WINDOW, 2 * WINDOW), 1)
    distance = query_index - key_index + WINDOW
    in_band = (distance >= 0) & (distance < WINDOW)
    sink_logit = sinks.reshape(KVH, group_size, 1, 1)

    def one_block(block_data):
        query_block, key_block, value_block, block_index = block_data
        scores = jnp.einsum('qhgd,khd->hgqk', query_block.astype(jnp.float32), key_block.astype(jnp.float32)) * HD ** (-0.5)
        key_position = block_index * WINDOW - WINDOW + key_index
        allowed = in_band & (key_position >= 0)
        scores = jnp.where(allowed[None, None], scores, MASKED)
        ceiling = jnp.maximum(lax.optimization_barrier(jnp.max(scores, axis=-1, keepdims=True)), sink_logit)
        weights = jnp.exp(scores - ceiling)
        partition = jnp.exp(sink_logit - ceiling) + lax.optimization_barrier(jnp.sum(weights, axis=-1, keepdims=True))
        log_part = (ceiling + jnp.log(partition))[..., 0].transpose(2, 0, 1).reshape(WINDOW, QH)
        probs = (weights / partition).astype(jnp.bfloat16)
        head_out = jnp.einsum('hgqk,khd->qhgd', probs.astype(jnp.float32), value_block.astype(jnp.float32))
        return (head_out.astype(jnp.bfloat16).reshape(WINDOW, QH * HD), log_part)
    attn_blocks, log_blocks = lax.map(one_block, (q_blocks, key_window, value_window, jnp.arange(block_count, dtype=jnp.int32)))
    attn_out = attn_blocks.reshape(ITEM_COUNT, QH * HD)
    log_total = log_blocks.reshape(ITEM_COUNT, QH)
    log_in = gate_pre[:, 0, :] - 0.5 * math.log(ITEM_COUNT)
    log_forget = jax.nn.log_sigmoid(gate_pre[:, 1, :] + forget_bias) + forget_shift
    mem_blocks = ITEM_COUNT // BLK

    def blocks(array):
        return array.astype(jnp.float32).reshape(mem_blocks, BLK, CELL_SUBSPACES, HD).transpose(0, 2, 1, 3)

    def gate_blocks(array):
        return array.reshape(mem_blocks, BLK, CELL_SUBSPACES).transpose(0, 2, 1)
    initial = (jnp.zeros((CELL_SUBSPACES, HD, HD), jnp.float32), jnp.zeros((CELL_SUBSPACES, HD), jnp.float32), jnp.full((CELL_SUBSPACES,), MASKED, jnp.float32))
    inputs = (blocks(mem_query), blocks(mem_key) * HD ** (-0.5), blocks(mem_value), gate_blocks(log_in), gate_blocks(log_forget))
    _, recall = lax.scan(block_step, initial, inputs)
    recall = recall.transpose(0, 2, 1, 3).reshape(ITEM_COUNT, CELL_SUBSPACES * HD)
    mem_out = (recall * jax.nn.sigmoid(mem_gate.astype(jnp.float32))).astype(jnp.bfloat16)
    joined = jnp.concatenate([attn_out, mem_out], axis=1)
    mixed = jnp.dot(joined, w_out, preferred_element_type=jnp.float32).astype(jnp.bfloat16)
    return (mixed, log_total)
```

```python
import functools
import math

import jax
import jax.numpy as jnp
from jax import lax
from jax.experimental import pallas as pl
from jax.experimental.pallas import tpu as pltpu
from jax.sharding import Mesh
from jax.sharding import PartitionSpec as P

HD = 64
WINDOW = 128
BLK = 128
EPSILON = 1e-06
MASKED = -1e30
exact_precision = lax.Precision.HIGHEST
MESH = pl.DeviceIdType.MESH
RING = 4
TOK = 96
ROWS = 8 * TOK
D = 4096
PLANE = ("z", "y")
MAX_COPIES = 192


class Wires:
    def __init__(self, send_sem, recv_sem):
        self.send_sem, self.recv_sem = send_sem, recv_sem
        self.count = 0
        self.started = []
        z, y, c, x = (lax.axis_index(a) for a in ("z", "y", "c", "x"))
        self.at = {"z": z, "y": y, "c": c, "x": x}

    def moved(self, **new):
        where = dict(self.at)
        where.update(new)
        return (where["z"], where["y"], where["c"], where["x"])

    def step(self, axis, distance):
        return lax.rem(self.at[axis] + distance + RING, RING)

    def neighbour(self, axis, distance):
        return self.moved(**{axis: self.step(axis, distance)})

    def partner(self):
        return self.moved(c=1 - self.at["c"])

    def send(self, src, dst, device):
        k = self.count
        self.count += 1
        copy = pltpu.make_async_remote_copy(
            src_ref=src,
            dst_ref=dst,
            send_sem=self.send_sem.at[k],
            recv_sem=self.recv_sem.at[k],
            device_id=device,
            device_id_type=MESH,
        )
        copy.start()
        self.started.append(copy)
        return k

    def arrived(self, k, dst):
        pltpu.make_async_remote_copy(
            src_ref=dst,
            dst_ref=dst,
            send_sem=self.send_sem.at[k],
            recv_sem=self.recv_sem.at[k],
            device_id=self.partner(),
            device_id_type=MESH,
        ).wait_recv()

    def finish(self):
        for copy in self.started:
            copy.wait_send()


class PlaneGather:
    def __init__(self, wires, whole, depth, core):
        self.w, self.whole, self.depth, self.core = wires, whole, depth, core
        self.first, self.second = ("z", "y") if core == 0 else ("y", "z")
        self.sent = {}

    def rows(self, d1, d2, part=None):
        i1, i2 = self.w.step(self.first, d1), self.w.step(self.second, d2)
        z, y = (i1, i2) if self.core == 0 else (i2, i1)
        start = ((z * RING + y) * 2 + self.core) * self.depth
        half = self.depth // 2
        if part is None:
            return self.whole.at[pl.ds(pl.multiple_of(start, 16), self.depth)]
        return self.whole.at[pl.ds(pl.multiple_of(start + part * half, 16), half)]

    def go(self, name, d1, d2, axis, distance, part=None):
        block = self.rows(d1, d2, part)
        self.sent[name] = self.w.send(block, block, self.w.neighbour(axis, distance))

    def came(self, name, d1, d2, part=None):
        self.w.arrived(self.sent[name], self.rows(d1, d2, part))

    def second_round(self, d1):
        self.go(("b+", d1), d1, 0, self.second, 1)
        self.go(("b-", d1), d1, 0, self.second, -1)

    def start_first(self):
        self.go("a+", 0, 0, self.first, 1)
        self.go("a-", 0, 0, self.first, -1)

    def start_second(self):
        self.second_round(0)

    def first_came(self):
        self.came("a+", -1, 0)
        self.go("ah+", -1, 0, self.first, 1, 0)
        self.second_round(-1)
        self.came("a-", 1, 0)
        self.go("ah-", 1, 0, self.first, -1, 1)
        self.second_round(1)

    def second_came(self, d1):
        self.came(("b+", d1), d1, -1)
        self.go(("bh+", d1), d1, -1, self.second, 1, 0)
        self.came(("b-", d1), d1, 1)
        self.go(("bh-", d1), d1, 1, self.second, -1, 1)

    def first_done(self):
        self.came("ah+", 2, 0, 0)
        self.came("ah-", 2, 0, 1)
        self.second_round(2)

    def second_done(self, d1):
        self.came(("bh+", d1), d1, 2, 0)
        self.came(("bh-", d1), d1, 2, 1)


def plane_steps(wires, whole, depth):
    pair = [PlaneGather(wires, whole, depth, core) for core in (0, 1)]
    steps = []
    for name in ("start_first", "start_second", "first_came"):
        steps += [functools.partial(getattr(g, name)) for g in pair]
    steps += [functools.partial(g.second_came, 0) for g in pair]
    steps += [g.first_done for g in pair]
    for d1 in (-1, 1, 2):
        steps += [functools.partial(g.second_came, d1) for g in pair]
    for d1 in (0, -1, 1, 2):
        steps += [functools.partial(g.second_done, d1) for g in pair]
    return steps


class TokenGather:
    def __init__(self, wires, whole):
        self.w, self.whole = wires, whole

    def rows(self, dx, other=False, part=None):
        c = self.w.at["c"]
        c = 1 - c if other else c
        start = (c * RING + self.w.step("x", dx)) * TOK
        half = TOK // 2
        if part is None:
            return self.whole.at[pl.ds(pl.multiple_of(start, 16), TOK)]
        return self.whole.at[pl.ds(pl.multiple_of(start + part * half, 16), half)]

    def start(self):
        own = self.rows(0)
        self.right = self.w.send(own, own, self.w.neighbour("x", 1))
        self.left = self.w.send(own, own, self.w.neighbour("x", -1))
        self.over = {0: self.w.send(own, own, self.w.partner())}

    def came(self):
        w = self.w
        for k, dx, part in ((self.right, -1, 0), (self.left, 1, 1)):
            block = self.rows(dx)
            w.arrived(k, block)
            piece = self.rows(dx, part=part)
            k2 = w.send(piece, piece, w.neighbour("x", -dx))
            if dx < 0:
                self.right2 = k2
            else:
                self.left2 = k2
            self.over[dx] = w.send(block, block, w.partner())

    def done(self):
        w = self.w
        w.arrived(self.right2, self.rows(2, part=0))
        w.arrived(self.left2, self.rows(2, part=1))
        block = self.rows(2)
        self.over[2] = w.send(block, block, w.partner())
        for dx in (0, -1, 1, 2):
            w.arrived(self.over[dx], self.rows(dx, other=True))


def gather_kernel(
    tok, gain, wq, wk, wv, wmq, wmk, wmv, wmg, wo,
    normed, w1, w2, w3,
    kv, send_sem, recv_sem, local_sem,
):
    w = Wires(send_sem, recv_sem)
    z, y, c = w.at["z"], w.at["y"], w.at["c"]
    barrier = pltpu.get_barrier_semaphore()
    greeted = [w.neighbour(a, d) for a in ("z", "y", "x") for d in (1, -1)] + [w.partner()]
    for device in greeted:
        pl.semaphore_signal(barrier, inc=1, device_id=device, device_id_type=MESH)

    kv[0] = jnp.concatenate([wk[:, :HD], wv[:, :HD]], axis=1)
    kv[1] = jnp.concatenate([wk[:, HD:], wv[:, HD:]], axis=1)
    values = tok[...].astype(jnp.float32)
    rescale = lax.rsqrt(jnp.mean(values * values, axis=-1, keepdims=True) + EPSILON)
    own_rows = pl.ds(pl.multiple_of((c * RING + w.at["x"]) * TOK, 16), TOK)
    normed[own_rows, :] = (values * rescale * gain[...]).astype(jnp.bfloat16)
    pl.semaphore_wait(barrier, len(greeted))

    block = (z * RING + y) * 2 + c
    r128 = pl.ds(pl.multiple_of(block * 128, 128), 128)
    r96 = pl.ds(pl.multiple_of(block * 96, 16), 96)

    def cut(ref, width):
        return lambda h: ref.at[:, pl.ds(pl.multiple_of(h * width, 128), width)]

    pieces = [
        (cut(wmk, 128), w1.at[r128, 0:128]),
        (cut(wmv, 128), w1.at[r128, 128:256]),
        (lambda h: kv.at[h], w1.at[r128, 256:384]),
        (cut(wq, 256), w2.at[r128, 0:256]),
        (cut(wmq, 128), w2.at[r128, 256:384]),
        (cut(wmg, 128), w2.at[r128, 384:512]),
        (cut(wo, 512), w3.at[r96, :]),
    ]
    local = []
    over = []
    for n, (half_of, dst) in enumerate(pieces):
        copy = pltpu.make_async_copy(half_of(c), dst, local_sem.at[n])
        copy.start()
        local.append(copy)
        over.append(w.send(half_of(1 - c), dst, w.partner()))

    theirs = (z * RING + y) * 2 + 1 - c
    t128 = pl.ds(pl.multiple_of(theirs * 128, 128), 128)
    t96 = pl.ds(pl.multiple_of(theirs * 96, 16), 96)
    landing = [
        w1.at[t128, 0:128], w1.at[t128, 128:256], w1.at[t128, 256:384],
        w2.at[t128, 0:256], w2.at[t128, 256:384], w2.at[t128, 384:512], w3.at[t96, :],
    ]
    tokens = TokenGather(w, normed)
    tokens.start()
    for n, copy in enumerate(local):
        copy.wait()
        w.arrived(over[n], landing[n])

    g1 = plane_steps(w, w1, 128)
    g2 = plane_steps(w, w2, 128)
    g3 = plane_steps(w, w3, 96)
    for step in g1[:8]:
        step()
    for step in g2[:4]:
        step()
    for step in g1[8:12]:
        step()
    tokens.came()
    for step in g1[12:]:
        step()
    for step in g3[:4]:
        step()
    for step in g2[4:12]:
        step()
    tokens.done()
    for step in g2[12:]:
        step()
    for step in g3[4:]:
        step()
    w.finish()


def gather_all(tok, gain, wq, wk, wv, wmq, wmk, wmv, wmg, wo):
    vmem = pl.BlockSpec(memory_space=pltpu.VMEM)
    bf = jnp.bfloat16
    return pl.pallas_call(
        gather_kernel,
        out_shape=[
            jax.ShapeDtypeStruct((ROWS, D), bf),
            jax.ShapeDtypeStruct((D, 384), bf),
            jax.ShapeDtypeStruct((D, 512), bf),
            jax.ShapeDtypeStruct((3072, 512), bf),
        ],
        in_specs=[vmem] * 10,
        out_specs=[vmem] * 4,
        scratch_shapes=[
            pltpu.VMEM((2, 128, 128), bf),
            pltpu.SemaphoreType.DMA((MAX_COPIES,)),
            pltpu.SemaphoreType.DMA((MAX_COPIES,)),
            pltpu.SemaphoreType.DMA((8,)),
        ],
        compiler_params=pltpu.CompilerParams(
            collective_id=0, has_side_effects=True, vmem_limit_bytes=60 * 1024 * 1024
        ),
        name="gather_all",
    )(tok, gain.reshape(1, D), wq, wk, wv, wmq, wmk, wmv, wmg, wo)


def passed_along(block, axis, distance):
    devices = range(lax.axis_size(axis))
    route = [(i - distance, i) for i in devices if i - distance in devices]
    return lax.ppermute(block, axis, route)


def nothing_yet(x, identity):
    return jax.tree.map(
        lambda a, e: jnp.broadcast_to(jnp.asarray(e, a.dtype), a.shape), x, identity
    )


def collected_together(x, axis):
    leaves = jax.tree.leaves(x)
    turns = sorted(range(len(leaves)), key=lambda k: -leaves[k].size)
    width = (1, *leaves[turns[0]].shape)[-1]
    lines = [
        jnp.pad(leaves[k].reshape(-1), (0, -leaves[k].size % width)).reshape(-1, width)
        for k in turns
    ]
    both, at, found = (lax.all_gather(jnp.concatenate(lines), axis), 0, {})
    for k, line in zip(turns, lines):
        section = both[:, at : at + len(line)].reshape(len(both), -1)
        found[k] = section[:, : leaves[k].size].reshape(-1, *leaves[k].shape)
        at += len(line)
    numbers = iter(range(len(leaves)))
    return jax.tree.map(lambda _: found[next(numbers)], x)


def entering(x, axes, combine, identity):
    before = start = nothing_yet(x, identity)
    total = x
    for axis in reversed(axes):
        length, mine = (lax.axis_size(axis), lax.axis_index(axis))
        pieces = collected_together(
            jax.tree.map(
                lambda part, kind: part.astype(kind),
                total,
                (jnp.bfloat16, jnp.bfloat16, jnp.bfloat16, jnp.bfloat16),
            ),
            axis,
        )
        inside, total = (start, start)
        for k in range(length):
            passed = k < mine
            total = combine(
                total, jax.tree.map(lambda part, own: part[k].astype(own.dtype), pieces, x)
            )
            inside = jax.tree.map(lambda new, old: jnp.where(passed, new, old), total, inside)
        before = combine(inside, before)
    return before


def from_everyone(x, axis):
    copies = jnp.broadcast_to(x, (lax.axis_size(axis), *x.shape))
    return lax.all_to_all(copies, axis, split_axis=0, concat_axis=0, tiled=True)


def joined_along(pieces, dim):
    pieces = jnp.moveaxis(pieces, 0, dim)
    shape = pieces.shape
    return pieces.reshape(*shape[:dim], shape[dim] * shape[dim + 1], *shape[dim + 2 :])


def advance(carried, key_block, value_block, in_block, cumulative):
    memory_state, normalizer, stabilizer = carried
    block_total = cumulative[:, -1]
    decays = block_total[:, None] - cumulative + in_block
    new_stabilizer = jnp.maximum(block_total + stabilizer, jnp.max(decays, axis=-1))
    weights = jnp.exp(decays - new_stabilizer[:, None])
    rescale = jnp.exp(block_total + stabilizer - new_stabilizer)
    new_state = rescale[:, None, None] * memory_state + jnp.einsum(
        "hsv,hsk->hvk", value_block * weights[:, :, None], key_block, precision=exact_precision
    )
    new_normalizer = rescale[:, None] * normalizer + jnp.einsum(
        "hs,hsk->hk", weights, key_block, precision=exact_precision
    )
    return (new_state, new_normalizer, new_stabilizer)


def block_step(carried, block_data):
    memory_state, normalizer, stabilizer = carried
    query_block, key_block, value_block, in_block, forget_block = block_data
    length = in_block.shape[-1]
    cumulative = jnp.cumsum(forget_block, axis=-1)
    causal = lax.broadcasted_iota(jnp.int32, (length, length), 0) >= lax.broadcasted_iota(
        jnp.int32, (length, length), 1
    )
    log_weight = jnp.where(
        causal[None], cumulative[:, :, None] - cumulative[:, None, :] + in_block[:, None, :], MASKED
    )
    row_level = jnp.maximum(cumulative + stabilizer[:, None], jnp.max(log_weight, axis=-1))
    carried_part = jnp.exp(cumulative + stabilizer[:, None] - row_level)
    affinity = jnp.einsum(
        "htd,hsd->hts", query_block, key_block, precision=exact_precision
    ) * jnp.exp(log_weight - row_level[:, :, None])
    numerator = carried_part[:, :, None] * jnp.einsum(
        "hvk,htk->htv", memory_state, query_block, precision=exact_precision
    ) + jnp.einsum("hts,hsv->htv", affinity, value_block, precision=exact_precision)
    denominator = carried_part * jnp.einsum(
        "hk,htk->ht", normalizer, query_block, precision=exact_precision
    ) + jnp.sum(affinity, axis=-1)
    recall = numerator / jnp.maximum(jnp.abs(denominator), jnp.exp(-row_level))[:, :, None]
    return (advance(carried, key_block, value_block, in_block, cumulative), recall)


def join_states(earlier, later):
    passed_one, state_one, normal_one, level_one = earlier
    passed_two, state_two, normal_two, level_two = later
    new_level = jnp.maximum(passed_two + level_one, level_two)
    weight_one = jnp.exp(passed_two + level_one - new_level)
    weight_two = jnp.exp(level_two - new_level)
    new_state = weight_one[:, None, None] * state_one + weight_two[:, None, None] * state_two
    new_normal = weight_one[:, None] * normal_one + weight_two[:, None] * normal_two
    return (passed_one + passed_two, new_state, new_normal, new_level)


def attend(query, key_rows, value_rows, sinks):
    row_count = query.shape[0]
    kv_local = key_rows.shape[1] // HD
    group_size = query.shape[1] // HD // kv_local
    block_count = row_count // WINDOW
    rim_key, rim_value = passed_along(
        (key_rows[row_count - WINDOW :], value_rows[row_count - WINDOW :]), PLANE, 1
    )
    padded_keys = jnp.concatenate([rim_key, key_rows], axis=0).reshape(
        block_count + 1, WINDOW, kv_local, HD
    )
    padded_values = jnp.concatenate([rim_value, value_rows], axis=0).reshape(
        block_count + 1, WINDOW, kv_local, HD
    )
    key_window = jnp.concatenate([padded_keys[:-1], padded_keys[1:]], axis=1)
    value_window = jnp.concatenate([padded_values[:-1], padded_values[1:]], axis=1)
    q_blocks = query.reshape(block_count, WINDOW, kv_local, group_size, HD)
    scores = jnp.einsum(
        "nqhgd,nkhd->nhgqk", q_blocks, key_window, preferred_element_type=jnp.float32
    ) * HD ** (-0.5)
    query_index = lax.broadcasted_iota(jnp.int32, (WINDOW, 2 * WINDOW), 0)
    key_index = lax.broadcasted_iota(jnp.int32, (WINDOW, 2 * WINDOW), 1)
    distance = query_index - key_index + WINDOW
    in_band = (distance >= 0) & (distance < WINDOW)
    block_index = lax.broadcasted_iota(jnp.int32, (block_count, WINDOW, 2 * WINDOW), 0)
    key_position = lax.axis_index(PLANE) * row_count + block_index * WINDOW - WINDOW + key_index[None]
    allowed = (in_band[None] & (key_position >= 0))[:, None, None]
    scores = jnp.where(allowed, scores, MASKED)
    sink_logit = sinks.reshape(1, kv_local, group_size, 1, 1)
    ceiling = jnp.maximum(jnp.max(scores, axis=-1, keepdims=True), sink_logit)
    weights = jnp.exp(scores - ceiling)
    partition = jnp.exp(sink_logit - ceiling) + jnp.sum(weights, axis=-1, keepdims=True)
    log_total = (
        (ceiling + jnp.log(partition))[..., 0]
        .transpose(0, 3, 1, 2)
        .reshape(row_count, kv_local * group_size)
    )
    probs = (weights / partition).astype(jnp.bfloat16)
    head_out = jnp.einsum(
        "nhgqk,nkhd->nqhgd", probs, value_window, preferred_element_type=jnp.float32
    )
    return (head_out.astype(jnp.bfloat16).reshape(row_count, kv_local * group_size * HD), log_total)


def memory(mem_query, mem_key, mem_value, mem_gate, gate_pre, forget_bias, forget_shift):
    row_count = mem_query.shape[0]
    head_count = forget_bias.shape[0]
    block_count = row_count // BLK
    sequence_total = row_count * lax.axis_size(PLANE)

    def blocks(array):
        return (
            array.astype(jnp.float32)
            .reshape(block_count, BLK, head_count, HD)
            .transpose(0, 2, 1, 3)
        )

    def gate_blocks(array):
        return array.reshape(block_count, BLK, head_count).transpose(0, 2, 1)

    log_in = gate_pre[:, 0, :] - 0.5 * math.log(sequence_total)
    log_forget = jax.nn.log_sigmoid(gate_pre[:, 1, :] + forget_bias) + forget_shift
    query_blocks = blocks(mem_query)
    key_blocks = blocks(mem_key) * HD ** (-0.5)
    value_blocks = blocks(mem_value)
    in_blocks = gate_blocks(log_in)
    forget_blocks = gate_blocks(log_forget)
    initial = (
        jnp.zeros((head_count, HD, HD), jnp.float32),
        jnp.zeros((head_count, HD), jnp.float32),
        jnp.full((head_count,), MASKED, jnp.float32),
    )

    def summarize(carried, block_data):
        key_block, value_block, in_block, forget_block = block_data
        return (
            advance(carried, key_block, value_block, in_block, jnp.cumsum(forget_block, axis=-1)),
            None,
        )

    summary, _ = lax.scan(summarize, initial, (key_blocks, value_blocks, in_blocks, forget_blocks))
    passed = jnp.sum(log_forget, axis=0)
    identity = (jnp.zeros((head_count,), jnp.float32), initial[0], initial[1], initial[2])
    incoming = entering((passed, summary[0], summary[1], summary[2]), PLANE, join_states, identity)
    _, recall = lax.scan(
        block_step,
        (incoming[1], incoming[2], incoming[3]),
        (query_blocks, key_blocks, value_blocks, in_blocks, forget_blocks),
    )
    recall = recall.transpose(0, 2, 1, 3).reshape(row_count, head_count * HD)
    return (recall * jax.nn.sigmoid(mem_gate.astype(jnp.float32))).astype(jnp.bfloat16)


def swapped(x):
    return lax.all_to_all(x, "c", split_axis=0, concat_axis=0, tiled=True)


def shards(
    tokens, norm_gain, w_query, w_key, w_value, w_mem_query, w_mem_key, w_mem_value, w_mem_gate,
    w_gates, sinks, forget_bias, forget_shift, w_out,
):
    c, x = lax.axis_index("c"), lax.axis_index("x")
    normed, w1, w2, w3 = gather_all(
        tokens, norm_gain, w_query, w_key, w_value, w_mem_query, w_mem_key, w_mem_value,
        w_mem_gate, w_out,
    )
    part1 = jnp.dot(normed, w1, preferred_element_type=jnp.float32).astype(jnp.bfloat16)
    part2 = jnp.dot(normed, w2, preferred_element_type=jnp.float32).astype(jnp.bfloat16)
    gates = lax.dynamic_slice_in_dim(w_gates, x * 4 + c * 2, 2, 2).reshape(D, 4)
    gate_pre = jnp.dot(normed, gates, preferred_element_type=jnp.float32).reshape(ROWS, 2, 2)
    shift = forget_shift.reshape(384, 2, 2).transpose(1, 0, 2).reshape(2 * 384, 2)
    shift = swapped(shift)
    attn_out, log_total = attend(
        part2[:, :256], part1[:, 256:320], part1[:, 320:384], lax.dynamic_slice_in_dim(sinks, c * 4, 4)
    )
    mem_out = memory(
        part2[:, 256:384], part1[:, :128], part1[:, 128:256], part2[:, 384:512],
        gate_pre, lax.dynamic_slice_in_dim(forget_bias, c * 2, 2), shift,
    )
    outs = from_everyone(jnp.concatenate([attn_out, mem_out], axis=1), ("x", "c"))
    outs = outs.reshape(8, ROWS, 384)
    joined = jnp.concatenate(
        [joined_along(outs[:, :, :256], 1), joined_along(outs[:, :, 256:], 1)], axis=1
    )
    mixed = jnp.dot(joined, w3, preferred_element_type=jnp.float32).astype(jnp.bfloat16)
    mixed = swapped(mixed).reshape(2, 384, 512).transpose(1, 0, 2).reshape(384, 1024)
    log_total = swapped(log_total).reshape(2, 384, 4).transpose(1, 0, 2).reshape(384, 8)
    return (mixed, log_total)


def solution(mesh):
    torus = Mesh(mesh.devices.reshape(4, 4, 2, mesh.shape["tp"]), ("z", "y", "c", "x"))
    sp = ("z", "y", "c")
    placed = (
        (P(("z", "y", "c", "x"), None), P())
        + (P(sp, "x"),) * 7
        + (P(), P("x"), P("x"), P(sp, "x"), P(sp, "x"))
    )
    return jax.shard_map(
        shards, mesh=torus, in_specs=placed, out_specs=(P(sp, "x"), P(sp, "x")), check_vma=False
    )
```

```python
import functools
import math

import jax
import jax.numpy as jnp
from jax import lax
from jax.experimental import pallas as pl
from jax.experimental.pallas import tpu as pltpu
from jax.sharding import Mesh
from jax.sharding import PartitionSpec as P

HD = 64
WINDOW = 128
BLK = 128
EPSILON = 1e-06
MASKED = -1e30
MESH = pl.DeviceIdType.MESH
RING = 4
TOK = 96
ROWS = 8 * TOK
D = 4096
PLANE = ("z", "y")
MAX_COPIES = 200
HALF = ROWS // 2
BLOCKS = ROWS // BLK
CHIPS = RING * RING


class Wires:
    def __init__(self, send_sem, recv_sem):
        self.send_sem, self.recv_sem = send_sem, recv_sem
        self.count = 0
        self.started = []
        z, y, c, x = (lax.axis_index(a) for a in ("z", "y", "c", "x"))
        self.at = {"z": z, "y": y, "c": c, "x": x}

    def moved(self, **new):
        where = dict(self.at)
        where.update(new)
        return (where["z"], where["y"], where["c"], where["x"])

    def step(self, axis, distance):
        return lax.rem(self.at[axis] + distance + RING, RING)

    def neighbour(self, axis, distance):
        return self.moved(**{axis: self.step(axis, distance)})

    def partner(self):
        return self.moved(c=1 - self.at["c"])

    def send(self, src, dst, device):
        k = self.count
        self.count += 1
        copy = pltpu.make_async_remote_copy(
            src_ref=src,
            dst_ref=dst,
            send_sem=self.send_sem.at[k],
            recv_sem=self.recv_sem.at[k],
            device_id=device,
            device_id_type=MESH,
        )
        copy.start()
        self.started.append(copy)
        return k

    def arrived(self, k, dst):
        pltpu.make_async_remote_copy(
            src_ref=dst,
            dst_ref=dst,
            send_sem=self.send_sem.at[k],
            recv_sem=self.recv_sem.at[k],
            device_id=self.partner(),
            device_id_type=MESH,
        ).wait_recv()

    def finish(self):
        for copy in self.started:
            copy.wait_send()


class PlaneGather:
    def __init__(self, wires, whole, depth, core):
        self.w, self.whole, self.depth, self.core = wires, whole, depth, core
        self.first, self.second = ("z", "y") if core == 0 else ("y", "z")
        self.sent = {}

    def rows(self, d1, d2, part=None):
        i1, i2 = self.w.step(self.first, d1), self.w.step(self.second, d2)
        z, y = (i1, i2) if self.core == 0 else (i2, i1)
        start = ((z * RING + y) * 2 + self.core) * self.depth
        half = self.depth // 2
        if part is None:
            return self.whole.at[pl.ds(pl.multiple_of(start, 16), self.depth)]
        return self.whole.at[pl.ds(pl.multiple_of(start + part * half, 16), half)]

    def go(self, name, d1, d2, axis, distance, part=None):
        block = self.rows(d1, d2, part)
        self.sent[name] = self.w.send(block, block, self.w.neighbour(axis, distance))

    def came(self, name, d1, d2, part=None):
        self.w.arrived(self.sent[name], self.rows(d1, d2, part))

    def second_round(self, d1):
        self.go(("b+", d1), d1, 0, self.second, 1)
        self.go(("b-", d1), d1, 0, self.second, -1)

    def start_first(self):
        self.go("a+", 0, 0, self.first, 1)
        self.go("a-", 0, 0, self.first, -1)

    def start_second(self):
        self.second_round(0)

    def first_came(self):
        self.came("a+", -1, 0)
        self.go("ah+", -1, 0, self.first, 1, 0)
        self.second_round(-1)
        self.came("a-", 1, 0)
        self.go("ah-", 1, 0, self.first, -1, 1)
        self.second_round(1)

    def second_came(self, d1):
        self.came(("b+", d1), d1, -1)
        self.go(("bh+", d1), d1, -1, self.second, 1, 0)
        self.came(("b-", d1), d1, 1)
        self.go(("bh-", d1), d1, 1, self.second, -1, 1)

    def first_done(self):
        self.came("ah+", 2, 0, 0)
        self.came("ah-", 2, 0, 1)
        self.second_round(2)

    def second_done(self, d1):
        self.came(("bh+", d1), d1, 2, 0)
        self.came(("bh-", d1), d1, 2, 1)


def plane_steps(wires, whole, depth):
    pair = [PlaneGather(wires, whole, depth, core) for core in (0, 1)]
    steps = []
    for name in ("start_first", "start_second", "first_came"):
        steps += [functools.partial(getattr(g, name)) for g in pair]
    steps += [functools.partial(g.second_came, 0) for g in pair]
    steps += [g.first_done for g in pair]
    for d1 in (-1, 1, 2):
        steps += [functools.partial(g.second_came, d1) for g in pair]
    for d1 in (0, -1, 1, 2):
        steps += [functools.partial(g.second_done, d1) for g in pair]
    return steps


class RowGather:
    def __init__(self, wires, region):
        self.w, self.region = wires, region

    def piece(self, dx, other=False, part=None):
        c = self.w.at["c"]
        return self.region(self.w.step("x", dx), 1 - c if other else c, part)

    def start(self):
        own, w = self.piece(0), self.w
        self.right = w.send(own, own, w.neighbour("x", 1))
        self.left = w.send(own, own, w.neighbour("x", -1))
        self.over = {0: w.send(own, own, w.partner())}

    def came(self):
        w = self.w
        block, half = self.piece(-1), self.piece(-1, part=0)
        w.arrived(self.right, block)
        self.right2 = w.send(half, half, w.neighbour("x", 1))
        self.over[-1] = w.send(block, block, w.partner())
        block, half = self.piece(1), self.piece(1, part=1)
        w.arrived(self.left, block)
        self.left2 = w.send(half, half, w.neighbour("x", -1))
        self.over[1] = w.send(block, block, w.partner())

    def done(self):
        w = self.w
        w.arrived(self.right2, self.piece(2, part=0))
        w.arrived(self.left2, self.piece(2, part=1))
        block = self.piece(2)
        self.over[2] = w.send(block, block, w.partner())

    def shared(self):
        for dx in (0, -1, 1, 2):
            self.w.arrived(self.over[dx], self.piece(dx, other=True))


def dot(a, b, dims=((1,), (0,))):
    return lax.dot_general(a, b, (dims, ((), ())), preferred_element_type=jnp.float32)


def by_head(lane, first, second):
    return jnp.where(lane < HD, first, second)


def joined(one, two):
    passed_one, state_one, normal_one, level_one = one
    passed_two, state_two, normal_two, level_two = two
    level = jnp.maximum(passed_two + level_one, level_two)
    weight_one = jnp.exp(passed_two + level_one - level)
    weight_two = jnp.exp(level_two - level)
    return (
        passed_one + passed_two,
        weight_one * state_one + weight_two * state_two,
        weight_one * normal_one + weight_two * normal_two,
        level,
    )


def put_state(ref, state):
    ref[0:HD, :] = state[1]
    ref[HD : HD + 1, :] = state[2]
    ref[HD + 1 : HD + 2, :] = state[3]
    ref[HD + 2 : HD + 3, :] = state[0]


def get_state(ref):
    return (
        ref[HD + 2 : HD + 3, :], ref[0:HD, :], ref[HD : HD + 1, :], ref[HD + 1 : HD + 2, :]
    )


def layer_kernel(
    tok, gain, wq, wk, wv, wmq, wmk, wmv, wmg, wo, wg, sinks, fbias, fshift,
    out, lt_out,
    tokv, rawkv, kvp, normed, w1, w2, w3, wgv, p1, gate, p2, kd, vd, sh, msgs, pre, outs, lt, ltin,
    stage, rows_in, rows_f, rows_sh, square, send_sem, recv_sem, local_sem,
):
    bf, f32 = jnp.bfloat16, jnp.float32
    w = Wires(send_sem, recv_sem)
    z, y, c, x = (w.at[a] for a in ("z", "y", "c", "x"))
    chip = z * RING + y
    barrier = pltpu.get_barrier_semaphore()
    plane = [(dz, dy) for dz in range(RING) for dy in range(RING) if dz or dy]
    greeted = [w.moved(z=w.step("z", dz), y=w.step("y", dy)) for dz, dy in plane]
    greeted += [w.neighbour("x", 1), w.neighbour("x", -1), w.partner()]
    for device in greeted:
        pl.semaphore_signal(barrier, inc=1, device_id=device, device_id_type=MESH)

    local = []

    def fetch(src, dst):
        copy = pltpu.make_async_copy(src, dst, local_sem.at[len(local)])
        copy.start()
        local.append(copy)
        return copy

    token_copy = fetch(tok, tokv)
    k_copy, v_copy = fetch(wk, rawkv.at[0]), fetch(wv, rawkv.at[1])

    def block_rows(ref, core, depth, cols):
        start = pl.multiple_of(((z * RING + y) * 2 + core) * depth, 16)
        return ref.at[pl.ds(start, depth), cols]

    def cut(ref, width):
        return lambda h: ref.at[:, pl.ds(pl.multiple_of(h * width, 128), width)]

    pieces = [
        (cut(wmk, 128), w1, 128, slice(0, 128)),
        (cut(wmv, 128), w1, 128, slice(128, 256)),
        (cut(wmq, 128), w1, 128, slice(256, 384)),
        (cut(wmg, 128), w1, 128, slice(384, 512)),
        (cut(wq, 256), w2, 128, slice(0, 256)),
        (lambda h: kvp.at[h], w2, 128, slice(256, 384)),
        (cut(wo, 512), w3, 96, slice(0, 512)),
    ]
    kept = [None] * len(pieces)
    for n, (half_of, dst, depth, cols) in enumerate(pieces):
        if n != 5:
            kept[n] = fetch(half_of(c), block_rows(dst, c, depth, cols))
    gate_copy = fetch(wg, wgv)

    k_copy.wait()
    v_copy.wait()
    kvp[0] = jnp.concatenate([rawkv[0, :, :HD], rawkv[1, :, :HD]], axis=1)
    kvp[1] = jnp.concatenate([rawkv[0, :, HD:], rawkv[1, :, HD:]], axis=1)
    sh[c] = fshift[...]
    token_copy.wait()
    first_row = (c * RING + x) * TOK

    def normalize(i, carry):
        values = tokv[pl.ds(pl.multiple_of(i * 16, 16), 16), :].astype(f32)
        rescale = lax.rsqrt(jnp.mean(values * values, axis=-1, keepdims=True) + EPSILON)
        normed[pl.ds(pl.multiple_of(first_row + i * 16, 16), 16), :] = (
            values * rescale * gain[...]
        ).astype(bf)
        return carry

    lax.fori_loop(0, TOK // 16, normalize, 0)
    kept[5] = fetch(kvp.at[c], block_rows(w2, c, 128, slice(256, 384)))
    pl.semaphore_wait(barrier, len(greeted))

    over = [
        w.send(half_of(1 - c), block_rows(dst, c, depth, cols), w.partner())
        for half_of, dst, depth, cols in pieces
    ]

    def token_rows(xi, ci, part):
        start = (ci * RING + xi) * TOK
        if part is None:
            return normed.at[pl.ds(pl.multiple_of(start, 16), TOK)]
        return normed.at[pl.ds(pl.multiple_of(start + part * (TOK // 2), 16), TOK // 2)]

    tokens = RowGather(w, token_rows)
    tokens.start()
    shift_over = w.send(fshift, sh.at[c], w.partner())

    def ready(first, last):
        for n in range(first, last):
            _, dst, depth, cols = pieces[n]
            kept[n].wait()
            w.arrived(over[n], block_rows(dst, 1 - c, depth, cols))

    groups = [plane_steps(w, w1, 128), plane_steps(w, w2, 128), plane_steps(w, w3, 96)]
    groups[0].insert(0, lambda: ready(0, 4))
    groups[1].insert(0, lambda: ready(4, 6))
    groups[2].insert(0, lambda: ready(6, 7))
    at = [0, 0, 0]

    def pump(group, upto):
        while at[group] < min(upto, len(groups[group])):
            groups[group][at[group]]()
            at[group] += 1

    def first_projection(i, carry):
        rows = pl.ds(pl.multiple_of(i * HALF, HALF), HALF)
        p1[rows, :] = dot(normed[rows, :], w1[...]).astype(bf)
        gate[rows, :] = dot(normed[rows, :], wgv[...])
        return carry

    def second_projection(i, carry):
        rows = pl.ds(pl.multiple_of(i * HALF, HALF), HALF)
        both = dot(normed[rows, :], w2[...])
        p2[rows, :] = both[:, :256].astype(bf)
        kv = both[:, 256:]
        turned = pltpu.roll(kv, HD, 1)
        lane = lax.broadcasted_iota(jnp.int32, kv.shape, 1)
        after = pl.ds(pl.multiple_of(i * HALF + WINDOW, WINDOW), HALF)
        kd[after, :] = by_head(lane, kv, turned).astype(bf)
        vd[after, :] = by_head(lane, turned, kv).astype(bf)
        return carry

    lane1 = lax.broadcasted_iota(jnp.int32, (1, 128), 1)
    lane = lax.broadcasted_iota(jnp.int32, (128, 128), 1)
    row = lax.broadcasted_iota(jnp.int32, (128, 128), 0)
    scale = HD ** (-0.5)
    feature_attn = 512 * x + 256 * c
    feature_mem = 2048 + 256 * x + 128 * c

    def memory_gates():
        rows_in[...] = jnp.zeros_like(rows_in)
        rows_f[...] = jnp.zeros_like(rows_f)
        rows_sh[...] = jnp.zeros_like(rows_sh)
        square[...] = jnp.zeros_like(square)
        w.arrived(shift_over, sh.at[1 - c])
        for b in range(BLOCKS):
            turned = jnp.transpose(gate[b * BLK : (b + 1) * BLK, :])
            rows_in[2 * b : 2 * b + 2, :] = turned[0:2]
            rows_f[2 * b : 2 * b + 2, :] = turned[2:4]
            q, at_col = b // 3, (b % 3) * BLK
            both = sh[q, :, at_col : at_col + BLK]
            rows_sh[2 * b : 2 * b + 2, :] = jnp.where(c == 0, both[0:2], both[2:4])
        head = lax.broadcasted_iota(jnp.int32, (16, 128), 0) % 2
        pre_forget = rows_f[...] + jnp.where(head == 0, fbias[2 * c], fbias[2 * c + 1])
        log_forget = (
            jnp.minimum(pre_forget, 0.0)
            - jnp.log1p(jnp.exp(-jnp.abs(pre_forget)))
            + rows_sh[...]
        )
        upto = (row <= lane).astype(f32)
        cumulative = jnp.dot(
            log_forget, upto, precision=lax.Precision.HIGHEST, preferred_element_type=f32
        )
        a = rows_in[...] - 0.5 * math.log(CHIPS * ROWS) - cumulative
        top = jnp.max(a, axis=1, keepdims=True)
        weights = jnp.exp(a - top)
        square[0:16, :] = cumulative
        square[16:32, :] = weights
        rows_in[...] = a
        rows_f[...] = weights
        columns = jnp.transpose(square[...])
        square[...] = columns
        total = cumulative[:, 127:128]
        state = (
            jnp.zeros((1, 128), f32), jnp.zeros((HD, 128), f32), jnp.zeros((1, 128), f32),
            jnp.full((1, 128), MASKED, f32),
        )
        for b in range(BLOCKS):
            put_state(pre.at[b], state)
            rows = slice(b * BLK, (b + 1) * BLK)
            keys, values = p1[rows, 0:128], p1[rows, 128:256]
            spread = by_head(
                lane, columns[:, 16 + 2 * b : 17 + 2 * b], columns[:, 17 + 2 * b : 18 + 2 * b]
            )
            weighted = (values.astype(f32) * spread).astype(bf)
            both = dot(keys, weighted, ((0,), (0,)))
            outer = by_head(lane[:HD], both[:HD], both[HD:]) * scale
            sums = dot(weights.astype(bf), keys)
            normal = by_head(lane1, sums[2 * b : 2 * b + 1], sums[2 * b + 1 : 2 * b + 2]) * scale
            passed = by_head(lane1, total[2 * b : 2 * b + 1], total[2 * b + 1 : 2 * b + 2])
            peak = by_head(lane1, top[2 * b : 2 * b + 1], top[2 * b + 1 : 2 * b + 2])
            state = joined(state, (passed, outer, normal, passed + peak))
        put_state(msgs.at[chip], state)
        msgs[chip, HD + 3 :, :] = jnp.zeros((5, 128), f32)

    told = []

    def tell_state():
        mine = msgs.at[chip]
        for dz, dy in plane:
            device = w.moved(z=w.step("z", dz), y=w.step("y", dy))
            told.append(w.send(mine, mine, device))

    def incoming_state():
        for k, (dz, dy) in zip(told, plane):
            w.arrived(k, msgs.at[w.step("z", -dz) * RING + w.step("y", -dy)])
        state = (
            jnp.zeros((1, 128), f32), jnp.zeros((HD, 128), f32), jnp.zeros((1, 128), f32),
            jnp.full((1, 128), MASKED, f32),
        )
        for other in range(CHIPS - 1):
            after = joined(state, get_state(msgs.at[other]))
            state = tuple(jnp.where(other < chip, new, old) for new, old in zip(after, state))
        return state

    def memory_block(b, incoming):
        rows = slice(b * BLK, (b + 1) * BLK)
        _, state, normal, level = joined(incoming, get_state(pre.at[b]))
        keys, values, query = p1[rows, 0:128], p1[rows, 128:256], p1[rows, 256:384]
        whole = jnp.concatenate(
            [jnp.where(lane[:HD] < HD, state, 0.0), jnp.where(lane[:HD] >= HD, state, 0.0)], axis=0
        ).astype(bf)
        carried_num = dot(query, whole)
        with_normal = query.astype(f32) * normal
        recalled = []
        for h in range(2):
            mine = (lane < HD) if h == 0 else (lane >= HD)
            r = 2 * b + h
            a = jnp.where(row >= lane, rows_in[r : r + 1, :], MASKED)
            stab = level[:, 64 * h : 64 * h + 1]
            high = jnp.maximum(jnp.max(a, axis=1, keepdims=True), stab)
            carried = jnp.exp(stab - high)
            query_h = jnp.where(mine, query, jnp.zeros_like(query))
            affinity = dot(query_h, keys, ((1,), (1,))) * scale * jnp.exp(a - high)
            den = carried * jnp.sum(jnp.where(mine, with_normal, 0.0), axis=1, keepdims=True)
            den = den + jnp.sum(affinity, axis=1, keepdims=True)
            num = carried * carried_num + dot(affinity.astype(bf), values)
            floor = jnp.exp(-(square[:, r : r + 1] + high))
            recalled.append(num / jnp.maximum(jnp.abs(den), floor))
        recall = by_head(lane, recalled[0], recalled[1])
        opened = 1.0 / (1.0 + jnp.exp(-p1[rows, 384:512].astype(f32)))
        outs[rows, pl.ds(pl.multiple_of(feature_mem, 128), 128)] = (recall * opened).astype(bf)

    def attention(first, last):
        query_index = lax.broadcasted_iota(jnp.int32, (WINDOW, 2 * WINDOW), 0)
        key_index = lax.broadcasted_iota(jnp.int32, (WINDOW, 2 * WINDOW), 1)
        distance = query_index - key_index + WINDOW
        in_band = (distance >= 0) & (distance < WINDOW)

        def one_block(b, carry):
            rows = pl.ds(pl.multiple_of(b * WINDOW, WINDOW), WINDOW)
            window = pl.ds(pl.multiple_of(b * WINDOW, WINDOW), 2 * WINDOW)
            keys, values = kd[window, :], vd[window, :]
            allowed = in_band & ((chip * BLOCKS + b) * WINDOW - WINDOW + key_index >= 0)
            logs = jnp.zeros((WINDOW, 128), f32)
            for pair in range(2):
                query = p2[rows, pair * 128 : (pair + 1) * 128]
                results = []
                for half in range(2):
                    h = 2 * pair + half
                    mine = (lane < HD) if half == 0 else (lane >= HD)
                    query_h = jnp.where(mine, query, jnp.zeros_like(query))
                    scores = dot(query_h, keys, ((1,), (1,))) * scale
                    scores = jnp.where(allowed, scores, MASKED)
                    sink = sinks[4 * c + h]
                    ceiling = jnp.maximum(jnp.max(scores, axis=1, keepdims=True), sink)
                    weights = jnp.exp(scores - ceiling)
                    part = jnp.exp(sink - ceiling) + jnp.sum(weights, axis=1, keepdims=True)
                    logs = jnp.where(lane == 4 * c + h, ceiling + jnp.log(part), logs)
                    probs = (weights * (1.0 / part)).astype(bf)
                    results.append(dot(probs, values))
                col = pl.multiple_of(feature_attn + pair * 128, 128)
                outs[rows, pl.ds(col, 128)] = by_head(lane, results[0], results[1]).astype(bf)
            lt[rows, :] = logs
            return carry

        lax.fori_loop(first, last, one_block, 0)

    def out_region(start, base, stride, width):
        def region(xi, ci, part):
            count = HALF if part is None else HALF // 2
            first = start if part is None else start + part * (HALF // 2)
            col = pl.multiple_of(base + 2 * stride * xi + stride * ci, 128)
            return outs.at[pl.ds(first, count), pl.ds(col, width)]

        return RowGather(w, region)

    mem_out = [out_region(r, 2048, 128, 128) for r in (0, HALF)]
    attn_out = [out_region(r, 0, 256, 256) for r in (0, HALF)]

    pump(0, 9)
    pump(1, 5)
    pump(0, 17)
    tokens.came()
    pump(0, 99)
    pump(2, 5)
    pump(1, 9)
    tokens.done()
    tokens.shared()
    gate_copy.wait()
    lax.fori_loop(0, 2, first_projection, 0)
    pump(1, 11)
    memory_gates()
    tell_state()
    pump(1, 17)
    pump(2, 9)
    incoming = incoming_state()
    for b in range(3):
        memory_block(b, incoming)
    mem_out[0].start()
    pump(1, 99)
    for b in range(3, 6):
        memory_block(b, incoming)
    mem_out[1].start()
    lax.fori_loop(0, 2, second_projection, 0)
    next_chip = w.moved(z=lax.rem(z + (y + 1) // RING, RING), y=w.step("y", 1))
    rim = [
        w.send(ref.at[ROWS : ROWS + WINDOW], ref.at[0:WINDOW], next_chip) for ref in (kd, vd)
    ]
    mem_out[0].came()
    pump(2, 13)
    w.arrived(rim[0], kd.at[0:WINDOW])
    w.arrived(rim[1], vd.at[0:WINDOW])
    attention(0, 3)
    attn_out[0].start()
    mem_out[1].came()
    pump(2, 17)
    attention(3, 6)
    attn_out[1].start()
    theirs = pl.ds(pl.multiple_of((1 - c) * HALF, HALF), HALF)
    ours = pl.ds(pl.multiple_of(c * HALF, HALF), HALF)
    log_over = w.send(lt.at[theirs], ltin, w.partner())
    for g in mem_out:
        g.done()
    pump(2, 99)
    for g in attn_out:
        g.came()
    for g in attn_out:
        g.done()
    for g in mem_out + attn_out:
        g.shared()
    stage[...] = dot(outs[theirs, :], w3[...]).astype(bf)
    mixed_over = w.send(stage, out.at[:, pl.ds(pl.multiple_of(c * 512, 512), 512)], w.partner())
    out[:, pl.ds(pl.multiple_of(c * 512, 512), 512)] = dot(outs[ours, :], w3[...]).astype(bf)
    w.arrived(log_over, ltin)
    lt_out[...] = (lt[ours, :] + ltin[...])[:, :8]
    w.arrived(mixed_over, out.at[:, pl.ds(pl.multiple_of((1 - c) * 512, 512), 512)])
    w.finish()


def shards(
    tokens, norm_gain, w_query, w_key, w_value, w_mem_query, w_mem_key, w_mem_value, w_mem_gate,
    w_gates, sinks, forget_bias, forget_shift, w_out,
):
    c, x = lax.axis_index("c"), lax.axis_index("x")
    gates = lax.dynamic_slice_in_dim(w_gates, x * 4 + c * 2, 2, 2).reshape(D, 4)
    gates = jnp.pad(gates, ((0, 0), (0, 124)))
    vmem = pl.BlockSpec(memory_space=pltpu.VMEM)
    smem = pl.BlockSpec(memory_space=pltpu.SMEM)
    anywhere = pl.BlockSpec(memory_space=pl.ANY)
    bf, f32 = jnp.bfloat16, jnp.float32
    mixed, log_total = pl.pallas_call(
        layer_kernel,
        out_shape=[
            jax.ShapeDtypeStruct((HALF, 1024), bf),
            jax.ShapeDtypeStruct((HALF, 8), f32),
        ],
        in_specs=[anywhere, vmem] + [anywhere] * 9 + [smem, smem, vmem],
        out_specs=[vmem, vmem],
        scratch_shapes=[
            pltpu.VMEM((TOK, D), bf),
            pltpu.VMEM((2, 128, 128), bf),
            pltpu.VMEM((2, 128, 128), bf),
            pltpu.VMEM((ROWS, D), bf),
            pltpu.VMEM((D, 512), bf),
            pltpu.VMEM((D, 384), bf),
            pltpu.VMEM((3072, 512), bf),
            pltpu.VMEM((D, 128), bf),
            pltpu.VMEM((ROWS, 512), bf),
            pltpu.VMEM((ROWS, 128), f32),
            pltpu.VMEM((ROWS, 256), bf),
            pltpu.VMEM((ROWS + WINDOW, 128), bf),
            pltpu.VMEM((ROWS + WINDOW, 128), bf),
            pltpu.VMEM((2, 4, HALF), f32),
            pltpu.VMEM((CHIPS, HD + 8, 128), f32),
            pltpu.VMEM((BLOCKS, HD + 8, 128), f32),
            pltpu.VMEM((ROWS, 3072), bf),
            pltpu.VMEM((ROWS, 128), f32),
            pltpu.VMEM((HALF, 128), f32),
            pltpu.VMEM((HALF, 512), bf),
            pltpu.VMEM((16, 128), f32),
            pltpu.VMEM((16, 128), f32),
            pltpu.VMEM((16, 128), f32),
            pltpu.VMEM((128, 128), f32),
            pltpu.SemaphoreType.DMA((MAX_COPIES,)),
            pltpu.SemaphoreType.DMA((MAX_COPIES,)),
            pltpu.SemaphoreType.DMA((16,)),
        ],
        compiler_params=pltpu.CompilerParams(
            collective_id=0, has_side_effects=True, vmem_limit_bytes=60 * 1024 * 1024
        ),
        name="layer",
    )(
        tokens, norm_gain.reshape(1, D), w_query, w_key, w_value, w_mem_query, w_mem_key,
        w_mem_value, w_mem_gate, w_out, gates, sinks, forget_bias, forget_shift.T,
    )
    return (mixed, log_total)


def solution(mesh):
    torus = Mesh(mesh.devices.reshape(4, 4, 2, mesh.shape["tp"]), ("z", "y", "c", "x"))
    sp = ("z", "y", "c")
    placed = (
        (P(("z", "y", "c", "x"), None), P())
        + (P(sp, "x"),) * 7
        + (P(), P("x"), P("x"), P(sp, "x"), P(sp, "x"))
    )
    return jax.shard_map(
        shards, mesh=torus, in_specs=placed, out_specs=(P(sp, "x"), P(sp, "x")), check_vma=False
    )
```

```python
import functools
import math
import types

import jax
import jax.numpy as jnp
from jax import lax
from jax.experimental import pallas as pl
from jax.experimental.pallas import tpu as pltpu
from jax.sharding import Mesh
from jax.sharding import PartitionSpec as P

HD = 64
WINDOW = 128
BLK = 128
EPSILON = 1e-06
MASKED = -1e30
MESH = pl.DeviceIdType.MESH
RING = 4
TOK = 96
ROWS = 8 * TOK
D = 4096
PLANE = ("z", "y")
MAX_COPIES = 208
HALF = ROWS // 2
BLOCKS = ROWS // BLK
CHIPS = RING * RING


class Wires:
    def __init__(self, send_sem, recv_sem):
        self.send_sem, self.recv_sem = send_sem, recv_sem
        self.count = 0
        self.started = []
        z, y, c, x = (lax.axis_index(a) for a in ("z", "y", "c", "x"))
        self.at = {"z": z, "y": y, "c": c, "x": x}
        self.steps = {}

    def moved(self, **new):
        where = dict(self.at)
        where.update(new)
        return (where["z"], where["y"], where["c"], where["x"])

    def step(self, axis, distance):
        if distance % RING == 0:
            return self.at[axis]
        key = (axis, distance % RING)
        if key not in self.steps:
            self.steps[key] = lax.rem(self.at[axis] + key[1], RING)
        return self.steps[key]

    def neighbour(self, axis, distance):
        return self.moved(**{axis: self.step(axis, distance)})

    def partner(self):
        return self.moved(c=1 - self.at["c"])

    def send(self, src, dst, device):
        k = self.count
        self.count += 1
        copy = pltpu.make_async_remote_copy(
            src_ref=src,
            dst_ref=dst,
            send_sem=self.send_sem.at[k],
            recv_sem=self.recv_sem.at[k],
            device_id=device,
            device_id_type=MESH,
        )
        copy.start()
        self.started.append(copy)
        return k

    def arrived(self, k, dst):
        pltpu.make_async_remote_copy(
            src_ref=dst,
            dst_ref=dst,
            send_sem=self.send_sem.at[k],
            recv_sem=self.recv_sem.at[k],
            device_id=self.partner(),
            device_id_type=MESH,
        ).wait_recv()

    def finish(self):
        for copy in self.started:
            copy.wait_send()


class PlaneGather:
    def __init__(self, wires, whole, depth, core):
        self.w, self.whole, self.depth, self.core = wires, whole, depth, core
        self.sent = {}

    def mixed(self, axis, one, two):
        first, second = (one, two) if axis == "z" else (two, one)
        return self.w.step(axis, first) * (1 - self.core) + self.w.step(axis, second) * self.core

    def rows(self, d1, d2, part=None):
        z, y = self.mixed("z", d1, d2), self.mixed("y", d1, d2)
        start = ((z * RING + y) * 2 + self.core) * self.depth
        half = self.depth // 2
        if part is None:
            return self.whole.at[pl.ds(pl.multiple_of(start, 16), self.depth)]
        return self.whole.at[pl.ds(pl.multiple_of(start + part * half, 16), half)]

    def go(self, name, d1, d2, first, distance, part=None):
        block = self.rows(d1, d2, part)
        one, two = (distance, 0) if first else (0, distance)
        device = self.w.moved(z=self.mixed("z", one, two), y=self.mixed("y", one, two))
        self.sent[name] = self.w.send(block, block, device)

    def came(self, name, d1, d2, part=None):
        self.w.arrived(self.sent[name], self.rows(d1, d2, part))

    def second_round(self, d1):
        self.go(("b", 1, d1), d1, 0, False, 1)
        self.go(("b", -1, d1), d1, 0, False, -1)

    def start(self):
        self.go(("a", 1), 0, 0, True, 1)
        self.go(("a", -1), 0, 0, True, -1)
        self.second_round(0)

    def first_came(self, side):
        self.came(("a", side), -side, 0)
        self.go(("ah", side), -side, 0, True, side, 0 if side > 0 else 1)
        self.second_round(-side)

    def second_came(self, d1, side):
        self.came(("b", side, d1), d1, -side)
        self.go(("bh", side, d1), d1, -side, False, side, 0 if side > 0 else 1)

    def first_done(self, side):
        self.came(("ah", side), 2, 0, 0 if side > 0 else 1)
        if side < 0:
            self.second_round(2)

    def second_done(self, d1, side):
        self.came(("bh", side, d1), d1, 2, 0 if side > 0 else 1)


def plane_steps(wires, whole, depth, own_ready, other_ready):
    c = wires.at["c"]
    pair = [PlaneGather(wires, whole, depth, core) for core in (c, 1 - c)]
    both = [(g, side) for side in (1, -1) for g in pair]
    steps = [own_ready, pair[0].start, other_ready, pair[1].start]
    steps += [functools.partial(g.first_came, side) for g, side in both]
    steps += [functools.partial(g.second_came, 0, side) for g, side in both]
    steps += [functools.partial(g.first_done, side) for g, side in both]
    for d1 in (-1, 1, 2):
        steps += [functools.partial(g.second_came, d1, side) for g, side in both]
    for d1 in (0, -1, 1, 2):
        steps += [functools.partial(g.second_done, d1, side) for g, side in both]
    return steps


class RowGather:
    def __init__(self, wires, region):
        self.w, self.region = wires, region

    def piece(self, dx, other=False, part=None):
        c = self.w.at["c"]
        return self.region(self.w.step("x", dx), 1 - c if other else c, part)

    def start(self):
        own, w = self.piece(0), self.w
        self.right = w.send(own, own, w.neighbour("x", 1))
        self.left = w.send(own, own, w.neighbour("x", -1))
        self.over = {0: w.send(own, own, w.partner())}
        self.again = {}

    def came(self, side):
        w, part = self.w, 0 if side > 0 else 1
        block, half = self.piece(-side), self.piece(-side, part=part)
        w.arrived(self.right if side > 0 else self.left, block)
        self.again[side] = w.send(half, half, w.neighbour("x", side))
        self.over[-side] = w.send(block, block, w.partner())

    def done(self, side):
        w = self.w
        w.arrived(self.again[side], self.piece(2, part=0 if side > 0 else 1))
        if side < 0:
            block = self.piece(2)
            self.over[2] = w.send(block, block, w.partner())

    def shared(self, dx):
        self.w.arrived(self.over[dx], self.piece(dx, other=True))


def dot(a, b, dims=((1,), (0,))):
    return lax.dot_general(a, b, (dims, ((), ())), preferred_element_type=jnp.float32)


def by_head(lane, first, second):
    return jnp.where(lane < HD, first, second)


def joined(one, two):
    passed_one, state_one, normal_one, level_one = one
    passed_two, state_two, normal_two, level_two = two
    level = jnp.maximum(passed_two + level_one, level_two)
    weight_one = jnp.exp(passed_two + level_one - level)
    weight_two = jnp.exp(level_two - level)
    return (
        passed_one + passed_two,
        weight_one * state_one + weight_two * state_two,
        weight_one * normal_one + weight_two * normal_two,
        level,
    )


def put_state(ref, state):
    ref[0:HD, :] = state[1]
    ref[HD : HD + 1, :] = state[2]
    ref[HD + 1 : HD + 2, :] = state[3]
    ref[HD + 2 : HD + 3, :] = state[0]


def get_state(ref):
    return (
        ref[HD + 2 : HD + 3, :], ref[0:HD, :], ref[HD : HD + 1, :], ref[HD + 1 : HD + 2, :]
    )


def layer_kernel(
    tok, gain, wq, wk, wv, wmq, wmk, wmv, wmg, wo, wg, sinks, fbias, fshift,
    out, lt_out,
    tokv, rawkv, kvp, normed, w1, w2, w3, wgv, p1, gate, p2, kd, vd, sh, msgs, pre, outs, lt, ltin,
    stage, total, turned, small, rows_in, rows_f, rows_sh, square, send_sem, recv_sem, local_sem,
):
    bf, f32 = jnp.bfloat16, jnp.float32
    w = Wires(send_sem, recv_sem)
    z, y, c, x = (w.at[a] for a in ("z", "y", "c", "x"))
    chip = z * RING + y
    barrier = pltpu.get_barrier_semaphore()
    plane = [(dz, dy) for dz in range(RING) for dy in range(RING) if dz or dy]
    greeted = [w.neighbour(axis, d) for axis in ("z", "y", "x") for d in (1, -1)]
    greeted.append(w.partner())
    for device in greeted:
        pl.semaphore_signal(barrier, inc=1, device_id=device, device_id_type=MESH)

    local = []

    def fetch(src, dst):
        copy = pltpu.make_async_copy(src, dst, local_sem.at[len(local)])
        copy.start()
        local.append(copy)
        return copy

    k_copy, v_copy = fetch(wk, rawkv.at[0]), fetch(wv, rawkv.at[1])
    token_copy = fetch(tok, tokv)

    def block_rows(ref, core, depth, cols):
        start = pl.multiple_of(((z * RING + y) * 2 + core) * depth, 16)
        return ref.at[pl.ds(start, depth), cols]

    def cut(ref, width):
        return lambda h: ref.at[:, pl.ds(pl.multiple_of(h * width, 128), width)]

    pieces = [
        (cut(wq, 256), w1, 128, slice(0, 256)),
        (lambda h: kvp.at[h], w1, 128, slice(256, 384)),
        (cut(wmk, 128), w1, 128, slice(384, 512)),
        (cut(wmv, 128), w1, 128, slice(512, 640)),
        (cut(wmq, 128), w2, 128, slice(0, 128)),
        (cut(wmg, 128), w2, 128, slice(128, 256)),
        (cut(wo, 512), w3, 96, slice(0, 512)),
    ]
    kept = [None] * len(pieces)
    for n, (half_of, dst, depth, cols) in enumerate(pieces):
        if n != 1:
            kept[n] = fetch(half_of(c), block_rows(dst, c, depth, cols))
    gate_copy = fetch(wg, wgv)

    k_copy.wait()
    v_copy.wait()
    kvp[0] = jnp.concatenate([rawkv[0, :, :HD], rawkv[1, :, :HD]], axis=1)
    kvp[1] = jnp.concatenate([rawkv[0, :, HD:], rawkv[1, :, HD:]], axis=1)
    sh[c] = fshift[...]
    kept[1] = fetch(kvp.at[c], block_rows(w1, c, 128, slice(256, 384)))
    pl.semaphore_wait(barrier, len(greeted))

    over = [
        w.send(half_of(1 - c), block_rows(dst, c, depth, cols), w.partner())
        for half_of, dst, depth, cols in pieces
    ]

    def token_rows(xi, ci, part):
        start = (ci * RING + xi) * TOK
        if part is None:
            return normed.at[pl.ds(pl.multiple_of(start, 16), TOK)]
        return normed.at[pl.ds(pl.multiple_of(start + part * (TOK // 2), 16), TOK // 2)]

    tokens = RowGather(w, token_rows)
    first_row = (c * RING + x) * TOK

    def normalize(i, carry):
        values = tokv[pl.ds(pl.multiple_of(i * 16, 16), 16), :].astype(f32)
        rescale = lax.rsqrt(jnp.mean(values * values, axis=-1, keepdims=True) + EPSILON)
        normed[pl.ds(pl.multiple_of(first_row + i * 16, 16), 16), :] = (
            values * rescale * gain[...]
        ).astype(bf)
        return carry

    shift_over = w.send(fshift, sh.at[c], w.partner())

    def own_ready(first, last):
        for n in range(first, last):
            kept[n].wait()

    def other_ready(first, last):
        for n in range(first, last):
            _, dst, depth, cols = pieces[n]
            w.arrived(over[n], block_rows(dst, 1 - c, depth, cols))

    groups = [
        plane_steps(
            w, whole, depth,
            functools.partial(own_ready, *span), functools.partial(other_ready, *span),
        )
        for whole, depth, span in ((w1, 128, (0, 4)), (w2, 128, (4, 6)), (w3, 96, (6, 7)))
    ]
    at = [0, 0, 0]

    def pump(group, upto):
        while at[group] < min(upto, len(groups[group])):
            groups[group][at[group]]()
            at[group] += 1

    def first_projection(i):
        rows = slice(i * HALF, (i + 1) * HALF)
        both = dot(normed[rows, :], w1[...])
        p2[rows, :] = both[:, :256].astype(bf)
        kv = both[:, 256:384]
        turned_kv = pltpu.roll(kv, HD, 1)
        lane = lax.broadcasted_iota(jnp.int32, kv.shape, 1)
        after = slice(i * HALF + WINDOW, (i + 1) * HALF + WINDOW)
        kd[after, :] = by_head(lane, kv, turned_kv).astype(bf)
        vd[after, :] = by_head(lane, turned_kv, kv).astype(bf)
        p1[rows, 0:256] = both[:, 384:].astype(bf)
        gate[rows, 0:32] = dot(normed[rows, :], wgv[...], ((1,), (1,)))

    def second_projection(i):
        rows = slice(i * HALF, (i + 1) * HALF)
        p1[rows, 256:512] = dot(normed[rows, :], w2[...]).astype(bf)

    lane1 = lax.broadcasted_iota(jnp.int32, (1, 128), 1)
    lane = lax.broadcasted_iota(jnp.int32, (128, 128), 1)
    row = lax.broadcasted_iota(jnp.int32, (128, 128), 0)
    scale = HD ** (-0.5)
    feature_attn = 512 * x + 256 * c
    feature_mem = 2048 + 256 * x + 128 * c

    def memory_gates():
        rows_in[...] = jnp.zeros_like(rows_in)
        rows_f[...] = jnp.zeros_like(rows_f)
        rows_sh[...] = jnp.zeros_like(rows_sh)
        gate[:, 32:] = jnp.zeros((ROWS, 96), f32)
        square[...] = jnp.zeros_like(square)
        w.arrived(shift_over, sh.at[1 - c])
        for b in range(BLOCKS):
            turned[...] = jnp.transpose(gate[b * BLK : (b + 1) * BLK, :])
            for h in range(2):
                own = 4 * x + 2 * c + h
                rows_in[2 * b + h : 2 * b + h + 1, :] = turned[pl.ds(own, 1), :]
                rows_f[2 * b + h : 2 * b + h + 1, :] = turned[pl.ds(16 + own, 1), :]
            q, at_col = b // 3, (b % 3) * BLK
            both = sh[q, :, at_col : at_col + BLK]
            rows_sh[2 * b : 2 * b + 2, :] = jnp.where(c == 0, both[0:2], both[2:4])
        head = lax.broadcasted_iota(jnp.int32, (16, 128), 0) % 2
        pre_forget = rows_f[...] + jnp.where(head == 0, fbias[2 * c], fbias[2 * c + 1])
        log_forget = (
            jnp.minimum(pre_forget, 0.0)
            - jnp.log1p(jnp.exp(-jnp.abs(pre_forget)))
            + rows_sh[...]
        )
        upto = (row <= lane).astype(f32)
        cumulative = jnp.dot(
            log_forget, upto, precision=lax.Precision.HIGHEST, preferred_element_type=f32
        )
        a = rows_in[...] - 0.5 * math.log(CHIPS * ROWS) - cumulative
        top = jnp.max(a, axis=1, keepdims=True)
        weights = jnp.exp(a - top)
        square[0:16, :] = cumulative
        square[16:32, :] = weights
        rows_in[...] = a
        rows_f[...] = weights
        columns = jnp.transpose(square[...])
        square[...] = columns
        ends = cumulative[:, 127:128]
        state = (
            jnp.zeros((1, 128), f32), jnp.zeros((HD, 128), f32), jnp.zeros((1, 128), f32),
            jnp.full((1, 128), MASKED, f32),
        )
        for b in range(BLOCKS):
            put_state(pre.at[b], state)
            rows = slice(b * BLK, (b + 1) * BLK)
            keys, values = p1[rows, 0:128], p1[rows, 128:256]
            spread = by_head(
                lane, columns[:, 16 + 2 * b : 17 + 2 * b], columns[:, 17 + 2 * b : 18 + 2 * b]
            )
            weighted = (values.astype(f32) * spread).astype(bf)
            both = dot(keys, weighted, ((0,), (0,)))
            outer = by_head(lane[:HD], both[:HD], both[HD:]) * scale
            sums = dot(weights.astype(bf), keys)
            normal = by_head(lane1, sums[2 * b : 2 * b + 1], sums[2 * b + 1 : 2 * b + 2]) * scale
            passed = by_head(lane1, ends[2 * b : 2 * b + 1], ends[2 * b + 1 : 2 * b + 2])
            peak = by_head(lane1, top[2 * b : 2 * b + 1], top[2 * b + 1 : 2 * b + 2])
            state = joined(state, (passed, outer, normal, passed + peak))
        small[...] = jnp.zeros_like(small)
        small[0:1, :] = state[2]
        for first, exact in ((1, state[3]), (4, state[0])):
            for k in range(3):
                term = exact.astype(bf).astype(f32)
                small[first + k : first + k + 1, :] = term
                exact = exact - term
        msgs[chip, 0:HD, :] = state[1].astype(bf)
        msgs[chip, HD : HD + 16, :] = small[...].astype(bf)

    told = []

    def tell_state():
        mine = msgs.at[chip]
        for dz, dy in plane:
            device = w.moved(z=w.step("z", dz), y=w.step("y", dy))
            told.append(w.send(mine, mine, device))

    def incoming_state():
        for k, (dz, dy) in zip(told, plane):
            w.arrived(k, msgs.at[w.step("z", -dz) * RING + w.step("y", -dy)])
        state = (
            jnp.zeros((1, 128), f32), jnp.zeros((HD, 128), f32), jnp.zeros((1, 128), f32),
            jnp.full((1, 128), MASKED, f32),
        )
        for other in range(CHIPS - 1):
            rest = msgs[other, HD : HD + 16, :].astype(f32)
            came = (
                rest[4:5] + rest[5:6] + rest[6:7], msgs[other, 0:HD, :].astype(f32),
                rest[0:1], rest[1:2] + rest[2:3] + rest[3:4],
            )
            after = joined(state, came)
            state = tuple(jnp.where(other < chip, new, old) for new, old in zip(after, state))
        return state

    def memory_block(b, incoming):
        rows = slice(b * BLK, (b + 1) * BLK)
        _, state, normal, level = joined(incoming, get_state(pre.at[b]))
        keys, values, query = p1[rows, 0:128], p1[rows, 128:256], p1[rows, 256:384]
        whole = jnp.concatenate(
            [jnp.where(lane[:HD] < HD, state, 0.0), jnp.where(lane[:HD] >= HD, state, 0.0)], axis=0
        ).astype(bf)
        carried_num = dot(query, whole)
        with_normal = query.astype(f32) * normal
        recalled = []
        for h in range(2):
            mine = (lane < HD) if h == 0 else (lane >= HD)
            r = 2 * b + h
            a = jnp.where(row >= lane, rows_in[r : r + 1, :], MASKED)
            stab = level[:, 64 * h : 64 * h + 1]
            high = jnp.maximum(jnp.max(a, axis=1, keepdims=True), stab)
            carried = jnp.exp(stab - high)
            query_h = jnp.where(mine, query, jnp.zeros_like(query))
            affinity = dot(query_h, keys, ((1,), (1,))) * scale * jnp.exp(a - high)
            den = carried * jnp.sum(jnp.where(mine, with_normal, 0.0), axis=1, keepdims=True)
            den = den + jnp.sum(affinity, axis=1, keepdims=True)
            num = carried * carried_num + dot(affinity.astype(bf), values)
            floor = jnp.exp(-(square[:, r : r + 1] + high))
            recalled.append(num / jnp.maximum(jnp.abs(den), floor))
        recall = by_head(lane, recalled[0], recalled[1])
        opened = 1.0 / (1.0 + jnp.exp(-p1[rows, 384:512].astype(f32)))
        outs[rows, pl.ds(pl.multiple_of(feature_mem, 128), 128)] = (recall * opened).astype(bf)

    def attention(first, last):
        query_index = lax.broadcasted_iota(jnp.int32, (WINDOW, 2 * WINDOW), 0)
        key_index = lax.broadcasted_iota(jnp.int32, (WINDOW, 2 * WINDOW), 1)
        distance = query_index - key_index + WINDOW
        in_band = (distance >= 0) & (distance < WINDOW)

        def one_block(b, carry):
            rows = pl.ds(pl.multiple_of(b * WINDOW, WINDOW), WINDOW)
            window = pl.ds(pl.multiple_of(b * WINDOW, WINDOW), 2 * WINDOW)
            keys, values = kd[window, :], vd[window, :]
            allowed = in_band & ((chip * BLOCKS + b) * WINDOW - WINDOW + key_index >= 0)
            logs = jnp.zeros((WINDOW, 128), f32)
            for pair in range(2):
                query = p2[rows, pair * 128 : (pair + 1) * 128]
                results = []
                for half in range(2):
                    h = 2 * pair + half
                    mine = (lane < HD) if half == 0 else (lane >= HD)
                    query_h = jnp.where(mine, query, jnp.zeros_like(query))
                    scores = dot(query_h, keys, ((1,), (1,))) * scale
                    scores = jnp.where(allowed, scores, MASKED)
                    sink = sinks[4 * c + h]
                    ceiling = jnp.maximum(jnp.max(scores, axis=1, keepdims=True), sink)
                    weights = jnp.exp(scores - ceiling)
                    part = jnp.exp(sink - ceiling) + jnp.sum(weights, axis=1, keepdims=True)
                    logs = jnp.where(lane == 4 * c + h, ceiling + jnp.log(part), logs)
                    probs = (weights * (1.0 / part)).astype(bf)
                    results.append(dot(probs, values))
                col = pl.multiple_of(feature_attn + pair * 128, 128)
                outs[rows, pl.ds(col, 128)] = by_head(lane, results[0], results[1]).astype(bf)
            lt[rows, :] = logs
            return carry

        lax.fori_loop(first, last, one_block, 0)

    third = ROWS // 3

    def out_region(start, base, stride, width):
        def region(xi, ci, part):
            count = third if part is None else third // 2
            first = start if part is None else start + part * (third // 2)
            col = pl.multiple_of(base + 2 * stride * xi + stride * ci, 128)
            return outs.at[pl.ds(first, count), pl.ds(col, width)]

        return RowGather(w, region)

    mem_out = [out_region(i * third, 2048, 128, 128) for i in range(3)]
    attn_out = [out_region(i * third, 0, 256, 256) for i in range(3)]
    theirs = pl.ds(pl.multiple_of((1 - c) * HALF, HALF), HALF)
    ours = pl.ds(pl.multiple_of(c * HALF, HALF), HALF)

    def normalize_all():
        token_copy.wait()
        lax.fori_loop(0, TOK // 16, normalize, 0)

    kept_values = {}

    def rim_start():
        next_chip = w.moved(z=lax.rem(z + (y + 1) // RING, RING), y=w.step("y", 1))
        kept_values["rim"] = [
            w.send(ref.at[ROWS : ROWS + WINDOW], ref.at[0:WINDOW], next_chip) for ref in (kd, vd)
        ]

    def rim_came():
        w.arrived(kept_values["rim"][0], kd.at[0:WINDOW])
        w.arrived(kept_values["rim"][1], vd.at[0:WINDOW])

    def state_came():
        kept_values["state"] = incoming_state()

    def memory_blocks(first, last):
        for b in range(first, last):
            memory_block(b, kept_values["state"])

    def out_first(half):
        rows = (theirs, ours)[half]
        total[rows, :] = dot(outs[rows, :2048], w3[:2048])

    def log_start():
        kept_values["log"] = w.send(lt.at[theirs], ltin, w.partner())

    def out_last():
        out_cols = out.at[:, pl.ds(pl.multiple_of(c * 512, 512), 512)]
        stage[...] = (total[theirs, :] + dot(outs[theirs, 2048:], w3[2048:])).astype(bf)
        mixed_over = w.send(stage, out_cols, w.partner())
        out[:, pl.ds(pl.multiple_of(c * 512, 512), 512)] = (
            total[ours, :] + dot(outs[ours, 2048:], w3[2048:])
        ).astype(bf)
        w.arrived(kept_values["log"], ltin)
        lt_out[...] = jnp.transpose(lt[ours, :] + ltin[...])[:8]
        w.arrived(mixed_over, out.at[:, pl.ds(pl.multiple_of((1 - c) * 512, 512), 512)])

    schedule(
        types.SimpleNamespace(
            pump=pump, normalize=normalize_all, finish=w.finish, tokens=tokens, gate_weights=gate_copy.wait,
            first_projection=first_projection, second_projection=second_projection,
            rim_start=rim_start, rim_came=rim_came, memory_gates=memory_gates,
            tell_state=tell_state, state_came=state_came, memory_blocks=memory_blocks,
            attention=attention, attn_out=attn_out, mem_out=mem_out, out_first=out_first,
            log_start=log_start, out_last=out_last,
        )
    )


def schedule(s):
    pump, attn, mem = s.pump, s.attn_out, s.mem_out
    pump(0, 2)
    s.normalize()
    s.tokens.start()
    pump(0, 21)
    pump(1, 4)
    pump(0, 23)
    s.tokens.came(1)
    s.tokens.came(-1)
    pump(0, 35)
    pump(1, 5)
    pump(0, 37)
    pump(1, 11)
    pump(0, 39)
    pump(1, 12)
    s.tokens.done(1)
    s.tokens.done(-1)
    s.tokens.shared(0)
    s.tokens.shared(-1)
    s.tokens.shared(1)
    pump(0, 43)
    pump(1, 13)
    s.tokens.shared(2)
    pump(0, 44)
    s.gate_weights()
    s.first_projection(0)
    pump(1, 24)
    pump(2, 4)
    s.first_projection(1)
    pump(1, 32)
    s.rim_start()
    s.memory_gates()
    pump(1, 40)
    s.tell_state()
    s.attention(2, 4)
    attn[1].start()
    s.attention(4, 6)
    attn[2].start()
    pump(2, 12)
    pump(1, 44)
    s.second_projection(0)
    s.rim_came()
    s.attention(0, 2)
    attn[0].start()
    attn[1].came(1)
    attn[1].came(-1)
    s.second_projection(1)
    attn[2].came(1)
    attn[2].came(-1)
    s.log_start()
    pump(2, 13)
    s.state_came()
    s.memory_blocks(0, 2)
    mem[0].start()
    attn[0].came(1)
    attn[0].came(-1)
    s.memory_blocks(2, 4)
    mem[1].start()
    pump(2, 15)
    attn[1].done(1)
    attn[1].done(-1)
    attn[1].shared(0)
    attn[1].shared(-1)
    attn[1].shared(1)
    s.memory_blocks(4, 6)
    mem[2].start()
    pump(2, 24)
    attn[1].shared(2)
    attn[2].done(1)
    attn[2].done(-1)
    attn[2].shared(0)
    attn[2].shared(-1)
    attn[2].shared(1)
    mem[0].came(1)
    mem[0].came(-1)
    attn[2].shared(2)
    attn[0].done(1)
    attn[0].done(-1)
    attn[0].shared(0)
    attn[0].shared(-1)
    attn[0].shared(1)
    pump(2, 25)
    attn[0].shared(2)
    mem[1].came(1)
    mem[1].came(-1)
    pump(2, 33)
    mem[2].came(1)
    mem[2].came(-1)
    pump(2, 37)
    mem[0].done(1)
    mem[0].done(-1)
    mem[0].shared(0)
    mem[0].shared(-1)
    mem[0].shared(1)
    pump(2, 41)
    mem[1].done(1)
    mem[1].done(-1)
    mem[1].shared(0)
    mem[1].shared(-1)
    mem[1].shared(1)
    mem[0].shared(2)
    pump(2, 44)
    s.out_first(0)
    mem[1].shared(2)
    mem[2].done(1)
    mem[2].done(-1)
    mem[2].shared(0)
    mem[2].shared(-1)
    mem[2].shared(1)
    s.out_first(1)
    mem[2].shared(2)
    s.out_last()
    s.finish()


def shards(
    tokens, norm_gain, w_query, w_key, w_value, w_mem_query, w_mem_key, w_mem_value, w_mem_gate,
    w_gates, sinks, forget_bias, forget_shift, w_out,
):
    gates = w_gates.transpose(1, 2, 0).reshape(32, D)
    vmem = pl.BlockSpec(memory_space=pltpu.VMEM)
    smem = pl.BlockSpec(memory_space=pltpu.SMEM)
    anywhere = pl.BlockSpec(memory_space=pl.ANY)
    bf, f32 = jnp.bfloat16, jnp.float32
    mixed, log_total = pl.pallas_call(
        layer_kernel,
        out_shape=[
            jax.ShapeDtypeStruct((HALF, 1024), bf),
            jax.ShapeDtypeStruct((8, HALF), f32),
        ],
        in_specs=[anywhere, vmem] + [anywhere] * 9 + [smem, smem, vmem],
        out_specs=[vmem, vmem],
        scratch_shapes=[
            pltpu.VMEM((TOK, D), bf),
            pltpu.VMEM((2, 128, 128), bf),
            pltpu.VMEM((2, 128, 128), bf),
            pltpu.VMEM((ROWS, D), bf),
            pltpu.VMEM((D, 640), bf),
            pltpu.VMEM((D, 256), bf),
            pltpu.VMEM((3072, 512), bf),
            pltpu.VMEM((32, D), bf),
            pltpu.VMEM((ROWS, 512), bf),
            pltpu.VMEM((ROWS, 128), f32),
            pltpu.VMEM((ROWS, 256), bf),
            pltpu.VMEM((ROWS + WINDOW, 128), bf),
            pltpu.VMEM((ROWS + WINDOW, 128), bf),
            pltpu.VMEM((2, 4, HALF), f32),
            pltpu.VMEM((CHIPS, HD + 16, 128), bf),
            pltpu.VMEM((BLOCKS, HD + 8, 128), f32),
            pltpu.VMEM((ROWS, 3072), bf),
            pltpu.VMEM((ROWS, 128), f32),
            pltpu.VMEM((HALF, 128), f32),
            pltpu.VMEM((HALF, 512), bf),
            pltpu.VMEM((ROWS, 512), f32),
            pltpu.VMEM((128, 128), f32),
            pltpu.VMEM((16, 128), f32),
            pltpu.VMEM((16, 128), f32),
            pltpu.VMEM((16, 128), f32),
            pltpu.VMEM((16, 128), f32),
            pltpu.VMEM((128, 128), f32),
            pltpu.SemaphoreType.DMA((MAX_COPIES,)),
            pltpu.SemaphoreType.DMA((MAX_COPIES,)),
            pltpu.SemaphoreType.DMA((16,)),
        ],
        compiler_params=pltpu.CompilerParams(
            collective_id=0, has_side_effects=True, vmem_limit_bytes=60 * 1024 * 1024
        ),
        name="layer",
    )(
        tokens, norm_gain.reshape(1, D), w_query, w_key, w_value, w_mem_query, w_mem_key,
        w_mem_value, w_mem_gate, w_out, gates, sinks, forget_bias, forget_shift.T,
    )
    return (mixed, log_total.T)


def solution(mesh):
    torus = Mesh(mesh.devices.reshape(4, 4, 2, mesh.shape["tp"]), ("z", "y", "c", "x"))
    sp = ("z", "y", "c")
    placed = (
        (P(("z", "y", "c", "x"), None), P())
        + (P(sp, "x"),) * 7
        + (P(), P("x"), P("x"), P(sp, "x"), P(sp, "x"))
    )
    return jax.shard_map(
        shards, mesh=torus, in_specs=placed, out_specs=(P(sp, "x"), P(sp, "x")), check_vma=False
    )
```

```python
import functools
import math
import types

import jax
import jax.numpy as jnp
from jax import lax
from jax.experimental import pallas as pl
from jax.experimental.pallas import tpu as pltpu
from jax.sharding import Mesh
from jax.sharding import PartitionSpec as P

HD = 64
WINDOW = 128
BLK = 128
EPSILON = 1e-06
MASKED = -1e30
MESH = pl.DeviceIdType.MESH
RING = 4
TOK = 96
ROWS = 8 * TOK
D = 4096
PLANE = ("z", "y")
SENDS = 12
RECEIVES = 72
HALF = ROWS // 2
BLOCKS = ROWS // BLK
CHIPS = RING * RING


class Wires:
    def __init__(self, send_sem, recv_sem):
        self.send_sem, self.recv_sem = send_sem, recv_sem
        self.groups, self.keys, self.steps = {}, {}, {}
        z, y, c, x = (lax.axis_index(a) for a in ("z", "y", "c", "x"))
        self.at = {"z": z, "y": y, "c": c, "x": x}

    def moved(self, **new):
        where = dict(self.at)
        where.update(new)
        return (where["z"], where["y"], where["c"], where["x"])

    def step(self, axis, distance):
        if distance % RING == 0:
            return self.at[axis]
        key = (axis, distance % RING)
        if key not in self.steps:
            self.steps[key] = lax.rem(self.at[axis] + key[1], RING)
        return self.steps[key]

    def neighbour(self, axis, distance):
        return self.moved(**{axis: self.step(axis, distance)})

    def partner(self):
        return self.moved(c=1 - self.at["c"])

    def copy(self, src, dst, device, group, key):
        return pltpu.make_async_remote_copy(
            src_ref=src,
            dst_ref=dst,
            send_sem=self.send_sem.at[self.groups.setdefault(group, len(self.groups))],
            recv_sem=self.recv_sem.at[self.keys.setdefault(key, len(self.keys))],
            device_id=device,
            device_id_type=MESH,
        )

    def send(self, src, dst, device, group, key):
        self.copy(src, dst, device, group, key).start()

    def arrived(self, key, size):
        group = next(iter(self.groups))
        self.copy(size, size, self.partner(), group, key).wait_recv()

    def all_sent(self, group, size):
        key = next(iter(self.keys))
        self.copy(size, size, self.partner(), group, key).wait_send()


class PlaneGather:
    def __init__(self, wires, whole, width, depth, core, name):
        self.w, self.whole, self.width = wires, whole, width
        self.depth, self.core, self.name = depth, core, name

    def mixed(self, axis, one, two):
        first, second = (one, two) if axis == "z" else (two, one)
        return self.w.step(axis, first) * (1 - self.core) + self.w.step(axis, second) * self.core

    def rows(self, d1, d2, part=None):
        z, y = self.mixed("z", d1, d2), self.mixed("y", d1, d2)
        start = ((z * RING + y) * 2 + self.core) * self.depth
        half = self.depth // 2
        if part is None:
            return self.whole.at[pl.ds(pl.multiple_of(start, 16), self.depth), : self.width]
        return self.whole.at[pl.ds(pl.multiple_of(start + part * half, 16), half), : self.width]

    def go(self, key, d1, d2, first, distance, part=None):
        block = self.rows(d1, d2, part)
        one, two = (distance, 0) if first else (0, distance)
        device = self.w.moved(z=self.mixed("z", one, two), y=self.mixed("y", one, two))
        self.w.send(block, block, device, self.name[0], key)

    def came(self, key, blocks):
        self.w.arrived(key, self.whole.at[pl.ds(0, blocks * self.depth), : self.width])

    def second_round(self, d1):
        for side in (1, -1):
            self.go((self.name, "second", d1), d1, 0, False, side)

    def start(self):
        for side in (1, -1):
            self.go((self.name, "first"), 0, 0, True, side)
        self.second_round(0)

    def first_came(self):
        self.came((self.name, "first"), 2)
        for side in (1, -1):
            self.go((self.name, "again"), -side, 0, True, side, 0 if side > 0 else 1)
            self.second_round(-side)

    def second_came(self, d1):
        self.came((self.name, "second", d1), 2)
        for side in (1, -1):
            self.go((self.name[0], "last"), d1, -side, False, side, 0 if side > 0 else 1)

    def first_done(self):
        self.came((self.name, "again"), 1)
        self.second_round(2)

    def all_done(self):
        self.came((self.name[0], "last"), 8)

    def all_sent(self):
        self.w.all_sent(self.name[0], self.whole.at[pl.ds(0, 30 * self.depth), : self.width])


def plane_steps(wires, whole, width, depth, name, own_ready, other_ready):
    c = wires.at["c"]
    pair = [
        PlaneGather(wires, whole, width, depth, core, (name, k))
        for k, core in enumerate((c, 1 - c))
    ]
    steps = [own_ready, pair[0].start, other_ready, pair[1].start]
    steps += [g.first_came for g in pair]
    steps += [functools.partial(g.second_came, 0) for g in pair]
    steps += [g.first_done for g in pair]
    for d1 in (-1, 1, 2):
        steps += [functools.partial(g.second_came, d1) for g in pair]
    return steps + [pair[0].all_done], pair[0].all_sent


class RowGather:
    def __init__(self, wires, region, group, name, relative=False):
        self.w, self.region, self.relative = wires, region, relative
        self.group, self.name = group, name

    def piece(self, dx, other=False, part=None):
        c = self.w.at["c"]
        where = dx if self.relative else self.w.step("x", dx)
        return self.region(where, 1 - c if other else c, part)

    def there(self, dx, side, part=None):
        if self.relative:
            dx = (0, 1, 2, -1)[(dx - side) % RING]
        return self.piece(dx, part=part)

    def share(self, dx):
        block = self.piece(dx)
        key = (self.group, "shared", self.relative and dx in (1, 2))
        self.w.send(block, block, self.w.partner(), self.group, key)

    def start(self):
        for side in (1, -1):
            self.w.send(
                self.piece(0), self.there(0, side), self.w.neighbour("x", side),
                self.group, (self.group, self.name, side),
            )
        self.share(0)

    def came(self, side):
        part = 0 if side > 0 else 1
        self.w.arrived((self.group, self.name, side), self.piece(-side))
        self.w.send(
            self.piece(-side, part=part), self.there(-side, side, part),
            self.w.neighbour("x", side), self.group, (self.group, self.name, 0),
        )
        self.share(-side)

    def done(self):
        self.w.arrived((self.group, self.name, 0), self.piece(2))
        self.share(2)


def dot(a, b, dims=((1,), (0,))):
    return lax.dot_general(a, b, (dims, ((), ())), preferred_element_type=jnp.float32)


def by_head(lane, first, second):
    return jnp.where(lane < HD, first, second)


def joined(one, two):
    passed_one, state_one, normal_one, level_one = one
    passed_two, state_two, normal_two, level_two = two
    level = jnp.maximum(passed_two + level_one, level_two)
    weight_one = jnp.exp(passed_two + level_one - level)
    weight_two = jnp.exp(level_two - level)
    return (
        passed_one + passed_two,
        weight_one * state_one + weight_two * state_two,
        weight_one * normal_one + weight_two * normal_two,
        level,
    )


def put_state(ref, state):
    ref[0:HD, :] = state[1]
    ref[HD : HD + 1, :] = state[2]
    ref[HD + 1 : HD + 2, :] = state[3]
    ref[HD + 2 : HD + 3, :] = state[0]


def get_state(ref):
    return (
        ref[HD + 2 : HD + 3, :], ref[0:HD, :], ref[HD : HD + 1, :], ref[HD + 1 : HD + 2, :]
    )


def layer_kernel(
    tok, gain, wq, wk, wv, wmq, wmk, wmv, wmg, wo, wg, sinks, fbias, fshift,
    out, lt_out,
    tokv, rawkv, kvp, normed, w1, w2, w3, wgv, p1, gate, p2, kd, vd, sh, msgs, pre, outs, lt, ltin,
    stage, turned, small, rows_in, rows_f, rows_sh, square, send_sem, recv_sem, local_sem,
):
    bf, f32 = jnp.bfloat16, jnp.float32
    w = Wires(send_sem, recv_sem)
    z, y, c, x = (w.at[a] for a in ("z", "y", "c", "x"))
    chip = z * RING + y
    barrier = pltpu.get_barrier_semaphore()
    plane = [(dz, dy) for dz in range(RING) for dy in range(RING) if dz or dy]
    greeted = [w.neighbour(axis, d) for axis in ("z", "y", "x") for d in (1, -1)]
    greeted.append(w.partner())
    for device in greeted:
        pl.semaphore_signal(barrier, inc=1, device_id=device, device_id_type=MESH)

    local = []

    def fetch(src, dst):
        copy = pltpu.make_async_copy(src, dst, local_sem.at[len(local)])
        copy.start()
        local.append(copy)
        return copy

    k_copy, v_copy = fetch(wk, rawkv.at[0]), fetch(wv, rawkv.at[1])
    token_copy = fetch(tok, tokv)

    def block_rows(ref, core, depth, cols):
        start = pl.multiple_of(((z * RING + y) * 2 + core) * depth, 16)
        return ref.at[pl.ds(start, depth), cols]

    def cut(ref, width):
        return lambda h: ref.at[:, pl.ds(pl.multiple_of(h * width, 128), width)]

    pieces = [
        (cut(wq, 256), w1, 128, slice(0, 256)),
        (lambda h: kvp.at[h], w1, 128, slice(256, 384)),
        (cut(wmk, 128), w1, 128, slice(384, 512)),
        (cut(wmv, 128), w1, 128, slice(512, 640)),
        (cut(wmq, 128), w2, 128, slice(0, 128)),
        (cut(wmg, 128), w2, 128, slice(128, 256)),
        (cut(wo, 512), w3, 96, slice(0, 512)),
    ]
    kept = [None] * len(pieces)
    for n, (half_of, dst, depth, cols) in enumerate(pieces):
        if n != 1:
            kept[n] = fetch(half_of(c), block_rows(dst, c, depth, cols))
    gate_copy = fetch(wg, wgv)

    k_copy.wait()
    v_copy.wait()
    kvp[0] = jnp.concatenate([rawkv[0, :, :HD], rawkv[1, :, :HD]], axis=1)
    kvp[1] = jnp.concatenate([rawkv[0, :, HD:], rawkv[1, :, HD:]], axis=1)
    sh[c] = fshift[...]
    kept[1] = fetch(kvp.at[c], block_rows(w1, c, 128, slice(256, 384)))
    pl.semaphore_wait(barrier, len(greeted))

    sizes = (w1.at[0:128, 0:640], w2.at[0:128, :], w3.at[0:96, :])
    for n, (half_of, dst, depth, cols) in enumerate(pieces):
        key = ("over", (n >= 4) + (n >= 6))
        w.send(half_of(1 - c), block_rows(dst, c, depth, cols), w.partner(), "over", key)

    slots = {0: 0, -1: 1, 1: 2, 2: 3}

    def token_rows(dx, ci, part):
        start = slots[dx] * 2 * TOK + ci * TOK
        if part is None:
            return normed.at[pl.ds(pl.multiple_of(start, 16), TOK)]
        return normed.at[pl.ds(pl.multiple_of(start + part * (TOK // 2), 16), TOK // 2)]

    tokens = RowGather(w, token_rows, "tokens", "", relative=True)
    first_row = c * TOK

    def normalize(i, carry):
        values = tokv[pl.ds(pl.multiple_of(i * 16, 16), 16), :].astype(f32)
        rescale = lax.rsqrt(jnp.mean(values * values, axis=-1, keepdims=True) + EPSILON)
        normed[pl.ds(pl.multiple_of(first_row + i * 16, 16), 16), :] = (
            values * rescale * gain[...]
        ).astype(bf)
        return carry

    w.send(fshift, sh.at[c], w.partner(), "shift", "shift")

    def own_ready(first, last):
        for n in range(first, last):
            kept[n].wait()

    def other_ready(group):
        w.arrived(("over", group), sizes[group])

    groups, sent = [], []
    for n, (whole, width, depth, pair) in enumerate(
        ((w1, 640, 128, (0, 4)), (w2, 256, 128, (4, 6)), (w3, 512, 96, (6, 7)))
    ):
        steps, all_sent = plane_steps(
            w, whole, width, depth, ("weights", n),
            functools.partial(own_ready, *pair), functools.partial(other_ready, n),
        )
        groups.append(steps)
        sent.append(all_sent)
    at = [0, 0, 0]

    def pump(group, upto):
        while at[group] < min(upto, len(groups[group])):
            groups[group][at[group]]()
            at[group] += 1

    def pieces_of(i):
        for j in range(4):
            dx, ci = (0, -1, 1, 2)[2 * i + j // 2], j % 2
            yield slice(j * TOK, (j + 1) * TOK), (ci * RING + w.step("x", dx)) * TOK

    def span(start):
        return pl.ds(pl.multiple_of(start, 16), TOK)

    def gate_weights():
        gate_copy.wait()
        for k in range(D // 128):
            turned_gates = jnp.transpose(wgv[:, k * 128 : (k + 1) * 128].astype(f32))
            w1[k * 128 : (k + 1) * 128, 640:672] = turned_gates.astype(bf)

    def attn_projection(i):
        both = dot(normed[i * HALF : (i + 1) * HALF, :], w1[:, :384])
        kv = both[:, 256:]
        turned_kv = pltpu.roll(kv, HD, 1)
        lane = lax.broadcasted_iota(jnp.int32, kv.shape, 1)
        keys = by_head(lane, kv, turned_kv).astype(bf)
        values = by_head(lane, turned_kv, kv).astype(bf)
        for rows, start in pieces_of(i):
            p2[span(start), :] = both[rows, :256].astype(bf)
            kd[span(start + WINDOW), :] = keys[rows]
            vd[span(start + WINDOW), :] = values[rows]

    def first_projection(i):
        both = dot(normed[i * HALF : (i + 1) * HALF, :], w1[:, 384:])
        for rows, start in pieces_of(i):
            p1[span(start), 0:256] = both[rows, :256].astype(bf)
            gate[span(start), 0:32] = both[rows, 256:]

    def second_projection(i):
        both = dot(normed[i * HALF : (i + 1) * HALF, :], w2[...]).astype(bf)
        for rows, start in pieces_of(i):
            p1[span(start), 256:512] = both[rows]

    lane1 = lax.broadcasted_iota(jnp.int32, (1, 128), 1)
    lane = lax.broadcasted_iota(jnp.int32, (128, 128), 1)
    row = lax.broadcasted_iota(jnp.int32, (128, 128), 0)
    scale = HD ** (-0.5)
    feature_attn = 512 * x + 256 * c
    feature_mem = 2048 + 256 * x + 128 * c

    def memory_gates():
        rows_in[...] = jnp.zeros_like(rows_in)
        rows_f[...] = jnp.zeros_like(rows_f)
        rows_sh[...] = jnp.zeros_like(rows_sh)
        gate[:, 32:] = jnp.zeros((ROWS, 96), f32)
        square[...] = jnp.zeros_like(square)
        w.arrived("shift", sh.at[1 - c])
        for b in range(BLOCKS):
            turned[...] = jnp.transpose(gate[b * BLK : (b + 1) * BLK, :])
            for h in range(2):
                own = 4 * x + 2 * c + h
                rows_in[2 * b + h : 2 * b + h + 1, :] = turned[pl.ds(own, 1), :]
                rows_f[2 * b + h : 2 * b + h + 1, :] = turned[pl.ds(16 + own, 1), :]
            q, at_col = b // 3, (b % 3) * BLK
            both = sh[q, :, at_col : at_col + BLK]
            rows_sh[2 * b : 2 * b + 2, :] = jnp.where(c == 0, both[0:2], both[2:4])
        head = lax.broadcasted_iota(jnp.int32, (16, 128), 0) % 2
        pre_forget = rows_f[...] + jnp.where(head == 0, fbias[2 * c], fbias[2 * c + 1])
        log_forget = (
            jnp.minimum(pre_forget, 0.0)
            - jnp.log1p(jnp.exp(-jnp.abs(pre_forget)))
            + rows_sh[...]
        )
        upto = (row <= lane).astype(f32)
        cumulative = jnp.dot(
            log_forget, upto, precision=lax.Precision.HIGHEST, preferred_element_type=f32
        )
        a = rows_in[...] - 0.5 * math.log(CHIPS * ROWS) - cumulative
        top = jnp.max(a, axis=1, keepdims=True)
        weights = jnp.exp(a - top)
        square[0:16, :] = cumulative
        square[16:32, :] = weights
        rows_in[...] = a
        rows_f[...] = weights
        columns = jnp.transpose(square[...])
        square[...] = columns
        ends = cumulative[:, 127:128]
        state = (
            jnp.zeros((1, 128), f32), jnp.zeros((HD, 128), f32), jnp.zeros((1, 128), f32),
            jnp.full((1, 128), MASKED, f32),
        )
        for b in range(BLOCKS):
            put_state(pre.at[b], state)
            rows = slice(b * BLK, (b + 1) * BLK)
            keys, values = p1[rows, 0:128], p1[rows, 128:256]
            spread = by_head(
                lane, columns[:, 16 + 2 * b : 17 + 2 * b], columns[:, 17 + 2 * b : 18 + 2 * b]
            )
            weighted = (values.astype(f32) * spread).astype(bf)
            both = dot(keys, weighted, ((0,), (0,)))
            outer = by_head(lane[:HD], both[:HD], both[HD:]) * scale
            sums = dot(weights.astype(bf), keys)
            normal = by_head(lane1, sums[2 * b : 2 * b + 1], sums[2 * b + 1 : 2 * b + 2]) * scale
            passed = by_head(lane1, ends[2 * b : 2 * b + 1], ends[2 * b + 1 : 2 * b + 2])
            peak = by_head(lane1, top[2 * b : 2 * b + 1], top[2 * b + 1 : 2 * b + 2])
            state = joined(state, (passed, outer, normal, passed + peak))
        small[...] = jnp.zeros_like(small)
        small[0:1, :] = state[2]
        for first, exact in ((1, state[3]), (4, state[0])):
            for k in range(3):
                term = exact.astype(bf).astype(f32)
                small[first + k : first + k + 1, :] = term
                exact = exact - term
        msgs[chip, 0:HD, :] = state[1].astype(bf)
        msgs[chip, HD : HD + 16, :] = small[...].astype(bf)

    def tell_state():
        mine = msgs.at[chip]
        for dz, dy in plane:
            device = w.moved(z=w.step("z", dz), y=w.step("y", dy))
            w.send(mine, mine, device, "state", "state")

    def incoming_state():
        w.arrived("state", msgs.at[0 : CHIPS - 1])
        state = (
            jnp.zeros((1, 128), f32), jnp.zeros((HD, 128), f32), jnp.zeros((1, 128), f32),
            jnp.full((1, 128), MASKED, f32),
        )
        for other in range(CHIPS - 1):
            rest = msgs[other, HD : HD + 16, :].astype(f32)
            came = (
                rest[4:5] + rest[5:6] + rest[6:7], msgs[other, 0:HD, :].astype(f32),
                rest[0:1], rest[1:2] + rest[2:3] + rest[3:4],
            )
            after = joined(state, came)
            state = tuple(jnp.where(other < chip, new, old) for new, old in zip(after, state))
        return state

    def memory_block(b, incoming):
        rows = slice(b * BLK, (b + 1) * BLK)
        _, state, normal, level = joined(incoming, get_state(pre.at[b]))
        keys, values, query = p1[rows, 0:128], p1[rows, 128:256], p1[rows, 256:384]
        whole = jnp.concatenate(
            [jnp.where(lane[:HD] < HD, state, 0.0), jnp.where(lane[:HD] >= HD, state, 0.0)], axis=0
        ).astype(bf)
        carried_num = dot(query, whole)
        with_normal = query.astype(f32) * normal
        recalled = []
        for h in range(2):
            mine = (lane < HD) if h == 0 else (lane >= HD)
            r = 2 * b + h
            a = jnp.where(row >= lane, rows_in[r : r + 1, :], MASKED)
            stab = level[:, 64 * h : 64 * h + 1]
            high = jnp.maximum(jnp.max(a, axis=1, keepdims=True), stab)
            carried = jnp.exp(stab - high)
            query_h = jnp.where(mine, query, jnp.zeros_like(query))
            affinity = dot(query_h, keys, ((1,), (1,))) * scale * jnp.exp(a - high)
            den = carried * jnp.sum(jnp.where(mine, with_normal, 0.0), axis=1, keepdims=True)
            den = den + jnp.sum(affinity, axis=1, keepdims=True)
            num = carried * carried_num + dot(affinity.astype(bf), values)
            floor = jnp.exp(-(square[:, r : r + 1] + high))
            recalled.append(num / jnp.maximum(jnp.abs(den), floor))
        recall = by_head(lane, recalled[0], recalled[1])
        opened = 1.0 / (1.0 + jnp.exp(-p1[rows, 384:512].astype(f32)))
        outs[rows, pl.ds(pl.multiple_of(feature_mem, 128), 128)] = (recall * opened).astype(bf)

    def attention(first, last):
        query_index = lax.broadcasted_iota(jnp.int32, (WINDOW, 2 * WINDOW), 0)
        key_index = lax.broadcasted_iota(jnp.int32, (WINDOW, 2 * WINDOW), 1)
        distance = query_index - key_index + WINDOW
        in_band = (distance >= 0) & (distance < WINDOW)

        def one_block(b, carry):
            rows = pl.ds(pl.multiple_of(b * WINDOW, WINDOW), WINDOW)
            window = pl.ds(pl.multiple_of(b * WINDOW, WINDOW), 2 * WINDOW)
            keys, values = kd[window, :], vd[window, :]
            allowed = in_band & ((chip * BLOCKS + b) * WINDOW - WINDOW + key_index >= 0)
            logs = jnp.zeros((WINDOW, 128), f32)
            for pair in range(2):
                query = p2[rows, pair * 128 : (pair + 1) * 128]
                results = []
                for half in range(2):
                    h = 2 * pair + half
                    mine = (lane < HD) if half == 0 else (lane >= HD)
                    query_h = jnp.where(mine, query, jnp.zeros_like(query))
                    scores = dot(query_h, keys, ((1,), (1,))) * scale
                    scores = jnp.where(allowed, scores, MASKED)
                    sink = sinks[4 * c + h]
                    ceiling = jnp.maximum(jnp.max(scores, axis=1, keepdims=True), sink)
                    weights = jnp.exp(scores - ceiling)
                    part = jnp.exp(sink - ceiling) + jnp.sum(weights, axis=1, keepdims=True)
                    logs = jnp.where(lane == 4 * c + h, ceiling + jnp.log(part), logs)
                    probs = (weights * (1.0 / part)).astype(bf)
                    results.append(dot(probs, values))
                col = pl.multiple_of(feature_attn + pair * 128, 128)
                outs[rows, pl.ds(col, 128)] = by_head(lane, results[0], results[1]).astype(bf)
            lt[rows, :] = logs
            return carry

        lax.fori_loop(first, last, one_block, 0)

    third = ROWS // 3

    def out_region(start, base, stride, width, group):
        def region(xi, ci, part):
            count = third if part is None else third // 2
            first = start if part is None else start + part * (third // 2)
            col = pl.multiple_of(base + 2 * stride * xi + stride * ci, 128)
            return outs.at[pl.ds(first, count), pl.ds(col, width)]

        return RowGather(w, region, group, start)

    mem_out = [out_region(i * third, 2048, 128, 128, "mem") for i in range(3)]
    attn_out = [out_region(i * third, 0, 256, 256, "attn") for i in range(3)]
    theirs = pl.ds(pl.multiple_of((1 - c) * HALF, HALF), HALF)
    ours = pl.ds(pl.multiple_of(c * HALF, HALF), HALF)

    def normalize_all():
        token_copy.wait()
        lax.fori_loop(0, TOK // 16, normalize, 0)

    kept_values = {}

    def rim_start():
        next_chip = w.moved(z=lax.rem(z + (y + 1) // RING, RING), y=w.step("y", 1))
        for ref in (kd, vd):
            w.send(ref.at[ROWS : ROWS + WINDOW], ref.at[0:WINDOW], next_chip, "rim", "rim")

    def rim_came():
        w.arrived("rim", kd.at[0 : 2 * WINDOW])

    def tokens_shared(late):
        w.arrived(("tokens", "shared", bool(late)), normed.at[0 : 2 * TOK])

    def attn_shared():
        w.arrived(("attn", "shared", False), outs.at[:, 0:1024])

    def mem_shared():
        w.arrived(("mem", "shared", False), outs.at[:, 0:512])

    def finish():
        for all_sent in sent:
            all_sent()
        for group, size in (
            ("over", w1.at[0:256, 0:640]), ("tokens", normed.at[0 : 7 * TOK]), ("shift", sh.at[0]),
            ("state", msgs.at[0 : CHIPS - 1]), ("rim", kd.at[0 : 2 * WINDOW]),
            ("attn", outs.at[:, 0:1792]), ("mem", outs.at[:, 0:896]), ("log", ltin), ("out", stage),
        ):
            w.all_sent(group, size)

    def state_came():
        kept_values["state"] = incoming_state()

    def memory_blocks(first, last):
        for b in range(first, last):
            memory_block(b, kept_values["state"])

    def log_start():
        w.send(lt.at[theirs], ltin, w.partner(), "log", "log")

    def out_last():
        out_cols = out.at[:, pl.ds(pl.multiple_of(c * 512, 512), 512)]
        stage[...] = dot(outs[theirs, :], w3[...]).astype(bf)
        w.send(stage, out_cols, w.partner(), "out", "out")
        out[:, pl.ds(pl.multiple_of(c * 512, 512), 512)] = dot(
            outs[ours, :], w3[...]
        ).astype(bf)
        w.arrived("log", ltin)
        lt_out[...] = jnp.transpose(lt[ours, :] + ltin[...])[:8]
        w.arrived("out", out.at[:, pl.ds(pl.multiple_of((1 - c) * 512, 512), 512)])

    schedule(
        types.SimpleNamespace(
            pump=pump, normalize=normalize_all, finish=finish, tokens_shared=tokens_shared,
            attn_shared=attn_shared, mem_shared=mem_shared, tokens=tokens, gate_weights=gate_weights,
            attn_projection=attn_projection, first_projection=first_projection, second_projection=second_projection,
            rim_start=rim_start, rim_came=rim_came, memory_gates=memory_gates,
            tell_state=tell_state, state_came=state_came, memory_blocks=memory_blocks,
            attention=attention, attn_out=attn_out, mem_out=mem_out, log_start=log_start, out_last=out_last,
        )
    )


def schedule(s):
    pump, attn, mem = s.pump, s.attn_out, s.mem_out
    pump(0, 2)
    s.normalize()
    s.tokens.start()
    pump(0, 8)
    s.gate_weights()
    pump(0, 14)
    s.tokens.came(1)
    s.tokens.came(-1)
    s.tokens_shared(0)
    pump(0, 16)
    pump(1, 4)
    pump(0, 17)
    s.attn_projection(0)
    pump(1, 5)
    s.tokens.done()
    s.first_projection(0)
    pump(1, 8)
    s.tokens_shared(1)
    s.attn_projection(1)
    pump(1, 9)
    s.rim_start()
    s.attention(2, 4)
    attn[1].start()
    pump(1, 13)
    s.attention(4, 6)
    attn[2].start()
    pump(1, 15)
    pump(2, 4)
    s.first_projection(1)
    pump(1, 16)
    s.rim_came()
    s.attention(0, 2)
    attn[0].start()
    attn[1].came(1)
    attn[1].came(-1)
    s.log_start()
    s.memory_gates()
    s.tell_state()
    pump(2, 5)
    attn[2].came(1)
    attn[2].came(-1)
    pump(2, 8)
    pump(1, 17)
    s.second_projection(0)
    attn[0].came(1)
    attn[0].came(-1)
    s.second_projection(1)
    attn[1].done()
    attn[2].done()
    attn[0].done()
    pump(2, 9)
    s.state_came()
    s.memory_blocks(0, 2)
    mem[0].start()
    s.attn_shared()
    s.memory_blocks(2, 4)
    mem[1].start()
    s.memory_blocks(4, 6)
    mem[2].start()
    pump(2, 14)
    mem[0].came(1)
    mem[0].came(-1)
    mem[1].came(1)
    mem[1].came(-1)
    pump(2, 15)
    mem[2].came(1)
    mem[2].came(-1)
    pump(2, 16)
    mem[0].done()
    mem[1].done()
    mem[2].done()
    s.mem_shared()
    pump(2, 17)
    s.out_last()
    s.finish()


def shards(
    tokens, norm_gain, w_query, w_key, w_value, w_mem_query, w_mem_key, w_mem_value, w_mem_gate,
    w_gates, sinks, forget_bias, forget_shift, w_out,
):
    gates = w_gates.transpose(1, 2, 0).reshape(32, D)
    vmem = pl.BlockSpec(memory_space=pltpu.VMEM)
    smem = pl.BlockSpec(memory_space=pltpu.SMEM)
    anywhere = pl.BlockSpec(memory_space=pl.ANY)
    bf, f32 = jnp.bfloat16, jnp.float32
    mixed, log_total = pl.pallas_call(
        layer_kernel,
        out_shape=[
            pltpu.VMEM((HALF, 1024), bf),
            pltpu.VMEM((8, HALF), f32),
        ],
        in_specs=[anywhere, vmem] + [anywhere] * 9 + [smem, smem, vmem],
        out_specs=[vmem, vmem],
        scratch_shapes=[
            pltpu.VMEM((TOK, D), bf),
            pltpu.VMEM((2, 128, 128), bf),
            pltpu.VMEM((2, 128, 128), bf),
            pltpu.VMEM((ROWS, D), bf),
            pltpu.VMEM((D, 672), bf),
            pltpu.VMEM((D, 256), bf),
            pltpu.VMEM((3072, 512), bf),
            pltpu.VMEM((32, D), bf),
            pltpu.VMEM((ROWS, 512), bf),
            pltpu.VMEM((ROWS, 128), f32),
            pltpu.VMEM((ROWS, 256), bf),
            pltpu.VMEM((ROWS + WINDOW, 128), bf),
            pltpu.VMEM((ROWS + WINDOW, 128), bf),
            pltpu.VMEM((2, 4, HALF), f32),
            pltpu.VMEM((CHIPS, HD + 16, 128), bf),
            pltpu.VMEM((BLOCKS, HD + 8, 128), f32),
            pltpu.VMEM((ROWS, 3072), bf),
            pltpu.VMEM((ROWS, 128), f32),
            pltpu.VMEM((HALF, 128), f32),
            pltpu.VMEM((HALF, 512), bf),
            pltpu.VMEM((128, 128), f32),
            pltpu.VMEM((16, 128), f32),
            pltpu.VMEM((16, 128), f32),
            pltpu.VMEM((16, 128), f32),
            pltpu.VMEM((16, 128), f32),
            pltpu.VMEM((128, 128), f32),
            pltpu.SemaphoreType.DMA((SENDS,)),
            pltpu.SemaphoreType.DMA((RECEIVES,)),
            pltpu.SemaphoreType.DMA((11,)),
        ],
        compiler_params=pltpu.CompilerParams(
            collective_id=0, has_side_effects=True, vmem_limit_bytes=60 * 1024 * 1024
        ),
        name="layer",
    )(
        tokens, norm_gain.reshape(1, D), w_query, w_key, w_value, w_mem_query, w_mem_key,
        w_mem_value, w_mem_gate, w_out, gates, sinks, forget_bias, forget_shift.T,
    )
    return (mixed, log_total.T)


def solution(mesh):
    torus = Mesh(mesh.devices.reshape(4, 4, 2, mesh.shape["tp"]), ("z", "y", "c", "x"))
    sp = ("z", "y", "c")
    placed = (
        (P(("z", "y", "c", "x"), None), P())
        + (P(sp, "x"),) * 7
        + (P(), P("x"), P("x"), P(sp, "x"), P(sp, "x"))
    )
    return jax.shard_map(
        shards, mesh=torus, in_specs=placed, out_specs=(P(sp, "x"), P(sp, "x")), check_vma=False
    )
```

```python
import functools
import math
import types

import jax
import jax.numpy as jnp
from jax import lax
from jax.experimental import pallas as pl
from jax.experimental.pallas import tpu as pltpu
from jax.sharding import Mesh
from jax.sharding import PartitionSpec as P

HD = 64
WINDOW = 128
BLK = 128
EPSILON = 1e-06
MASKED = -1e30
MESH = pl.DeviceIdType.MESH
RING = 4
TOK = 96
ROWS = 8 * TOK
D = 4096
PLANE = ("z", "y")
SENDS = 26
RECEIVES = 86
HALF = ROWS // 2
BLOCKS = ROWS // BLK
CHIPS = RING * RING


class Wires:
    def __init__(self, send_sem, recv_sem):
        self.send_sem, self.recv_sem = send_sem, recv_sem
        self.groups, self.keys, self.steps = {}, {}, {}
        z, y, c, x = (lax.axis_index(a) for a in ("z", "y", "c", "x"))
        self.at = {"z": z, "y": y, "c": c, "x": x}
        for axis in ("z", "y", "x"):
            for distance in range(1, RING):
                self.step(axis, distance)

    def moved(self, **new):
        where = dict(self.at)
        where.update(new)
        return (where["z"], where["y"], where["c"], where["x"])

    def step(self, axis, distance):
        if distance % RING == 0:
            return self.at[axis]
        key = (axis, distance % RING)
        if key not in self.steps:
            self.steps[key] = lax.rem(self.at[axis] + key[1], RING)
        return self.steps[key]

    def neighbour(self, axis, distance):
        return self.moved(**{axis: self.step(axis, distance)})

    def partner(self):
        return self.moved(c=1 - self.at["c"])

    def copy(self, src, dst, device, group, key):
        return pltpu.make_async_remote_copy(
            src_ref=src,
            dst_ref=dst,
            send_sem=self.send_sem.at[self.groups.setdefault(group, len(self.groups))],
            recv_sem=self.recv_sem.at[self.keys.setdefault(key, len(self.keys))],
            device_id=device,
            device_id_type=MESH,
        )

    def reserve(self, group, key):
        self.groups.setdefault(group, len(self.groups))
        self.keys.setdefault(key, len(self.keys))

    def send(self, src, dst, device, group, key):
        self.copy(src, dst, device, group, key).start()

    def arrived(self, key, size):
        group = next(iter(self.groups))
        self.copy(size, size, self.partner(), group, key).wait_recv()

    def all_sent(self, group, size):
        key = next(iter(self.keys))
        self.copy(size, size, self.partner(), group, key).wait_send()


class PlaneGather:
    def __init__(self, wires, whole, width, depth, core, name):
        self.w, self.whole, self.width = wires, whole, width
        self.depth, self.core, self.name = depth, core, name

    def mixed(self, axis, one, two):
        first, second = (one, two) if axis == "z" else (two, one)
        return self.w.step(axis, first) * (1 - self.core) + self.w.step(axis, second) * self.core

    def rows(self, d1, d2, part=None):
        z, y = self.mixed("z", d1, d2), self.mixed("y", d1, d2)
        start = ((z * RING + y) * 2 + self.core) * self.depth
        half = self.depth // 2
        if part is None:
            return self.whole.at[pl.ds(pl.multiple_of(start, 16), self.depth), : self.width]
        return self.whole.at[pl.ds(pl.multiple_of(start + part * half, 16), half), : self.width]

    def go(self, key, d1, d2, first, distance, part=None):
        block = self.rows(d1, d2, part)
        one, two = (distance, 0) if first else (0, distance)
        device = self.w.moved(z=self.mixed("z", one, two), y=self.mixed("y", one, two))
        self.w.send(block, block, device, self.name[0], key)

    def came(self, key, blocks):
        self.w.arrived(key, self.whole.at[pl.ds(0, blocks * self.depth), : self.width])

    def second_round(self, d1):
        for side in (1, -1):
            self.go((self.name, "second", d1), d1, 0, False, side)

    def start(self):
        for side in (1, -1):
            self.go((self.name, "first"), 0, 0, True, side)
        self.second_round(0)

    def first_came(self):
        self.came((self.name, "first"), 2)
        for side in (1, -1):
            self.go((self.name, "again"), -side, 0, True, side, 0 if side > 0 else 1)
            self.second_round(-side)

    def second_came(self, d1):
        self.came((self.name, "second", d1), 2)
        for side in (1, -1):
            self.go((self.name[0], "last"), d1, -side, False, side, 0 if side > 0 else 1)

    def first_done(self):
        self.came((self.name, "again"), 1)
        self.second_round(2)

    def all_done(self):
        self.came((self.name[0], "last"), 8)

    def all_sent(self):
        self.w.all_sent(self.name[0], self.whole.at[pl.ds(0, 30 * self.depth), : self.width])


def plane_steps(wires, whole, width, depth, name, own_ready, other_ready):
    c = wires.at["c"]
    pair = [
        PlaneGather(wires, whole, width, depth, core, (name, k))
        for k, core in enumerate((c, 1 - c))
    ]
    steps = [own_ready, pair[0].start, other_ready, pair[1].start]
    steps += [g.first_came for g in pair]
    steps += [functools.partial(g.second_came, 0) for g in pair]
    steps += [g.first_done for g in pair]
    for d1 in (-1, 1, 2):
        steps += [functools.partial(g.second_came, d1) for g in pair]
    return steps + [pair[0].all_done], pair[0].all_sent


class RowGather:
    def __init__(self, wires, region, group, name, relative=False):
        self.w, self.region, self.relative = wires, region, relative
        self.group, self.name = group, name

    def piece(self, dx, other=False, part=None):
        c = self.w.at["c"]
        where = dx if self.relative else self.w.step("x", dx)
        return self.region(where, 1 - c if other else c, part)

    def there(self, dx, side, part=None):
        if self.relative:
            dx = (0, 1, 2, -1)[(dx - side) % RING]
        return self.piece(dx, part=part)

    def share(self, dx):
        block = self.piece(dx)
        key = (self.group, "shared", self.relative and dx in (1, 2))
        self.w.send(block, block, self.w.partner(), self.group, key)

    def start(self):
        for side in (1, -1):
            self.w.send(
                self.piece(0), self.there(0, side), self.w.neighbour("x", side),
                self.group, (self.group, self.name, side),
            )
        self.share(0)

    def came(self, side):
        part = 0 if side > 0 else 1
        self.w.arrived((self.group, self.name, side), self.piece(-side))
        self.w.send(
            self.piece(-side, part=part), self.there(-side, side, part),
            self.w.neighbour("x", side), self.group, (self.group, self.name, 0),
        )
        self.share(-side)

    def done(self):
        self.w.arrived((self.group, self.name, 0), self.piece(2))
        self.share(2)


def dot(a, b, dims=((1,), (0,))):
    return lax.dot_general(a, b, (dims, ((), ())), preferred_element_type=jnp.float32)


def by_head(lane, first, second):
    return jnp.where(lane < HD, first, second)


def joined(one, two):
    passed_one, state_one, normal_one, level_one = one
    passed_two, state_two, normal_two, level_two = two
    level = jnp.maximum(passed_two + level_one, level_two)
    weight_one = jnp.exp(passed_two + level_one - level)
    weight_two = jnp.exp(level_two - level)
    return (
        passed_one + passed_two,
        weight_one * state_one + weight_two * state_two,
        weight_one * normal_one + weight_two * normal_two,
        level,
    )


def put_state(ref, state):
    ref[0:HD, :] = state[1]
    ref[HD : HD + 1, :] = state[2]
    ref[HD + 1 : HD + 2, :] = state[3]
    ref[HD + 2 : HD + 3, :] = state[0]


def get_state(ref):
    return (
        ref[HD + 2 : HD + 3, :], ref[0:HD, :], ref[HD : HD + 1, :], ref[HD + 1 : HD + 2, :]
    )


def layer_kernel(
    tok, gain, wq, wk, wv, wmq, wmk, wmv, wmg, wo, wg, sinks, fbias, fshift,
    out, lt_out,
    tokv, rawkv, kvp, normed, w1, w2, w3, wgv, p1, gate, p2, kd, vd, sh, msgs, pre, outs, lt, ltin,
    stage, total, turned, small, rows_in, rows_f, rows_sh, square, send_sem, recv_sem, local_sem,
):
    bf, f32 = jnp.bfloat16, jnp.float32
    w = Wires(send_sem, recv_sem)
    z, y, c, x = (w.at[a] for a in ("z", "y", "c", "x"))
    chip = z * RING + y
    barrier = pltpu.get_barrier_semaphore()
    plane = [(dz, dy) for dz in range(RING) for dy in range(RING) if dz or dy]
    greeted = [w.neighbour(axis, d) for axis in ("z", "y", "x") for d in (1, -1)]
    greeted.append(w.partner())
    for device in greeted:
        pl.semaphore_signal(barrier, inc=1, device_id=device, device_id_type=MESH)

    local = []

    def fetch(src, dst):
        copy = pltpu.make_async_copy(src, dst, local_sem.at[len(local)])
        copy.start()
        local.append(copy)
        return copy

    k_copy, v_copy = fetch(wk, rawkv.at[0]), fetch(wv, rawkv.at[1])
    token_copy = fetch(tok, tokv)

    def block_rows(ref, core, depth, cols):
        start = pl.multiple_of(((z * RING + y) * 2 + core) * depth, 16)
        return ref.at[pl.ds(start, depth), cols]

    def cut(ref, width):
        return lambda h: ref.at[:, pl.ds(pl.multiple_of(h * width, 128), width)]

    pieces = [
        (cut(wq, 256), w1, 128, slice(0, 256)),
        (lambda h: kvp.at[h], w1, 128, slice(256, 384)),
        (cut(wmk, 128), w1, 128, slice(384, 512)),
        (cut(wmv, 128), w1, 128, slice(512, 640)),
        (cut(wmq, 128), w2, 128, slice(0, 128)),
        (cut(wmg, 128), w2, 128, slice(128, 256)),
        (cut(wo, 512), w3, 96, slice(0, 512)),
    ]
    kept = [None] * len(pieces)
    for n, (half_of, dst, depth, cols) in enumerate(pieces):
        if n != 1:
            kept[n] = fetch(half_of(c), block_rows(dst, c, depth, cols))
    gate_copy = fetch(wg, wgv)

    k_copy.wait()
    v_copy.wait()
    kvp[0] = jnp.concatenate([rawkv[0, :, :HD], rawkv[1, :, :HD]], axis=1)
    kvp[1] = jnp.concatenate([rawkv[0, :, HD:], rawkv[1, :, HD:]], axis=1)
    sh[c] = fshift[...]
    kept[1] = fetch(kvp.at[c], block_rows(w1, c, 128, slice(256, 384)))
    pl.semaphore_wait(barrier, len(greeted))

    sizes = (w1.at[0:128, 0:640], w2.at[0:128, :], w3.at[0:96, :])
    for n, (half_of, dst, depth, cols) in enumerate(pieces):
        key = ("over", (n >= 4) + (n >= 6))
        w.send(half_of(1 - c), block_rows(dst, c, depth, cols), w.partner(), "over", key)

    slots = {0: 0, -1: 1, 1: 2, 2: 3}

    def token_rows(dx, ci, part):
        start = slots[dx] * 2 * TOK + ci * TOK
        if part is None:
            return normed.at[pl.ds(pl.multiple_of(start, 16), TOK)]
        return normed.at[pl.ds(pl.multiple_of(start + part * (TOK // 2), 16), TOK // 2)]

    tokens = RowGather(w, token_rows, "tokens", "", relative=True)
    first_row = c * TOK

    def normalize(i, carry):
        values = tokv[pl.ds(pl.multiple_of(i * 16, 16), 16), :].astype(f32)
        rescale = lax.rsqrt(jnp.mean(values * values, axis=-1, keepdims=True) + EPSILON)
        normed[pl.ds(pl.multiple_of(first_row + i * 16, 16), 16), :] = (
            values * rescale * gain[...]
        ).astype(bf)
        return carry

    w.send(fshift, sh.at[c], w.partner(), "shift", "shift")

    def own_ready(first, last):
        for n in range(first, last):
            kept[n].wait()

    def other_ready(group):
        w.arrived(("over", group), sizes[group])

    groups, sent = [], []
    for n, (whole, width, depth, pair) in enumerate(
        ((w1, 640, 128, (0, 4)), (w2, 256, 128, (4, 6)), (w3, 512, 96, (6, 7)))
    ):
        steps, all_sent = plane_steps(
            w, whole, width, depth, ("weights", n),
            functools.partial(own_ready, *pair), functools.partial(other_ready, n),
        )
        groups.append(steps)
        sent.append(all_sent)
    at = [0, 0, 0]

    def pump(group, upto):
        while at[group] < min(upto, len(groups[group])):
            groups[group][at[group]]()
            at[group] += 1

    def pieces_of(i):
        for j in range(4):
            dx, ci = (0, -1, 1, 2)[2 * i + j // 2], j % 2
            yield slice(j * TOK, (j + 1) * TOK), (ci * RING + w.step("x", dx)) * TOK

    def span(start):
        return pl.ds(pl.multiple_of(start, 16), TOK)

    def gate_weights():
        gate_copy.wait()
        for k in range(D // 128):
            turned_gates = jnp.transpose(wgv[:, k * 128 : (k + 1) * 128].astype(f32))
            w1[k * 128 : (k + 1) * 128, 640:672] = turned_gates.astype(bf)

    def attn_projection(i):
        both = dot(normed[i * HALF : (i + 1) * HALF, :], w1[:, :384])
        kv = both[:, 256:]
        turned_kv = pltpu.roll(kv, HD, 1)
        lane = lax.broadcasted_iota(jnp.int32, kv.shape, 1)
        keys = by_head(lane, kv, turned_kv).astype(bf)
        values = by_head(lane, turned_kv, kv).astype(bf)
        for rows, start in pieces_of(i):
            p2[span(start), :] = both[rows, :256].astype(bf)
            kd[span(start + WINDOW), :] = keys[rows]
            vd[span(start + WINDOW), :] = values[rows]

    def first_projection(i):
        both = dot(normed[i * HALF : (i + 1) * HALF, :], w1[:, 384:])
        for rows, start in pieces_of(i):
            p1[span(start), 0:256] = both[rows, :256].astype(bf)
            gate[span(start), 0:32] = both[rows, 256:]

    def second_projection(i):
        both = dot(normed[i * HALF : (i + 1) * HALF, :], w2[...]).astype(bf)
        for rows, start in pieces_of(i):
            p1[span(start), 256:512] = both[rows]

    lane1 = lax.broadcasted_iota(jnp.int32, (1, 128), 1)
    lane = lax.broadcasted_iota(jnp.int32, (128, 128), 1)
    row = lax.broadcasted_iota(jnp.int32, (128, 128), 0)
    scale = HD ** (-0.5)
    feature_attn = 512 * x + 256 * c
    feature_mem = 2048 + 256 * x + 128 * c

    def memory_gates():
        rows_in[...] = jnp.zeros_like(rows_in)
        rows_f[...] = jnp.zeros_like(rows_f)
        rows_sh[...] = jnp.zeros_like(rows_sh)
        gate[:, 32:] = jnp.zeros((ROWS, 96), f32)
        square[...] = jnp.zeros_like(square)
        w.arrived("shift", sh.at[1 - c])
        for b in range(BLOCKS):
            turned[...] = jnp.transpose(gate[b * BLK : (b + 1) * BLK, :])
            for h in range(2):
                own = 4 * x + 2 * c + h
                rows_in[2 * b + h : 2 * b + h + 1, :] = turned[pl.ds(own, 1), :]
                rows_f[2 * b + h : 2 * b + h + 1, :] = turned[pl.ds(16 + own, 1), :]
            q, at_col = b // 3, (b % 3) * BLK
            both = sh[q, :, at_col : at_col + BLK]
            rows_sh[2 * b : 2 * b + 2, :] = jnp.where(c == 0, both[0:2], both[2:4])
        head = lax.broadcasted_iota(jnp.int32, (16, 128), 0) % 2
        pre_forget = rows_f[...] + jnp.where(head == 0, fbias[2 * c], fbias[2 * c + 1])
        log_forget = (
            jnp.minimum(pre_forget, 0.0)
            - jnp.log1p(jnp.exp(-jnp.abs(pre_forget)))
            + rows_sh[...]
        )
        upto = (row <= lane).astype(f32)
        cumulative = jnp.dot(
            log_forget, upto, precision=lax.Precision.HIGHEST, preferred_element_type=f32
        )
        a = rows_in[...] - 0.5 * math.log(CHIPS * ROWS) - cumulative
        top = jnp.max(a, axis=1, keepdims=True)
        weights = jnp.exp(a - top)
        square[0:16, :] = cumulative
        square[16:32, :] = weights
        rows_in[...] = a
        rows_f[...] = weights
        columns = jnp.transpose(square[...])
        square[...] = columns
        ends = cumulative[:, 127:128]
        state = (
            jnp.zeros((1, 128), f32), jnp.zeros((HD, 128), f32), jnp.zeros((1, 128), f32),
            jnp.full((1, 128), MASKED, f32),
        )
        for b in range(BLOCKS):
            put_state(pre.at[b], state)
            rows = slice(b * BLK, (b + 1) * BLK)
            keys, values = p1[rows, 0:128], p1[rows, 128:256]
            spread = by_head(
                lane, columns[:, 16 + 2 * b : 17 + 2 * b], columns[:, 17 + 2 * b : 18 + 2 * b]
            )
            weighted = (values.astype(f32) * spread).astype(bf)
            both = dot(keys, weighted, ((0,), (0,)))
            outer = by_head(lane[:HD], both[:HD], both[HD:]) * scale
            sums = dot(weights.astype(bf), keys)
            normal = by_head(lane1, sums[2 * b : 2 * b + 1], sums[2 * b + 1 : 2 * b + 2]) * scale
            passed = by_head(lane1, ends[2 * b : 2 * b + 1], ends[2 * b + 1 : 2 * b + 2])
            peak = by_head(lane1, top[2 * b : 2 * b + 1], top[2 * b + 1 : 2 * b + 2])
            state = joined(state, (passed, outer, normal, passed + peak))
        small[...] = jnp.zeros_like(small)
        small[0:1, :] = state[2]
        for first, exact in ((1, state[3]), (4, state[0])):
            for k in range(3):
                term = exact.astype(bf).astype(f32)
                small[first + k : first + k + 1, :] = term
                exact = exact - term
        msgs[chip, 0:HD, :] = state[1].astype(bf)
        msgs[chip, HD : HD + 16, :] = small[...].astype(bf)

    def chip_at(dz, dy):
        return w.step("z", dz) * RING + w.step("y", dy)

    def tell_state():
        mine = msgs.at[chip]
        for dz, dy in plane:
            key = ("state", dz, dy)
            w.reserve(key, key)

            @pl.when(chip_at(dz, dy) > chip)
            def _():
                device = w.moved(z=w.step("z", dz), y=w.step("y", dy))
                w.send(mine, mine, device, key, key)

    def incoming_state():
        for dz, dy in plane:

            @pl.when(chip_at(-dz, -dy) < chip)
            def _():
                w.arrived(("state", dz, dy), msgs.at[0])

        state = (
            jnp.zeros((1, 128), f32), jnp.zeros((HD, 128), f32), jnp.zeros((1, 128), f32),
            jnp.full((1, 128), MASKED, f32),
        )
        for other in range(CHIPS - 1):
            rest = msgs[other, HD : HD + 16, :].astype(f32)
            came = (
                rest[4:5] + rest[5:6] + rest[6:7], msgs[other, 0:HD, :].astype(f32),
                rest[0:1], rest[1:2] + rest[2:3] + rest[3:4],
            )
            after = joined(state, came)
            state = tuple(jnp.where(other < chip, new, old) for new, old in zip(after, state))
        return state

    def memory_block(b, incoming):
        rows = slice(b * BLK, (b + 1) * BLK)
        _, state, normal, level = joined(incoming, get_state(pre.at[b]))
        keys, values, query = p1[rows, 0:128], p1[rows, 128:256], p1[rows, 256:384]
        whole = jnp.concatenate(
            [jnp.where(lane[:HD] < HD, state, 0.0), jnp.where(lane[:HD] >= HD, state, 0.0)], axis=0
        ).astype(bf)
        carried_num = dot(query, whole)
        with_normal = query.astype(f32) * normal
        recalled = []
        for h in range(2):
            mine = (lane < HD) if h == 0 else (lane >= HD)
            r = 2 * b + h
            a = jnp.where(row >= lane, rows_in[r : r + 1, :], MASKED)
            stab = level[:, 64 * h : 64 * h + 1]
            high = jnp.maximum(jnp.max(a, axis=1, keepdims=True), stab)
            carried = jnp.exp(stab - high)
            query_h = jnp.where(mine, query, jnp.zeros_like(query))
            affinity = dot(query_h, keys, ((1,), (1,))) * scale * jnp.exp(a - high)
            den = carried * jnp.sum(jnp.where(mine, with_normal, 0.0), axis=1, keepdims=True)
            den = den + jnp.sum(affinity, axis=1, keepdims=True)
            num = carried * carried_num + dot(affinity.astype(bf), values)
            floor = jnp.exp(-(square[:, r : r + 1] + high))
            recalled.append(num / jnp.maximum(jnp.abs(den), floor))
        recall = by_head(lane, recalled[0], recalled[1])
        opened = 1.0 / (1.0 + jnp.exp(-p1[rows, 384:512].astype(f32)))
        outs[rows, pl.ds(pl.multiple_of(feature_mem, 128), 128)] = (recall * opened).astype(bf)

    def attention(first, last):
        query_index = lax.broadcasted_iota(jnp.int32, (WINDOW, 2 * WINDOW), 0)
        key_index = lax.broadcasted_iota(jnp.int32, (WINDOW, 2 * WINDOW), 1)
        distance = query_index - key_index + WINDOW
        in_band = (distance >= 0) & (distance < WINDOW)

        def one_block(b, carry):
            rows = pl.ds(pl.multiple_of(b * WINDOW, WINDOW), WINDOW)
            window = pl.ds(pl.multiple_of(b * WINDOW, WINDOW), 2 * WINDOW)
            keys, values = kd[window, :], vd[window, :]
            allowed = in_band & ((chip * BLOCKS + b) * WINDOW - WINDOW + key_index >= 0)
            logs = jnp.zeros((WINDOW, 128), f32)
            for pair in range(2):
                query = p2[rows, pair * 128 : (pair + 1) * 128]
                results = []
                for half in range(2):
                    h = 2 * pair + half
                    mine = (lane < HD) if half == 0 else (lane >= HD)
                    query_h = jnp.where(mine, query, jnp.zeros_like(query))
                    scores = dot(query_h, keys, ((1,), (1,))) * scale
                    scores = jnp.where(allowed, scores, MASKED)
                    sink = sinks[4 * c + h]
                    ceiling = jnp.maximum(jnp.max(scores, axis=1, keepdims=True), sink)
                    weights = jnp.exp(scores - ceiling)
                    part = jnp.exp(sink - ceiling) + jnp.sum(weights, axis=1, keepdims=True)
                    logs = jnp.where(lane == 4 * c + h, ceiling + jnp.log(part), logs)
                    probs = (weights * (1.0 / part)).astype(bf)
                    results.append(dot(probs, values))
                col = pl.multiple_of(feature_attn + pair * 128, 128)
                outs[rows, pl.ds(col, 128)] = by_head(lane, results[0], results[1]).astype(bf)
            lt[rows, :] = logs
            return carry

        lax.fori_loop(first, last, one_block, 0)

    third = ROWS // 3

    def out_region(start, base, stride, width, group):
        def region(xi, ci, part):
            count = third if part is None else third // 2
            first = start if part is None else start + part * (third // 2)
            col = pl.multiple_of(base + 2 * stride * xi + stride * ci, 128)
            return outs.at[pl.ds(first, count), pl.ds(col, width)]

        return RowGather(w, region, group, start)

    mem_out = [out_region(i * third, 2048, 128, 128, "mem") for i in range(3)]
    attn_out = [out_region(i * third, 0, 256, 256, "attn") for i in range(3)]
    theirs = pl.ds(pl.multiple_of((1 - c) * HALF, HALF), HALF)
    ours = pl.ds(pl.multiple_of(c * HALF, HALF), HALF)

    def normalize_all():
        token_copy.wait()
        lax.fori_loop(0, TOK // 16, normalize, 0)

    kept_values = {}

    def rim_start():
        next_chip = w.moved(z=lax.rem(z + (y + 1) // RING, RING), y=w.step("y", 1))
        for ref in (kd, vd):
            w.send(ref.at[ROWS : ROWS + WINDOW], ref.at[0:WINDOW], next_chip, "rim", "rim")

    def rim_came():
        w.arrived("rim", kd.at[0 : 2 * WINDOW])

    def tokens_shared(late):
        w.arrived(("tokens", "shared", bool(late)), normed.at[0 : 2 * TOK])

    def attn_shared():
        w.arrived(("attn", "shared", False), outs.at[:, 0:1024])

    def mem_shared():
        w.arrived(("mem", "shared", False), outs.at[:, 0:512])

    def finish():
        for all_sent in sent:
            all_sent()
        for group, size in (
            ("over", w1.at[0:256, 0:640]), ("tokens", normed.at[0 : 7 * TOK]), ("shift", sh.at[0]),
            ("rim", kd.at[0 : 2 * WINDOW]),
            ("attn", outs.at[:, 0:1792]), ("mem", outs.at[:, 0:896]), ("log", ltin), ("out", stage),
        ):
            w.all_sent(group, size)
        for dz, dy in plane:

            @pl.when(chip_at(dz, dy) > chip)
            def _():
                w.all_sent(("state", dz, dy), msgs.at[0])

    def state_came():
        kept_values["state"] = incoming_state()

    def memory_blocks(first, last):
        for b in range(first, last):
            memory_block(b, kept_values["state"])

    def out_first(half):
        rows = (theirs, ours)[half]
        total[rows, :] = dot(outs[rows, :2048], w3[:2048])

    def log_start():
        w.send(lt.at[theirs], ltin, w.partner(), "log", "log")

    def out_last():
        out_cols = out.at[:, pl.ds(pl.multiple_of(c * 512, 512), 512)]
        stage[...] = (total[theirs, :] + dot(outs[theirs, 2048:], w3[2048:])).astype(bf)
        w.send(stage, out_cols, w.partner(), "out", "out")
        out[:, pl.ds(pl.multiple_of(c * 512, 512), 512)] = (
            total[ours, :] + dot(outs[ours, 2048:], w3[2048:])
        ).astype(bf)
        w.arrived("log", ltin)
        lt_out[...] = jnp.transpose(lt[ours, :] + ltin[...])[:8]
        w.arrived("out", out.at[:, pl.ds(pl.multiple_of((1 - c) * 512, 512), 512)])

    schedule(
        types.SimpleNamespace(
            pump=pump, normalize=normalize_all, finish=finish, tokens_shared=tokens_shared,
            attn_shared=attn_shared, mem_shared=mem_shared, tokens=tokens, gate_weights=gate_weights,
            attn_projection=attn_projection, first_projection=first_projection, second_projection=second_projection,
            rim_start=rim_start, rim_came=rim_came, memory_gates=memory_gates,
            tell_state=tell_state, state_came=state_came, memory_blocks=memory_blocks,
            attention=attention, attn_out=attn_out, mem_out=mem_out, log_start=log_start, out_first=out_first, out_last=out_last,
        )
    )


def schedule(s):
    pump, attn, mem = s.pump, s.attn_out, s.mem_out
    pump(0, 2)
    s.normalize()
    s.tokens.start()
    pump(0, 8)
    s.gate_weights()
    pump(0, 14)
    s.tokens.came(1)
    s.tokens.came(-1)
    s.tokens_shared(0)
    pump(0, 16)
    pump(1, 4)
    pump(0, 17)
    s.attn_projection(0)
    pump(1, 5)
    s.tokens.done()
    s.first_projection(0)
    pump(1, 8)
    s.tokens_shared(1)
    s.attn_projection(1)
    pump(1, 9)
    s.rim_start()
    s.attention(3, 4)
    s.attention(5, 6)
    pump(1, 13)
    s.first_projection(1)
    pump(1, 14)
    pump(2, 2)
    pump(1, 15)
    pump(2, 4)
    s.attention(4, 5)
    attn[2].start()
    s.memory_gates()
    pump(1, 16)
    s.rim_came()
    s.attention(0, 1)
    s.tell_state()
    s.attention(2, 3)
    attn[1].start()
    s.attention(1, 2)
    attn[0].start()
    pump(2, 5)
    s.log_start()
    attn[2].came(1)
    attn[2].came(-1)
    pump(2, 8)
    pump(1, 17)
    s.second_projection(0)
    attn[1].came(1)
    attn[1].came(-1)
    s.second_projection(1)
    pump(2, 9)
    s.state_came()
    attn[0].came(1)
    attn[0].came(-1)
    s.memory_blocks(0, 1)
    s.memory_blocks(1, 2)
    mem[0].start()
    attn[2].done()
    s.memory_blocks(2, 3)
    s.memory_blocks(3, 4)
    mem[1].start()
    attn[1].done()
    s.memory_blocks(4, 5)
    pump(2, 14)
    s.memory_blocks(5, 6)
    mem[2].start()
    attn[0].done()
    mem[0].came(1)
    mem[0].came(-1)
    s.attn_shared()
    pump(2, 15)
    mem[1].came(1)
    mem[1].came(-1)
    pump(2, 16)
    mem[2].came(1)
    mem[2].came(-1)
    mem[0].done()
    mem[1].done()
    pump(2, 17)
    s.out_first(0)
    mem[2].done()
    s.out_first(1)
    s.mem_shared()
    s.out_last()
    s.finish()


def shards(
    tokens, norm_gain, w_query, w_key, w_value, w_mem_query, w_mem_key, w_mem_value, w_mem_gate,
    w_gates, sinks, forget_bias, forget_shift, w_out,
):
    gates = w_gates.transpose(1, 2, 0).reshape(32, D)
    vmem = pl.BlockSpec(memory_space=pltpu.VMEM)
    smem = pl.BlockSpec(memory_space=pltpu.SMEM)
    anywhere = pl.BlockSpec(memory_space=pl.ANY)
    bf, f32 = jnp.bfloat16, jnp.float32
    mixed, log_total = pl.pallas_call(
        layer_kernel,
        out_shape=[
            pltpu.VMEM((HALF, 1024), bf),
            pltpu.VMEM((8, HALF), f32),
        ],
        in_specs=[anywhere, vmem] + [anywhere] * 9 + [smem, smem, vmem],
        out_specs=[vmem, vmem],
        scratch_shapes=[
            pltpu.VMEM((TOK, D), bf),
            pltpu.VMEM((2, 128, 128), bf),
            pltpu.VMEM((2, 128, 128), bf),
            pltpu.VMEM((ROWS, D), bf),
            pltpu.VMEM((D, 672), bf),
            pltpu.VMEM((D, 256), bf),
            pltpu.VMEM((3072, 512), bf),
            pltpu.VMEM((32, D), bf),
            pltpu.VMEM((ROWS, 512), bf),
            pltpu.VMEM((ROWS, 128), f32),
            pltpu.VMEM((ROWS, 256), bf),
            pltpu.VMEM((ROWS + WINDOW, 128), bf),
            pltpu.VMEM((ROWS + WINDOW, 128), bf),
            pltpu.VMEM((2, 4, HALF), f32),
            pltpu.VMEM((CHIPS, HD + 16, 128), bf),
            pltpu.VMEM((BLOCKS, HD + 8, 128), f32),
            pltpu.VMEM((ROWS, 3072), bf),
            pltpu.VMEM((ROWS, 128), f32),
            pltpu.VMEM((HALF, 128), f32),
            pltpu.VMEM((HALF, 512), bf),
            pltpu.VMEM((ROWS, 512), f32),
            pltpu.VMEM((128, 128), f32),
            pltpu.VMEM((16, 128), f32),
            pltpu.VMEM((16, 128), f32),
            pltpu.VMEM((16, 128), f32),
            pltpu.VMEM((16, 128), f32),
            pltpu.VMEM((128, 128), f32),
            pltpu.SemaphoreType.DMA((SENDS,)),
            pltpu.SemaphoreType.DMA((RECEIVES,)),
            pltpu.SemaphoreType.DMA((11,)),
        ],
        compiler_params=pltpu.CompilerParams(
            collective_id=0, has_side_effects=True, vmem_limit_bytes=60 * 1024 * 1024
        ),
        name="layer",
    )(
        tokens, norm_gain.reshape(1, D), w_query, w_key, w_value, w_mem_query, w_mem_key,
        w_mem_value, w_mem_gate, w_out, gates, sinks, forget_bias, forget_shift.T,
    )
    return (mixed, log_total.T)


def solution(mesh):
    torus = Mesh(mesh.devices.reshape(4, 4, 2, mesh.shape["tp"]), ("z", "y", "c", "x"))
    sp = ("z", "y", "c")
    placed = (
        (P(("z", "y", "c", "x"), None), P())
        + (P(sp, "x"),) * 7
        + (P(), P("x"), P("x"), P(sp, "x"), P(sp, "x"))
    )
    return jax.shard_map(
        shards, mesh=torus, in_specs=placed, out_specs=(P(sp, "x"), P(sp, "x")), check_vma=False
    )
```

```python
import functools
import math
import types

import jax
import jax.numpy as jnp
from jax import lax
from jax.experimental import pallas as pl
from jax.experimental.pallas import tpu as pltpu
from jax.sharding import Mesh
from jax.sharding import PartitionSpec as P

HD = 64
WINDOW = 128
BLK = 128
EPSILON = 1e-06
MASKED = -1e30
MESH = pl.DeviceIdType.MESH
RING = 4
TOK = 96
ROWS = 8 * TOK
D = 4096
PLANE = ("z", "y")
SENDS = 26
RECEIVES = 86
HALF = ROWS // 2
BLOCKS = ROWS // BLK
CHIPS = RING * RING


class Wires:
    def __init__(self, send_sem, recv_sem):
        self.send_sem, self.recv_sem = send_sem, recv_sem
        self.groups, self.keys, self.steps = {}, {}, {}
        z, y, c, x = (lax.axis_index(a) for a in ("z", "y", "c", "x"))
        self.at = {"z": z, "y": y, "c": c, "x": x}
        for axis in ("z", "y", "x"):
            for distance in range(1, RING):
                self.step(axis, distance)

    def moved(self, **new):
        where = dict(self.at)
        where.update(new)
        return (where["z"], where["y"], where["c"], where["x"])

    def step(self, axis, distance):
        if distance % RING == 0:
            return self.at[axis]
        key = (axis, distance % RING)
        if key not in self.steps:
            self.steps[key] = lax.rem(self.at[axis] + key[1], RING)
        return self.steps[key]

    def neighbour(self, axis, distance):
        return self.moved(**{axis: self.step(axis, distance)})

    def partner(self):
        return self.moved(c=1 - self.at["c"])

    def copy(self, src, dst, device, group, key):
        return pltpu.make_async_remote_copy(
            src_ref=src,
            dst_ref=dst,
            send_sem=self.send_sem.at[self.groups.setdefault(group, len(self.groups))],
            recv_sem=self.recv_sem.at[self.keys.setdefault(key, len(self.keys))],
            device_id=device,
            device_id_type=MESH,
        )

    def reserve(self, group, key):
        self.groups.setdefault(group, len(self.groups))
        self.keys.setdefault(key, len(self.keys))

    def send(self, src, dst, device, group, key):
        self.copy(src, dst, device, group, key).start()

    def arrived(self, key, size):
        group = next(iter(self.groups))
        self.copy(size, size, self.partner(), group, key).wait_recv()

    def all_sent(self, group, size):
        key = next(iter(self.keys))
        self.copy(size, size, self.partner(), group, key).wait_send()


class PlaneGather:
    def __init__(self, wires, whole, width, depth, core, name):
        self.w, self.whole, self.width = wires, whole, width
        self.depth, self.core, self.name = depth, core, name

    def mixed(self, axis, one, two):
        first, second = (one, two) if axis == "z" else (two, one)
        return self.w.step(axis, first) * (1 - self.core) + self.w.step(axis, second) * self.core

    def rows(self, d1, d2, part=None):
        z, y = self.mixed("z", d1, d2), self.mixed("y", d1, d2)
        start = ((z * RING + y) * 2 + self.core) * self.depth
        half = self.depth // 2
        if part is None:
            return self.whole.at[pl.ds(pl.multiple_of(start, 16), self.depth), : self.width]
        return self.whole.at[pl.ds(pl.multiple_of(start + part * half, 16), half), : self.width]

    def go(self, key, d1, d2, first, distance, part=None):
        block = self.rows(d1, d2, part)
        one, two = (distance, 0) if first else (0, distance)
        device = self.w.moved(z=self.mixed("z", one, two), y=self.mixed("y", one, two))
        self.w.send(block, block, device, self.name[0], key)

    def came(self, key, blocks):
        self.w.arrived(key, self.whole.at[pl.ds(0, blocks * self.depth), : self.width])

    def second_round(self, d1):
        for side in (1, -1):
            self.go((self.name, "second", d1), d1, 0, False, side)

    def start(self):
        for side in (1, -1):
            self.go((self.name, "first"), 0, 0, True, side)
        self.second_round(0)

    def first_came(self):
        self.came((self.name, "first"), 2)
        for side in (1, -1):
            self.go((self.name, "again"), -side, 0, True, side, 0 if side > 0 else 1)
            self.second_round(-side)

    def second_came(self, d1):
        self.came((self.name, "second", d1), 2)
        for side in (1, -1):
            self.go((self.name[0], "last"), d1, -side, False, side, 0 if side > 0 else 1)

    def first_done(self):
        self.came((self.name, "again"), 1)
        self.second_round(2)

    def all_done(self):
        self.came((self.name[0], "last"), 8)

    def all_sent(self):
        self.w.all_sent(self.name[0], self.whole.at[pl.ds(0, 30 * self.depth), : self.width])


def plane_steps(wires, whole, width, depth, name, own_ready, other_ready):
    c = wires.at["c"]
    pair = [
        PlaneGather(wires, whole, width, depth, core, (name, k))
        for k, core in enumerate((c, 1 - c))
    ]
    steps = [own_ready, pair[0].start, other_ready, pair[1].start]
    steps += [g.first_came for g in pair]
    steps += [functools.partial(g.second_came, 0) for g in pair]
    steps += [g.first_done for g in pair]
    for d1 in (-1, 1, 2):
        steps += [functools.partial(g.second_came, d1) for g in pair]
    return steps + [pair[0].all_done], pair[0].all_sent


class RowGather:
    def __init__(self, wires, region, group, name, relative=False):
        self.w, self.region, self.relative = wires, region, relative
        self.group, self.name = group, name

    def piece(self, dx, other=False, part=None):
        c = self.w.at["c"]
        where = dx if self.relative else self.w.step("x", dx)
        return self.region(where, 1 - c if other else c, part)

    def there(self, dx, side, part=None):
        if self.relative:
            dx = (0, 1, 2, -1)[(dx - side) % RING]
        return self.piece(dx, part=part)

    def share(self, dx):
        block = self.piece(dx)
        key = (self.group, "shared", self.relative and dx in (1, 2))
        self.w.send(block, block, self.w.partner(), self.group, key)

    def start(self):
        for side in (1, -1):
            self.w.send(
                self.piece(0), self.there(0, side), self.w.neighbour("x", side),
                self.group, (self.group, self.name, side),
            )
        self.share(0)

    def came(self, side):
        part = 0 if side > 0 else 1
        self.w.arrived((self.group, self.name, side), self.piece(-side))
        self.w.send(
            self.piece(-side, part=part), self.there(-side, side, part),
            self.w.neighbour("x", side), self.group, (self.group, self.name, 0),
        )
        self.share(-side)

    def done(self):
        self.w.arrived((self.group, self.name, 0), self.piece(2))
        self.share(2)


def dot(a, b, dims=((1,), (0,))):
    return lax.dot_general(a, b, (dims, ((), ())), preferred_element_type=jnp.float32)


def by_head(lane, first, second):
    return jnp.where(lane < HD, first, second)


def joined(one, two):
    passed_one, state_one, normal_one, level_one = one
    passed_two, state_two, normal_two, level_two = two
    level = jnp.maximum(passed_two + level_one, level_two)
    weight_one = jnp.exp(passed_two + level_one - level)
    weight_two = jnp.exp(level_two - level)
    return (
        passed_one + passed_two,
        weight_one * state_one + weight_two * state_two,
        weight_one * normal_one + weight_two * normal_two,
        level,
    )


def put_state(ref, state):
    ref[0:HD, :] = state[1]
    ref[HD : HD + 1, :] = state[2]
    ref[HD + 1 : HD + 2, :] = state[3]
    ref[HD + 2 : HD + 3, :] = state[0]


def get_state(ref):
    return (
        ref[HD + 2 : HD + 3, :], ref[0:HD, :], ref[HD : HD + 1, :], ref[HD + 1 : HD + 2, :]
    )


def layer_kernel(
    tok, gain, wq, wk, wv, wmq, wmk, wmv, wmg, wo, wg, sinks, fbias, fshift,
    out, lt_out,
    tokv, rawkv, kvp, normed, w1, w2, w3, wgv, p1, gate, p2, kd, vd, sh, msgs, pre, outs, lt, ltin,
    stage, total, turned, small, rows_in, rows_f, rows_sh, square, send_sem, recv_sem, local_sem,
):
    bf, f32 = jnp.bfloat16, jnp.float32
    w = Wires(send_sem, recv_sem)
    z, y, c, x = (w.at[a] for a in ("z", "y", "c", "x"))
    chip = z * RING + y
    barrier = pltpu.get_barrier_semaphore()
    plane = [(dz, dy) for dz in range(RING) for dy in range(RING) if dz or dy]
    greeted = [w.neighbour(axis, d) for axis in ("z", "y", "x") for d in (1, -1)]
    greeted.append(w.partner())
    for device in greeted:
        pl.semaphore_signal(barrier, inc=1, device_id=device, device_id_type=MESH)

    local = []

    def fetch(src, dst):
        copy = pltpu.make_async_copy(src, dst, local_sem.at[len(local)])
        copy.start()
        local.append(copy)
        return copy

    k_copy, v_copy = fetch(wk, rawkv.at[0]), fetch(wv, rawkv.at[1])
    token_copy = fetch(tok, tokv)

    def block_rows(ref, core, depth, cols):
        start = pl.multiple_of(((z * RING + y) * 2 + core) * depth, 16)
        return ref.at[pl.ds(start, depth), cols]

    def cut(ref, width):
        return lambda h: ref.at[:, pl.ds(pl.multiple_of(h * width, 128), width)]

    pieces = [
        (cut(wq, 256), w1, 128, slice(0, 256)),
        (lambda h: kvp.at[h], w1, 128, slice(256, 384)),
        (cut(wmk, 128), w1, 128, slice(384, 512)),
        (cut(wmv, 128), w1, 128, slice(512, 640)),
        (cut(wmq, 128), w2, 128, slice(0, 128)),
        (cut(wmg, 128), w2, 128, slice(128, 256)),
        (cut(wo, 512), w3, 96, slice(0, 512)),
    ]
    kept = [None] * len(pieces)
    for n, (half_of, dst, depth, cols) in enumerate(pieces):
        if n != 1:
            kept[n] = fetch(half_of(c), block_rows(dst, c, depth, cols))
    gate_copy = fetch(wg, wgv)

    k_copy.wait()
    v_copy.wait()
    kvp[0] = jnp.concatenate([rawkv[0, :, :HD], rawkv[1, :, :HD]], axis=1)
    kvp[1] = jnp.concatenate([rawkv[0, :, HD:], rawkv[1, :, HD:]], axis=1)
    sh[c] = fshift[...]
    kept[1] = fetch(kvp.at[c], block_rows(w1, c, 128, slice(256, 384)))
    pl.semaphore_wait(barrier, len(greeted))

    sizes = (w1.at[0:128, 0:640], w2.at[0:128, :], w3.at[0:96, :])
    for n, (half_of, dst, depth, cols) in enumerate(pieces):
        key = ("over", (n >= 4) + (n >= 6))
        w.send(half_of(1 - c), block_rows(dst, c, depth, cols), w.partner(), "over", key)

    slots = {0: 0, -1: 1, 1: 2, 2: 3}

    def token_rows(dx, ci, part):
        start = slots[dx] * 2 * TOK + ci * TOK
        if part is None:
            return normed.at[pl.ds(pl.multiple_of(start, 16), TOK)]
        return normed.at[pl.ds(pl.multiple_of(start + part * (TOK // 2), 16), TOK // 2)]

    tokens = RowGather(w, token_rows, "tokens", "", relative=True)
    first_row = c * TOK

    def normalize(i, carry):
        values = tokv[pl.ds(pl.multiple_of(i * 16, 16), 16), :].astype(f32)
        rescale = lax.rsqrt(jnp.mean(values * values, axis=-1, keepdims=True) + EPSILON)
        normed[pl.ds(pl.multiple_of(first_row + i * 16, 16), 16), :] = (
            values * rescale * gain[...]
        ).astype(bf)
        return carry

    w.send(fshift, sh.at[c], w.partner(), "shift", "shift")

    def own_ready(first, last):
        for n in range(first, last):
            kept[n].wait()

    def other_ready(group):
        w.arrived(("over", group), sizes[group])

    groups, sent = [], []
    for n, (whole, width, depth, pair) in enumerate(
        ((w1, 640, 128, (0, 4)), (w2, 256, 128, (4, 6)), (w3, 512, 96, (6, 7)))
    ):
        steps, all_sent = plane_steps(
            w, whole, width, depth, ("weights", n),
            functools.partial(own_ready, *pair), functools.partial(other_ready, n),
        )
        groups.append(steps)
        sent.append(all_sent)
    at = [0, 0, 0]

    def pump(group, upto):
        while at[group] < min(upto, len(groups[group])):
            groups[group][at[group]]()
            at[group] += 1

    def pieces_of(i):
        for j in range(4):
            dx, ci = (0, -1, 1, 2)[2 * i + j // 2], j % 2
            yield slice(j * TOK, (j + 1) * TOK), (ci * RING + w.step("x", dx)) * TOK

    def span(start):
        return pl.ds(pl.multiple_of(start, 16), TOK)

    def gate_weights():
        gate_copy.wait()
        for k in range(D // 128):
            turned_gates = jnp.transpose(wgv[:, k * 128 : (k + 1) * 128].astype(f32))
            w1[k * 128 : (k + 1) * 128, 640:672] = turned_gates.astype(bf)

    def attn_projection(i):
        both = dot(normed[i * HALF : (i + 1) * HALF, :], w1[:, :384])
        kv = both[:, 256:]
        turned_kv = pltpu.roll(kv, HD, 1)
        lane = lax.broadcasted_iota(jnp.int32, kv.shape, 1)
        keys = by_head(lane, kv, turned_kv).astype(bf)
        values = by_head(lane, turned_kv, kv).astype(bf)
        for rows, start in pieces_of(i):
            p2[span(start), :] = both[rows, :256].astype(bf)
            kd[span(start + WINDOW), :] = keys[rows]
            vd[span(start + WINDOW), :] = values[rows]

    def first_projection(i):
        both = dot(normed[i * HALF : (i + 1) * HALF, :], w1[:, 384:])
        for rows, start in pieces_of(i):
            p1[span(start), 0:256] = both[rows, :256].astype(bf)
            gate[span(start), 0:32] = both[rows, 256:]

    def second_projection(i):
        both = dot(normed[i * HALF : (i + 1) * HALF, :], w2[...]).astype(bf)
        for rows, start in pieces_of(i):
            p1[span(start), 256:512] = both[rows]

    lane1 = lax.broadcasted_iota(jnp.int32, (1, 128), 1)
    lane = lax.broadcasted_iota(jnp.int32, (128, 128), 1)
    row = lax.broadcasted_iota(jnp.int32, (128, 128), 0)
    scale = HD ** (-0.5)
    feature_attn = 512 * x + 256 * c
    feature_mem = 2048 + 256 * x + 128 * c

    def memory_gates():
        rows_in[...] = jnp.zeros_like(rows_in)
        rows_f[...] = jnp.zeros_like(rows_f)
        rows_sh[...] = jnp.zeros_like(rows_sh)
        gate[:, 32:] = jnp.zeros((ROWS, 96), f32)
        square[...] = jnp.zeros_like(square)
        w.arrived("shift", sh.at[1 - c])
        for b in range(BLOCKS):
            turned[...] = jnp.transpose(gate[b * BLK : (b + 1) * BLK, :])
            for h in range(2):
                own = 4 * x + 2 * c + h
                rows_in[2 * b + h : 2 * b + h + 1, :] = turned[pl.ds(own, 1), :]
                rows_f[2 * b + h : 2 * b + h + 1, :] = turned[pl.ds(16 + own, 1), :]
            q, at_col = b // 3, (b % 3) * BLK
            both = sh[q, :, at_col : at_col + BLK]
            rows_sh[2 * b : 2 * b + 2, :] = jnp.where(c == 0, both[0:2], both[2:4])
        head = lax.broadcasted_iota(jnp.int32, (16, 128), 0) % 2
        pre_forget = rows_f[...] + jnp.where(head == 0, fbias[2 * c], fbias[2 * c + 1])
        log_forget = (
            jnp.minimum(pre_forget, 0.0)
            - jnp.log1p(jnp.exp(-jnp.abs(pre_forget)))
            + rows_sh[...]
        )
        upto = (row <= lane).astype(f32)
        cumulative = jnp.dot(
            log_forget, upto, precision=lax.Precision.HIGHEST, preferred_element_type=f32
        )
        a = rows_in[...] - 0.5 * math.log(CHIPS * ROWS) - cumulative
        top = jnp.max(a, axis=1, keepdims=True)
        weights = jnp.exp(a - top)
        square[0:16, :] = cumulative
        square[16:32, :] = weights
        rows_in[...] = a
        rows_f[...] = weights
        columns = jnp.transpose(square[...])
        square[...] = columns
        ends = cumulative[:, 127:128]
        state = (
            jnp.zeros((1, 128), f32), jnp.zeros((HD, 128), f32), jnp.zeros((1, 128), f32),
            jnp.full((1, 128), MASKED, f32),
        )
        for b in range(BLOCKS):
            put_state(pre.at[b], state)
            rows = slice(b * BLK, (b + 1) * BLK)
            keys, values = p1[rows, 0:128], p1[rows, 128:256]
            spread = by_head(
                lane, columns[:, 16 + 2 * b : 17 + 2 * b], columns[:, 17 + 2 * b : 18 + 2 * b]
            )
            weighted = (values.astype(f32) * spread).astype(bf)
            both = dot(keys, weighted, ((0,), (0,)))
            outer = by_head(lane[:HD], both[:HD], both[HD:]) * scale
            sums = dot(weights.astype(bf), keys)
            normal = by_head(lane1, sums[2 * b : 2 * b + 1], sums[2 * b + 1 : 2 * b + 2]) * scale
            passed = by_head(lane1, ends[2 * b : 2 * b + 1], ends[2 * b + 1 : 2 * b + 2])
            peak = by_head(lane1, top[2 * b : 2 * b + 1], top[2 * b + 1 : 2 * b + 2])
            state = joined(state, (passed, outer, normal, passed + peak))
        small[...] = jnp.zeros_like(small)
        small[0:1, :] = state[2]
        for first, exact in ((1, state[3]), (4, state[0])):
            for k in range(3):
                term = exact.astype(bf).astype(f32)
                small[first + k : first + k + 1, :] = term
                exact = exact - term
        msgs[chip, 0:HD, :] = state[1].astype(bf)
        msgs[chip, HD : HD + 16, :] = small[...].astype(bf)

    def chip_at(dz, dy):
        return w.step("z", dz) * RING + w.step("y", dy)

    def tell_state():
        mine = msgs.at[chip]
        for dz, dy in plane:
            key = ("state", dz, dy)
            w.reserve(key, key)

            @pl.when(chip_at(dz, dy) > chip)
            def _():
                device = w.moved(z=w.step("z", dz), y=w.step("y", dy))
                w.send(mine, mine, device, key, key)

    def incoming_state():
        for dz, dy in plane:

            @pl.when(chip_at(-dz, -dy) < chip)
            def _():
                w.arrived(("state", dz, dy), msgs.at[0])

        state = (
            jnp.zeros((1, 128), f32), jnp.zeros((HD, 128), f32), jnp.zeros((1, 128), f32),
            jnp.full((1, 128), MASKED, f32),
        )
        for other in range(CHIPS - 1):
            rest = msgs[other, HD : HD + 16, :].astype(f32)
            came = (
                rest[4:5] + rest[5:6] + rest[6:7], msgs[other, 0:HD, :].astype(f32),
                rest[0:1], rest[1:2] + rest[2:3] + rest[3:4],
            )
            after = joined(state, came)
            state = tuple(jnp.where(other < chip, new, old) for new, old in zip(after, state))
        return state

    def memory_block(b, incoming):
        rows = slice(b * BLK, (b + 1) * BLK)
        _, state, normal, level = joined(incoming, get_state(pre.at[b]))
        keys, values, query = p1[rows, 0:128], p1[rows, 128:256], p1[rows, 256:384]
        whole = jnp.concatenate(
            [jnp.where(lane[:HD] < HD, state, 0.0), jnp.where(lane[:HD] >= HD, state, 0.0)], axis=0
        ).astype(bf)
        carried_num = dot(query, whole)
        with_normal = query.astype(f32) * normal
        recalled = []
        for h in range(2):
            mine = (lane < HD) if h == 0 else (lane >= HD)
            r = 2 * b + h
            a = jnp.where(row >= lane, rows_in[r : r + 1, :], MASKED)
            stab = level[:, 64 * h : 64 * h + 1]
            high = jnp.maximum(jnp.max(a, axis=1, keepdims=True), stab)
            carried = jnp.exp(stab - high)
            query_h = jnp.where(mine, query, jnp.zeros_like(query))
            affinity = dot(query_h, keys, ((1,), (1,))) * scale * jnp.exp(a - high)
            den = carried * jnp.sum(jnp.where(mine, with_normal, 0.0), axis=1, keepdims=True)
            den = den + jnp.sum(affinity, axis=1, keepdims=True)
            num = carried * carried_num + dot(affinity.astype(bf), values)
            floor = jnp.exp(-(square[:, r : r + 1] + high))
            recalled.append(num / jnp.maximum(jnp.abs(den), floor))
        recall = by_head(lane, recalled[0], recalled[1])
        opened = 1.0 / (1.0 + jnp.exp(-p1[rows, 384:512].astype(f32)))
        outs[rows, pl.ds(pl.multiple_of(feature_mem, 128), 128)] = (recall * opened).astype(bf)

    def attention(first, last):
        query_index = lax.broadcasted_iota(jnp.int32, (WINDOW, 2 * WINDOW), 0)
        key_index = lax.broadcasted_iota(jnp.int32, (WINDOW, 2 * WINDOW), 1)
        distance = query_index - key_index + WINDOW
        in_band = (distance >= 0) & (distance < WINDOW)

        def one_block(b, carry):
            rows = pl.ds(pl.multiple_of(b * WINDOW, WINDOW), WINDOW)
            window = pl.ds(pl.multiple_of(b * WINDOW, WINDOW), 2 * WINDOW)
            keys, values = kd[window, :], vd[window, :]
            allowed = in_band & ((chip * BLOCKS + b) * WINDOW - WINDOW + key_index >= 0)
            logs = jnp.zeros((WINDOW, 128), f32)
            for pair in range(2):
                query = p2[rows, pair * 128 : (pair + 1) * 128]
                results = []
                for half in range(2):
                    h = 2 * pair + half
                    mine = (lane < HD) if half == 0 else (lane >= HD)
                    query_h = jnp.where(mine, query, jnp.zeros_like(query))
                    scores = dot(query_h, keys, ((1,), (1,))) * scale
                    scores = jnp.where(allowed, scores, MASKED)
                    sink = sinks[4 * c + h]
                    ceiling = jnp.maximum(jnp.max(scores, axis=1, keepdims=True), sink)
                    weights = jnp.exp(scores - ceiling)
                    part = jnp.exp(sink - ceiling) + jnp.sum(weights, axis=1, keepdims=True)
                    logs = jnp.where(lane == 4 * c + h, ceiling + jnp.log(part), logs)
                    probs = (weights * (1.0 / part)).astype(bf)
                    results.append(dot(probs, values))
                col = pl.multiple_of(feature_attn + pair * 128, 128)
                outs[rows, pl.ds(col, 128)] = by_head(lane, results[0], results[1]).astype(bf)
            lt[rows, :] = logs
            return carry

        lax.fori_loop(first, last, one_block, 0)

    third = ROWS // 3

    def out_region(start, base, stride, width, group):
        def region(xi, ci, part):
            count = third if part is None else third // 2
            first = start if part is None else start + part * (third // 2)
            col = pl.multiple_of(base + 2 * stride * xi + stride * ci, 128)
            return outs.at[pl.ds(first, count), pl.ds(col, width)]

        return RowGather(w, region, group, start)

    mem_out = [out_region(i * third, 2048, 128, 128, "mem") for i in range(3)]
    attn_out = [out_region(i * third, 0, 256, 256, "attn") for i in range(3)]
    theirs = pl.ds(pl.multiple_of((1 - c) * HALF, HALF), HALF)
    ours = pl.ds(pl.multiple_of(c * HALF, HALF), HALF)

    def normalize_all():
        token_copy.wait()
        lax.fori_loop(0, TOK // 16, normalize, 0)

    kept_values = {}

    def rim_start():
        next_chip = w.moved(z=lax.rem(z + (y + 1) // RING, RING), y=w.step("y", 1))
        for ref in (kd, vd):
            w.send(ref.at[ROWS : ROWS + WINDOW], ref.at[0:WINDOW], next_chip, "rim", "rim")

    def rim_came():
        w.arrived("rim", kd.at[0 : 2 * WINDOW])

    def tokens_shared(late):
        w.arrived(("tokens", "shared", bool(late)), normed.at[0 : 2 * TOK])

    def attn_shared():
        w.arrived(("attn", "shared", False), outs.at[:, 0:1024])

    def mem_shared():
        w.arrived(("mem", "shared", False), outs.at[:, 0:512])

    def finish():
        for all_sent in sent:
            all_sent()
        for group, size in (
            ("over", w1.at[0:256, 0:640]), ("tokens", normed.at[0 : 7 * TOK]), ("shift", sh.at[0]),
            ("rim", kd.at[0 : 2 * WINDOW]),
            ("attn", outs.at[:, 0:1792]), ("mem", outs.at[:, 0:896]), ("log", ltin), ("out", stage),
        ):
            w.all_sent(group, size)
        for dz, dy in plane:

            @pl.when(chip_at(dz, dy) > chip)
            def _():
                w.all_sent(("state", dz, dy), msgs.at[0])

    def state_came():
        kept_values["state"] = incoming_state()

    def memory_blocks(first, last):
        for b in range(first, last):
            memory_block(b, kept_values["state"])

    def out_first(half):
        rows = (theirs, ours)[half]
        total[rows, :] = dot(outs[rows, :2048], w3[:2048])

    def log_start():
        w.send(lt.at[theirs], ltin, w.partner(), "log", "log")

    def out_last():
        out_cols = out.at[:, pl.ds(pl.multiple_of(c * 512, 512), 512)]
        stage[...] = (total[theirs, :] + dot(outs[theirs, 2048:], w3[2048:])).astype(bf)
        w.send(stage, out_cols, w.partner(), "out", "out")
        out[:, pl.ds(pl.multiple_of(c * 512, 512), 512)] = (
            total[ours, :] + dot(outs[ours, 2048:], w3[2048:])
        ).astype(bf)
        w.arrived("log", ltin)
        lt_out[...] = jnp.transpose(lt[ours, :] + ltin[...])[:8]
        w.arrived("out", out.at[:, pl.ds(pl.multiple_of((1 - c) * 512, 512), 512)])

    schedule(
        types.SimpleNamespace(
            pump=pump, normalize=normalize_all, finish=finish, tokens_shared=tokens_shared,
            attn_shared=attn_shared, mem_shared=mem_shared, tokens=tokens, gate_weights=gate_weights,
            attn_projection=attn_projection, first_projection=first_projection, second_projection=second_projection,
            rim_start=rim_start, rim_came=rim_came, memory_gates=memory_gates,
            tell_state=tell_state, state_came=state_came, memory_blocks=memory_blocks,
            attention=attention, attn_out=attn_out, mem_out=mem_out, log_start=log_start, out_first=out_first, out_last=out_last,
        )
    )


def schedule(s):
    pump, attn, mem = s.pump, s.attn_out, s.mem_out
    pump(0, 2)
    s.normalize()
    s.tokens.start()
    pump(0, 8)
    s.gate_weights()
    pump(0, 14)
    pump(1, 4)
    s.tokens.came(1)
    s.tokens.came(-1)
    pump(0, 16)
    s.tokens.done()
    pump(1, 6)
    pump(1, 8)
    pump(0, 17)
    s.tokens_shared(0)
    s.first_projection(0)
    pump(1, 9)
    s.attn_projection(0)
    pump(1, 14)
    pump(2, 4)
    s.tokens_shared(1)
    s.attn_projection(1)
    s.rim_start()
    s.attention(4, 5)
    pump(1, 15)
    s.attention(2, 3)
    s.attention(3, 4)
    attn[1].start()
    s.first_projection(1)
    pump(1, 16)
    s.memory_gates()
    s.tell_state()
    s.attention(1, 2)
    pump(2, 5)
    s.attention(5, 6)
    attn[2].start()
    pump(2, 7)
    attn[1].came(1)
    attn[1].came(-1)
    pump(2, 8)
    s.rim_came()
    s.attention(0, 1)
    attn[0].start()
    pump(1, 17)
    s.second_projection(0)
    s.second_projection(1)
    s.log_start()
    pump(2, 9)
    attn[2].came(1)
    attn[2].came(-1)
    s.state_came()
    s.memory_blocks(0, 1)
    s.memory_blocks(1, 2)
    mem[0].start()
    attn[1].done()
    s.memory_blocks(2, 3)
    s.memory_blocks(3, 4)
    mem[1].start()
    s.memory_blocks(4, 5)
    s.memory_blocks(5, 6)
    mem[2].start()
    pump(2, 14)
    attn[0].came(1)
    attn[0].came(-1)
    attn[2].done()
    mem[0].came(1)
    mem[0].came(-1)
    pump(2, 15)
    mem[1].came(1)
    mem[1].came(-1)
    pump(2, 16)
    mem[2].came(1)
    mem[2].came(-1)
    attn[0].done()
    mem[0].done()
    mem[1].done()
    mem[2].done()
    pump(2, 17)
    s.attn_shared()
    s.out_first(0)
    s.out_first(1)
    s.mem_shared()
    s.out_last()
    s.finish()


def shards(
    tokens, norm_gain, w_query, w_key, w_value, w_mem_query, w_mem_key, w_mem_value, w_mem_gate,
    w_gates, sinks, forget_bias, forget_shift, w_out,
):
    gates = w_gates.transpose(1, 2, 0).reshape(32, D)
    vmem = pl.BlockSpec(memory_space=pltpu.VMEM)
    smem = pl.BlockSpec(memory_space=pltpu.SMEM)
    anywhere = pl.BlockSpec(memory_space=pl.ANY)
    bf, f32 = jnp.bfloat16, jnp.float32
    mixed, log_total = pl.pallas_call(
        layer_kernel,
        out_shape=[
            pltpu.VMEM((HALF, 1024), bf),
            pltpu.VMEM((8, HALF), f32),
        ],
        in_specs=[anywhere, vmem] + [anywhere] * 9 + [smem, smem, vmem],
        out_specs=[vmem, vmem],
        scratch_shapes=[
            pltpu.VMEM((TOK, D), bf),
            pltpu.VMEM((2, 128, 128), bf),
            pltpu.VMEM((2, 128, 128), bf),
            pltpu.VMEM((ROWS, D), bf),
            pltpu.VMEM((D, 672), bf),
            pltpu.VMEM((D, 256), bf),
            pltpu.VMEM((3072, 512), bf),
            pltpu.VMEM((32, D), bf),
            pltpu.VMEM((ROWS, 512), bf),
            pltpu.VMEM((ROWS, 128), f32),
            pltpu.VMEM((ROWS, 256), bf),
            pltpu.VMEM((ROWS + WINDOW, 128), bf),
            pltpu.VMEM((ROWS + WINDOW, 128), bf),
            pltpu.VMEM((2, 4, HALF), f32),
            pltpu.VMEM((CHIPS, HD + 16, 128), bf),
            pltpu.VMEM((BLOCKS, HD + 8, 128), f32),
            pltpu.VMEM((ROWS, 3072), bf),
            pltpu.VMEM((ROWS, 128), f32),
            pltpu.VMEM((HALF, 128), f32),
            pltpu.VMEM((HALF, 512), bf),
            pltpu.VMEM((ROWS, 512), f32),
            pltpu.VMEM((128, 128), f32),
            pltpu.VMEM((16, 128), f32),
            pltpu.VMEM((16, 128), f32),
            pltpu.VMEM((16, 128), f32),
            pltpu.VMEM((16, 128), f32),
            pltpu.VMEM((128, 128), f32),
            pltpu.SemaphoreType.DMA((SENDS,)),
            pltpu.SemaphoreType.DMA((RECEIVES,)),
            pltpu.SemaphoreType.DMA((11,)),
        ],
        compiler_params=pltpu.CompilerParams(
            collective_id=0, has_side_effects=True, vmem_limit_bytes=60 * 1024 * 1024
        ),
        name="layer",
    )(
        tokens, norm_gain.reshape(1, D), w_query, w_key, w_value, w_mem_query, w_mem_key,
        w_mem_value, w_mem_gate, w_out, gates, sinks, forget_bias, forget_shift.T,
    )
    return (mixed, log_total.T)


def solution(mesh):
    torus = Mesh(mesh.devices.reshape(4, 4, 2, mesh.shape["tp"]), ("z", "y", "c", "x"))
    sp = ("z", "y", "c")
    placed = (
        (P(("z", "y", "c", "x"), None), P())
        + (P(sp, "x"),) * 7
        + (P(), P("x"), P("x"), P(sp, "x"), P(sp, "x"))
    )
    return jax.shard_map(
        shards, mesh=torus, in_specs=placed, out_specs=(P(sp, "x"), P(sp, "x")), check_vma=False
    )
```

```python
import functools
import math
import types

import jax
import jax.numpy as jnp
from jax import lax
from jax.experimental import pallas as pl
from jax.experimental.pallas import tpu as pltpu
from jax.sharding import Mesh
from jax.sharding import PartitionSpec as P

HD = 64
WINDOW = 128
BLK = 128
EPSILON = 1e-06
MASKED = -1e30
MESH = pl.DeviceIdType.MESH
RING = 4
TOK = 96
ROWS = 8 * TOK
D = 4096
PLANE = ("z", "y")
SENDS = 26
RECEIVES = 86
HALF = ROWS // 2
BLOCKS = ROWS // BLK
CHIPS = RING * RING


class Wires:
    def __init__(self, send_sem, recv_sem):
        self.send_sem, self.recv_sem = send_sem, recv_sem
        self.groups, self.keys, self.steps = {}, {}, {}
        z, y, c, x = (lax.axis_index(a) for a in ("z", "y", "c", "x"))
        self.at = {"z": z, "y": y, "c": c, "x": x}
        for axis in ("z", "y", "x"):
            for distance in range(1, RING):
                self.step(axis, distance)

    def moved(self, **new):
        where = dict(self.at)
        where.update(new)
        return (where["z"], where["y"], where["c"], where["x"])

    def step(self, axis, distance):
        if distance % RING == 0:
            return self.at[axis]
        key = (axis, distance % RING)
        if key not in self.steps:
            self.steps[key] = lax.rem(self.at[axis] + key[1], RING)
        return self.steps[key]

    def neighbour(self, axis, distance):
        return self.moved(**{axis: self.step(axis, distance)})

    def partner(self):
        return self.moved(c=1 - self.at["c"])

    def copy(self, src, dst, device, group, key):
        return pltpu.make_async_remote_copy(
            src_ref=src,
            dst_ref=dst,
            send_sem=self.send_sem.at[self.groups.setdefault(group, len(self.groups))],
            recv_sem=self.recv_sem.at[self.keys.setdefault(key, len(self.keys))],
            device_id=device,
            device_id_type=MESH,
        )

    def reserve(self, group, key):
        self.groups.setdefault(group, len(self.groups))
        self.keys.setdefault(key, len(self.keys))

    def send(self, src, dst, device, group, key):
        self.copy(src, dst, device, group, key).start()

    def arrived(self, key, size):
        group = next(iter(self.groups))
        self.copy(size, size, self.partner(), group, key).wait_recv()

    def all_sent(self, group, size):
        key = next(iter(self.keys))
        self.copy(size, size, self.partner(), group, key).wait_send()


class PlaneGather:
    def __init__(self, wires, whole, width, depth, core, name):
        self.w, self.whole, self.width = wires, whole, width
        self.depth, self.core, self.name = depth, core, name

    def mixed(self, axis, one, two):
        first, second = (one, two) if axis == "z" else (two, one)
        return self.w.step(axis, first) * (1 - self.core) + self.w.step(axis, second) * self.core

    def rows(self, d1, d2, part=None):
        z, y = self.mixed("z", d1, d2), self.mixed("y", d1, d2)
        start = ((z * RING + y) * 2 + self.core) * self.depth
        half = self.depth // 2
        if part is None:
            return self.whole.at[pl.ds(pl.multiple_of(start, 16), self.depth), : self.width]
        return self.whole.at[pl.ds(pl.multiple_of(start + part * half, 16), half), : self.width]

    def go(self, key, d1, d2, first, distance, part=None):
        block = self.rows(d1, d2, part)
        one, two = (distance, 0) if first else (0, distance)
        device = self.w.moved(z=self.mixed("z", one, two), y=self.mixed("y", one, two))
        self.w.send(block, block, device, self.name[0], key)

    def came(self, key, blocks):
        self.w.arrived(key, self.whole.at[pl.ds(0, blocks * self.depth), : self.width])

    def second_round(self, d1):
        for side in (1, -1):
            self.go((self.name, "second", d1), d1, 0, False, side)

    def start(self):
        for side in (1, -1):
            self.go((self.name, "first"), 0, 0, True, side)
        self.second_round(0)

    def first_came(self):
        self.came((self.name, "first"), 2)
        for side in (1, -1):
            self.go((self.name, "again"), -side, 0, True, side, 0 if side > 0 else 1)
            self.second_round(-side)

    def second_came(self, d1):
        self.came((self.name, "second", d1), 2)
        for side in (1, -1):
            self.go((self.name[0], "last"), d1, -side, False, side, 0 if side > 0 else 1)

    def first_done(self):
        self.came((self.name, "again"), 1)
        self.second_round(2)

    def all_done(self):
        self.came((self.name[0], "last"), 8)

    def all_sent(self):
        self.w.all_sent(self.name[0], self.whole.at[pl.ds(0, 30 * self.depth), : self.width])


def plane_steps(wires, whole, width, depth, name, own_ready, other_ready):
    c = wires.at["c"]
    pair = [
        PlaneGather(wires, whole, width, depth, core, (name, k))
        for k, core in enumerate((c, 1 - c))
    ]
    steps = [own_ready, pair[0].start, other_ready, pair[1].start]
    steps += [g.first_came for g in pair]
    steps += [functools.partial(g.second_came, 0) for g in pair]
    steps += [g.first_done for g in pair]
    for d1 in (-1, 1, 2):
        steps += [functools.partial(g.second_came, d1) for g in pair]
    return steps + [pair[0].all_done], pair[0].all_sent


class RowGather:
    def __init__(self, wires, region, group, name, relative=False):
        self.w, self.region, self.relative = wires, region, relative
        self.group, self.name = group, name

    def piece(self, dx, other=False, part=None):
        c = self.w.at["c"]
        where = dx if self.relative else self.w.step("x", dx)
        return self.region(where, 1 - c if other else c, part)

    def there(self, dx, side, part=None):
        if self.relative:
            dx = (0, 1, 2, -1)[(dx - side) % RING]
        return self.piece(dx, part=part)

    def share(self, dx):
        block = self.piece(dx)
        key = (self.group, "shared", self.relative and dx in (1, 2))
        self.w.send(block, block, self.w.partner(), self.group, key)

    def start(self):
        for side in (1, -1):
            self.w.send(
                self.piece(0), self.there(0, side), self.w.neighbour("x", side),
                self.group, (self.group, self.name, side),
            )
        self.share(0)

    def came(self, side):
        part = 0 if side > 0 else 1
        self.w.arrived((self.group, self.name, side), self.piece(-side))
        self.w.send(
            self.piece(-side, part=part), self.there(-side, side, part),
            self.w.neighbour("x", side), self.group, (self.group, self.name, 0),
        )
        self.share(-side)

    def done(self):
        self.w.arrived((self.group, self.name, 0), self.piece(2))
        self.share(2)


def dot(a, b, dims=((1,), (0,))):
    return lax.dot_general(a, b, (dims, ((), ())), preferred_element_type=jnp.float32)


def by_head(lane, first, second):
    return jnp.where(lane < HD, first, second)


def joined(one, two):
    passed_one, state_one, normal_one, level_one = one
    passed_two, state_two, normal_two, level_two = two
    level = jnp.maximum(passed_two + level_one, level_two)
    weight_one = jnp.exp(passed_two + level_one - level)
    weight_two = jnp.exp(level_two - level)
    return (
        passed_one + passed_two,
        weight_one * state_one + weight_two * state_two,
        weight_one * normal_one + weight_two * normal_two,
        level,
    )


def put_state(ref, state):
    ref[0:HD, :] = state[1]
    ref[HD : HD + 1, :] = state[2]
    ref[HD + 1 : HD + 2, :] = state[3]
    ref[HD + 2 : HD + 3, :] = state[0]


def get_state(ref):
    return (
        ref[HD + 2 : HD + 3, :], ref[0:HD, :], ref[HD : HD + 1, :], ref[HD + 1 : HD + 2, :]
    )


def layer_kernel(
    tok, gain, wq, wk, wv, wmq, wmk, wmv, wmg, wo, wg, sinks, fbias, fshift,
    out, lt_out,
    tokv, rawkv, kvp, normed, w1, w2, w3, wgv, p1, gate, p2, kd, vd, sh, msgs, pre, outs, lt, ltin,
    stage, total, turned, small, rows_in, rows_f, rows_sh, square, send_sem, recv_sem, local_sem,
):
    bf, f32 = jnp.bfloat16, jnp.float32
    w = Wires(send_sem, recv_sem)
    z, y, c, x = (w.at[a] for a in ("z", "y", "c", "x"))
    chip = z * RING + y
    barrier = pltpu.get_barrier_semaphore()
    plane = [(dz, dy) for dz in range(RING) for dy in range(RING) if dz or dy]
    greeted = [w.neighbour(axis, d) for axis in ("z", "y", "x") for d in (1, -1)]
    greeted.append(w.partner())
    for device in greeted:
        pl.semaphore_signal(barrier, inc=1, device_id=device, device_id_type=MESH)

    local = []

    def fetch(src, dst):
        copy = pltpu.make_async_copy(src, dst, local_sem.at[len(local)])
        copy.start()
        local.append(copy)
        return copy

    k_copy, v_copy = fetch(wk, rawkv.at[0]), fetch(wv, rawkv.at[1])
    token_copy = fetch(tok, tokv)

    def block_rows(ref, core, depth, cols):
        start = pl.multiple_of(((z * RING + y) * 2 + core) * depth, 16)
        return ref.at[pl.ds(start, depth), cols]

    def cut(ref, width):
        return lambda h: ref.at[:, pl.ds(pl.multiple_of(h * width, 128), width)]

    pieces = [
        (cut(wq, 256), w1, 128, slice(0, 256)),
        (lambda h: kvp.at[h], w1, 128, slice(256, 384)),
        (cut(wmk, 128), w1, 128, slice(384, 512)),
        (cut(wmv, 128), w1, 128, slice(512, 640)),
        (cut(wmq, 128), w2, 128, slice(0, 128)),
        (cut(wmg, 128), w2, 128, slice(128, 256)),
        (cut(wo, 512), w3, 96, slice(0, 512)),
    ]
    kept = [None] * len(pieces)
    for n, (half_of, dst, depth, cols) in enumerate(pieces):
        if n != 1:
            kept[n] = fetch(half_of(c), block_rows(dst, c, depth, cols))
    gate_copy = fetch(wg, wgv)

    pl.semaphore_wait(barrier, len(greeted))
    sizes = (w1.at[0:128, 0:640], w2.at[0:128, :], w3.at[0:96, :])

    def swap(n):
        half_of, dst, depth, cols = pieces[n]
        key = ("over", (n >= 4) + (n >= 6))
        w.send(half_of(1 - c), block_rows(dst, c, depth, cols), w.partner(), "over", key)

    for n in (0, 2, 3):
        swap(n)
    k_copy.wait()
    v_copy.wait()
    kvp[0] = jnp.concatenate([rawkv[0, :, :HD], rawkv[1, :, :HD]], axis=1)
    kvp[1] = jnp.concatenate([rawkv[0, :, HD:], rawkv[1, :, HD:]], axis=1)
    sh[c] = fshift[...]
    kept[1] = fetch(kvp.at[c], block_rows(w1, c, 128, slice(256, 384)))
    for n in (1, 4, 5, 6):
        swap(n)

    slots = {0: 0, -1: 1, 1: 2, 2: 3}

    def token_rows(dx, ci, part):
        start = slots[dx] * 2 * TOK + ci * TOK
        if part is None:
            return normed.at[pl.ds(pl.multiple_of(start, 16), TOK)]
        return normed.at[pl.ds(pl.multiple_of(start + part * (TOK // 2), 16), TOK // 2)]

    tokens = RowGather(w, token_rows, "tokens", "", relative=True)
    first_row = c * TOK

    def normalize(i, carry):
        values = tokv[pl.ds(pl.multiple_of(i * 16, 16), 16), :].astype(f32)
        rescale = lax.rsqrt(jnp.mean(values * values, axis=-1, keepdims=True) + EPSILON)
        normed[pl.ds(pl.multiple_of(first_row + i * 16, 16), 16), :] = (
            values * rescale * gain[...]
        ).astype(bf)
        return carry

    w.send(fshift, sh.at[c], w.partner(), "shift", "shift")

    def own_ready(first, last):
        for n in range(first, last):
            kept[n].wait()

    def other_ready(group):
        w.arrived(("over", group), sizes[group])

    groups, sent = [], []
    for n, (whole, width, depth, pair) in enumerate(
        ((w1, 640, 128, (0, 4)), (w2, 256, 128, (4, 6)), (w3, 512, 96, (6, 7)))
    ):
        steps, all_sent = plane_steps(
            w, whole, width, depth, ("weights", n),
            functools.partial(own_ready, *pair), functools.partial(other_ready, n),
        )
        groups.append(steps)
        sent.append(all_sent)
    at = [0, 0, 0]

    def pump(group, upto):
        while at[group] < min(upto, len(groups[group])):
            groups[group][at[group]]()
            at[group] += 1

    def pieces_of(i):
        for j in range(4):
            dx, ci = (0, -1, 1, 2)[2 * i + j // 2], j % 2
            yield slice(j * TOK, (j + 1) * TOK), (ci * RING + w.step("x", dx)) * TOK

    def span(start):
        return pl.ds(pl.multiple_of(start, 16), TOK)

    def gate_weights():
        gate_copy.wait()
        for k in range(D // 128):
            turned_gates = jnp.transpose(wgv[:, k * 128 : (k + 1) * 128].astype(f32))
            w1[k * 128 : (k + 1) * 128, 640:672] = turned_gates.astype(bf)

    def attn_projection(i):
        both = dot(normed[i * HALF : (i + 1) * HALF, :], w1[:, :384])
        kv = both[:, 256:]
        turned_kv = pltpu.roll(kv, HD, 1)
        lane = lax.broadcasted_iota(jnp.int32, kv.shape, 1)
        keys = by_head(lane, kv, turned_kv).astype(bf)
        values = by_head(lane, turned_kv, kv).astype(bf)
        for rows, start in pieces_of(i):
            p2[span(start), :] = both[rows, :256].astype(bf)
            kd[span(start + WINDOW), :] = keys[rows]
            vd[span(start + WINDOW), :] = values[rows]

    def first_projection(i):
        both = dot(normed[i * HALF : (i + 1) * HALF, :], w1[:, 384:])
        for rows, start in pieces_of(i):
            p1[span(start), 0:256] = both[rows, :256].astype(bf)
            gate[span(start), 0:32] = both[rows, 256:]

    def second_projection(i):
        both = dot(normed[i * HALF : (i + 1) * HALF, :], w2[...]).astype(bf)
        for rows, start in pieces_of(i):
            p1[span(start), 256:512] = both[rows]

    lane1 = lax.broadcasted_iota(jnp.int32, (1, 128), 1)
    lane = lax.broadcasted_iota(jnp.int32, (128, 128), 1)
    row = lax.broadcasted_iota(jnp.int32, (128, 128), 0)
    scale = HD ** (-0.5)
    feature_attn = 512 * x + 256 * c
    feature_mem = 2048 + 256 * x + 128 * c

    def memory_gates():
        rows_in[...] = jnp.zeros_like(rows_in)
        rows_f[...] = jnp.zeros_like(rows_f)
        rows_sh[...] = jnp.zeros_like(rows_sh)
        gate[:, 32:] = jnp.zeros((ROWS, 96), f32)
        square[...] = jnp.zeros_like(square)
        w.arrived("shift", sh.at[1 - c])
        for b in range(BLOCKS):
            turned[...] = jnp.transpose(gate[b * BLK : (b + 1) * BLK, :])
            for h in range(2):
                own = 4 * x + 2 * c + h
                rows_in[2 * b + h : 2 * b + h + 1, :] = turned[pl.ds(own, 1), :]
                rows_f[2 * b + h : 2 * b + h + 1, :] = turned[pl.ds(16 + own, 1), :]
            q, at_col = b // 3, (b % 3) * BLK
            both = sh[q, :, at_col : at_col + BLK]
            rows_sh[2 * b : 2 * b + 2, :] = jnp.where(c == 0, both[0:2], both[2:4])
        head = lax.broadcasted_iota(jnp.int32, (16, 128), 0) % 2
        pre_forget = rows_f[...] + jnp.where(head == 0, fbias[2 * c], fbias[2 * c + 1])
        log_forget = (
            jnp.minimum(pre_forget, 0.0)
            - jnp.log1p(jnp.exp(-jnp.abs(pre_forget)))
            + rows_sh[...]
        )
        upto = (row <= lane).astype(f32)
        cumulative = jnp.dot(
            log_forget, upto, precision=lax.Precision.HIGHEST, preferred_element_type=f32
        )
        a = rows_in[...] - 0.5 * math.log(CHIPS * ROWS) - cumulative
        top = jnp.max(a, axis=1, keepdims=True)
        weights = jnp.exp(a - top)
        square[0:16, :] = cumulative
        square[16:32, :] = weights
        rows_in[...] = a
        rows_f[...] = weights
        columns = jnp.transpose(square[...])
        square[...] = columns
        ends = cumulative[:, 127:128]
        state = (
            jnp.zeros((1, 128), f32), jnp.zeros((HD, 128), f32), jnp.zeros((1, 128), f32),
            jnp.full((1, 128), MASKED, f32),
        )
        for b in range(BLOCKS):
            put_state(pre.at[b], state)
            rows = slice(b * BLK, (b + 1) * BLK)
            keys, values = p1[rows, 0:128], p1[rows, 128:256]
            spread = by_head(
                lane, columns[:, 16 + 2 * b : 17 + 2 * b], columns[:, 17 + 2 * b : 18 + 2 * b]
            )
            weighted = (values.astype(f32) * spread).astype(bf)
            both = dot(keys, weighted, ((0,), (0,)))
            outer = by_head(lane[:HD], both[:HD], both[HD:]) * scale
            sums = dot(weights.astype(bf), keys)
            normal = by_head(lane1, sums[2 * b : 2 * b + 1], sums[2 * b + 1 : 2 * b + 2]) * scale
            passed = by_head(lane1, ends[2 * b : 2 * b + 1], ends[2 * b + 1 : 2 * b + 2])
            peak = by_head(lane1, top[2 * b : 2 * b + 1], top[2 * b + 1 : 2 * b + 2])
            state = joined(state, (passed, outer, normal, passed + peak))
        small[...] = jnp.zeros_like(small)
        small[0:1, :] = state[2]
        for first, exact in ((1, state[3]), (4, state[0])):
            for k in range(3):
                term = exact.astype(bf).astype(f32)
                small[first + k : first + k + 1, :] = term
                exact = exact - term
        msgs[chip, 0:HD, :] = state[1].astype(bf)
        msgs[chip, HD : HD + 16, :] = small[...].astype(bf)

    def chip_at(dz, dy):
        return w.step("z", dz) * RING + w.step("y", dy)

    def tell_state():
        mine = msgs.at[chip]
        for dz, dy in plane:
            key = ("state", dz, dy)
            w.reserve(key, key)

            @pl.when(chip_at(dz, dy) > chip)
            def _():
                device = w.moved(z=w.step("z", dz), y=w.step("y", dy))
                w.send(mine, mine, device, key, key)

    def incoming_state():
        for dz, dy in plane:

            @pl.when(chip_at(-dz, -dy) < chip)
            def _():
                w.arrived(("state", dz, dy), msgs.at[0])

        state = (
            jnp.zeros((1, 128), f32), jnp.zeros((HD, 128), f32), jnp.zeros((1, 128), f32),
            jnp.full((1, 128), MASKED, f32),
        )
        for other in range(CHIPS - 1):
            rest = msgs[other, HD : HD + 16, :].astype(f32)
            came = (
                rest[4:5] + rest[5:6] + rest[6:7], msgs[other, 0:HD, :].astype(f32),
                rest[0:1], rest[1:2] + rest[2:3] + rest[3:4],
            )
            after = joined(state, came)
            state = tuple(jnp.where(other < chip, new, old) for new, old in zip(after, state))
        return state

    def memory_block(b, incoming):
        rows = slice(b * BLK, (b + 1) * BLK)
        _, state, normal, level = joined(incoming, get_state(pre.at[b]))
        keys, values, query = p1[rows, 0:128], p1[rows, 128:256], p1[rows, 256:384]
        whole = jnp.concatenate(
            [jnp.where(lane[:HD] < HD, state, 0.0), jnp.where(lane[:HD] >= HD, state, 0.0)], axis=0
        ).astype(bf)
        carried_num = dot(query, whole)
        with_normal = query.astype(f32) * normal
        recalled = []
        for h in range(2):
            mine = (lane < HD) if h == 0 else (lane >= HD)
            r = 2 * b + h
            a = jnp.where(row >= lane, rows_in[r : r + 1, :], MASKED)
            stab = level[:, 64 * h : 64 * h + 1]
            high = jnp.maximum(jnp.max(a, axis=1, keepdims=True), stab)
            carried = jnp.exp(stab - high)
            query_h = jnp.where(mine, query, jnp.zeros_like(query))
            affinity = dot(query_h, keys, ((1,), (1,))) * scale * jnp.exp(a - high)
            den = carried * jnp.sum(jnp.where(mine, with_normal, 0.0), axis=1, keepdims=True)
            den = den + jnp.sum(affinity, axis=1, keepdims=True)
            num = carried * carried_num + dot(affinity.astype(bf), values)
            floor = jnp.exp(-(square[:, r : r + 1] + high))
            recalled.append(num / jnp.maximum(jnp.abs(den), floor))
        recall = by_head(lane, recalled[0], recalled[1])
        opened = 1.0 / (1.0 + jnp.exp(-p1[rows, 384:512].astype(f32)))
        outs[rows, pl.ds(pl.multiple_of(feature_mem, 128), 128)] = (recall * opened).astype(bf)

    def attention(first, last):
        query_index = lax.broadcasted_iota(jnp.int32, (WINDOW, 2 * WINDOW), 0)
        key_index = lax.broadcasted_iota(jnp.int32, (WINDOW, 2 * WINDOW), 1)
        distance = query_index - key_index + WINDOW
        in_band = (distance >= 0) & (distance < WINDOW)

        def one_block(b, carry):
            rows = pl.ds(pl.multiple_of(b * WINDOW, WINDOW), WINDOW)
            window = pl.ds(pl.multiple_of(b * WINDOW, WINDOW), 2 * WINDOW)
            keys, values = kd[window, :], vd[window, :]
            allowed = in_band & ((chip * BLOCKS + b) * WINDOW - WINDOW + key_index >= 0)
            logs = jnp.zeros((WINDOW, 128), f32)
            for pair in range(2):
                query = p2[rows, pair * 128 : (pair + 1) * 128]
                results = []
                for half in range(2):
                    h = 2 * pair + half
                    mine = (lane < HD) if half == 0 else (lane >= HD)
                    query_h = jnp.where(mine, query, jnp.zeros_like(query))
                    scores = dot(query_h, keys, ((1,), (1,))) * scale
                    scores = jnp.where(allowed, scores, MASKED)
                    sink = sinks[4 * c + h]
                    ceiling = jnp.maximum(jnp.max(scores, axis=1, keepdims=True), sink)
                    weights = jnp.exp(scores - ceiling)
                    part = jnp.exp(sink - ceiling) + jnp.sum(weights, axis=1, keepdims=True)
                    logs = jnp.where(lane == 4 * c + h, ceiling + jnp.log(part), logs)
                    probs = (weights * (1.0 / part)).astype(bf)
                    results.append(dot(probs, values))
                col = pl.multiple_of(feature_attn + pair * 128, 128)
                outs[rows, pl.ds(col, 128)] = by_head(lane, results[0], results[1]).astype(bf)
            lt[rows, :] = logs
            return carry

        lax.fori_loop(first, last, one_block, 0)

    third = ROWS // 3

    def out_region(start, base, stride, width, group):
        def region(xi, ci, part):
            count = third if part is None else third // 2
            first = start if part is None else start + part * (third // 2)
            col = pl.multiple_of(base + 2 * stride * xi + stride * ci, 128)
            return outs.at[pl.ds(first, count), pl.ds(col, width)]

        return RowGather(w, region, group, start)

    mem_out = [out_region(i * third, 2048, 128, 128, "mem") for i in range(3)]
    attn_out = [out_region(i * third, 0, 256, 256, "attn") for i in range(3)]
    theirs = pl.ds(pl.multiple_of((1 - c) * HALF, HALF), HALF)
    ours = pl.ds(pl.multiple_of(c * HALF, HALF), HALF)

    def normalize_all():
        token_copy.wait()
        lax.fori_loop(0, TOK // 16, normalize, 0)

    kept_values = {}

    def rim_start():
        next_chip = w.moved(z=lax.rem(z + (y + 1) // RING, RING), y=w.step("y", 1))
        for ref in (kd, vd):
            w.send(ref.at[ROWS : ROWS + WINDOW], ref.at[0:WINDOW], next_chip, "rim", "rim")

    def rim_came():
        w.arrived("rim", kd.at[0 : 2 * WINDOW])

    def tokens_shared(late):
        w.arrived(("tokens", "shared", bool(late)), normed.at[0 : 2 * TOK])

    def attn_shared():
        w.arrived(("attn", "shared", False), outs.at[:, 0:1024])

    def mem_shared():
        w.arrived(("mem", "shared", False), outs.at[:, 0:512])

    def finish():
        for all_sent in sent:
            all_sent()
        for group, size in (
            ("over", w1.at[0:256, 0:640]), ("tokens", normed.at[0 : 7 * TOK]), ("shift", sh.at[0]),
            ("rim", kd.at[0 : 2 * WINDOW]),
            ("attn", outs.at[:, 0:1792]), ("mem", outs.at[:, 0:896]), ("log", ltin), ("out", stage),
        ):
            w.all_sent(group, size)
        for dz, dy in plane:

            @pl.when(chip_at(dz, dy) > chip)
            def _():
                w.all_sent(("state", dz, dy), msgs.at[0])

    def state_came():
        kept_values["state"] = incoming_state()

    def memory_blocks(first, last):
        for b in range(first, last):
            memory_block(b, kept_values["state"])

    def out_first(half):
        rows = (theirs, ours)[half]
        total[rows, :] = dot(outs[rows, :2048], w3[:2048])

    def log_start():
        w.send(lt.at[theirs], ltin, w.partner(), "log", "log")

    def out_last():
        out_cols = out.at[:, pl.ds(pl.multiple_of(c * 512, 512), 512)]
        stage[...] = (total[theirs, :] + dot(outs[theirs, 2048:], w3[2048:])).astype(bf)
        w.send(stage, out_cols, w.partner(), "out", "out")
        out[:, pl.ds(pl.multiple_of(c * 512, 512), 512)] = (
            total[ours, :] + dot(outs[ours, 2048:], w3[2048:])
        ).astype(bf)
        w.arrived("log", ltin)
        lt_out[...] = jnp.transpose(lt[ours, :] + ltin[...])[:8]
        w.arrived("out", out.at[:, pl.ds(pl.multiple_of((1 - c) * 512, 512), 512)])

    schedule(
        types.SimpleNamespace(
            pump=pump, normalize=normalize_all, finish=finish, tokens_shared=tokens_shared,
            attn_shared=attn_shared, mem_shared=mem_shared, tokens=tokens, gate_weights=gate_weights,
            attn_projection=attn_projection, first_projection=first_projection, second_projection=second_projection,
            rim_start=rim_start, rim_came=rim_came, memory_gates=memory_gates,
            tell_state=tell_state, state_came=state_came, memory_blocks=memory_blocks,
            attention=attention, attn_out=attn_out, mem_out=mem_out, log_start=log_start, out_first=out_first, out_last=out_last,
        )
    )


def schedule(s):
    pump, attn, mem = s.pump, s.attn_out, s.mem_out
    pump(0, 2)
    s.normalize()
    s.tokens.start()
    pump(0, 8)
    s.gate_weights()
    pump(0, 12)
    s.tokens.came(1)
    s.tokens.came(-1)
    pump(0, 14)
    pump(1, 4)
    pump(0, 16)
    s.tokens.done()
    pump(1, 6)
    pump(1, 8)
    pump(0, 17)
    s.tokens_shared(0)
    s.first_projection(0)
    pump(1, 9)
    s.attn_projection(0)
    pump(1, 14)
    pump(2, 4)
    s.tokens_shared(1)
    s.attn_projection(1)
    s.rim_start()
    s.attention(4, 5)
    pump(1, 15)
    s.attention(2, 3)
    s.attention(3, 4)
    attn[1].start()
    s.first_projection(1)
    pump(1, 16)
    s.memory_gates()
    s.tell_state()
    s.attention(1, 2)
    pump(2, 5)
    s.attention(5, 6)
    attn[2].start()
    pump(2, 7)
    attn[1].came(1)
    attn[1].came(-1)
    pump(2, 8)
    s.rim_came()
    s.attention(0, 1)
    attn[0].start()
    pump(1, 17)
    s.second_projection(0)
    s.second_projection(1)
    s.log_start()
    pump(2, 9)
    attn[2].came(1)
    attn[2].came(-1)
    s.state_came()
    s.memory_blocks(0, 1)
    s.memory_blocks(1, 2)
    mem[0].start()
    attn[1].done()
    s.memory_blocks(2, 3)
    s.memory_blocks(3, 4)
    mem[1].start()
    s.memory_blocks(4, 5)
    s.memory_blocks(5, 6)
    mem[2].start()
    pump(2, 14)
    attn[0].came(1)
    attn[0].came(-1)
    attn[2].done()
    mem[0].came(1)
    mem[0].came(-1)
    pump(2, 15)
    mem[1].came(1)
    mem[1].came(-1)
    pump(2, 16)
    mem[2].came(1)
    mem[2].came(-1)
    attn[0].done()
    mem[0].done()
    mem[1].done()
    mem[2].done()
    pump(2, 17)
    s.attn_shared()
    s.out_first(0)
    s.out_first(1)
    s.mem_shared()
    s.out_last()
    s.finish()


def shards(
    tokens, norm_gain, w_query, w_key, w_value, w_mem_query, w_mem_key, w_mem_value, w_mem_gate,
    w_gates, sinks, forget_bias, forget_shift, w_out,
):
    gates = w_gates.transpose(1, 2, 0).reshape(32, D)
    vmem = pl.BlockSpec(memory_space=pltpu.VMEM)
    smem = pl.BlockSpec(memory_space=pltpu.SMEM)
    anywhere = pl.BlockSpec(memory_space=pl.ANY)
    bf, f32 = jnp.bfloat16, jnp.float32
    mixed, log_total = pl.pallas_call(
        layer_kernel,
        out_shape=[
            pltpu.VMEM((HALF, 1024), bf),
            pltpu.VMEM((8, HALF), f32),
        ],
        in_specs=[anywhere, vmem] + [anywhere] * 9 + [smem, smem, vmem],
        out_specs=[vmem, vmem],
        scratch_shapes=[
            pltpu.VMEM((TOK, D), bf),
            pltpu.VMEM((2, 128, 128), bf),
            pltpu.VMEM((2, 128, 128), bf),
            pltpu.VMEM((ROWS, D), bf),
            pltpu.VMEM((D, 672), bf),
            pltpu.VMEM((D, 256), bf),
            pltpu.VMEM((3072, 512), bf),
            pltpu.VMEM((32, D), bf),
            pltpu.VMEM((ROWS, 512), bf),
            pltpu.VMEM((ROWS, 128), f32),
            pltpu.VMEM((ROWS, 256), bf),
            pltpu.VMEM((ROWS + WINDOW, 128), bf),
            pltpu.VMEM((ROWS + WINDOW, 128), bf),
            pltpu.VMEM((2, 4, HALF), f32),
            pltpu.VMEM((CHIPS, HD + 16, 128), bf),
            pltpu.VMEM((BLOCKS, HD + 8, 128), f32),
            pltpu.VMEM((ROWS, 3072), bf),
            pltpu.VMEM((ROWS, 128), f32),
            pltpu.VMEM((HALF, 128), f32),
            pltpu.VMEM((HALF, 512), bf),
            pltpu.VMEM((ROWS, 512), f32),
            pltpu.VMEM((128, 128), f32),
            pltpu.VMEM((16, 128), f32),
            pltpu.VMEM((16, 128), f32),
            pltpu.VMEM((16, 128), f32),
            pltpu.VMEM((16, 128), f32),
            pltpu.VMEM((128, 128), f32),
            pltpu.SemaphoreType.DMA((SENDS,)),
            pltpu.SemaphoreType.DMA((RECEIVES,)),
            pltpu.SemaphoreType.DMA((11,)),
        ],
        compiler_params=pltpu.CompilerParams(
            collective_id=0, has_side_effects=True, vmem_limit_bytes=60 * 1024 * 1024
        ),
        name="layer",
    )(
        tokens, norm_gain.reshape(1, D), w_query, w_key, w_value, w_mem_query, w_mem_key,
        w_mem_value, w_mem_gate, w_out, gates, sinks, forget_bias, forget_shift.T,
    )
    return (mixed, log_total.T)


def solution(mesh):
    torus = Mesh(mesh.devices.reshape(4, 4, 2, mesh.shape["tp"]), ("z", "y", "c", "x"))
    sp = ("z", "y", "c")
    placed = (
        (P(("z", "y", "c", "x"), None), P())
        + (P(sp, "x"),) * 7
        + (P(), P("x"), P("x"), P(sp, "x"), P(sp, "x"))
    )
    return jax.shard_map(
        shards, mesh=torus, in_specs=placed, out_specs=(P(sp, "x"), P(sp, "x")), check_vma=False
    )
```
